32 devices in a mesh: grp: 2 (over x), ep: 16 (over z, y, core).
Axes of the slice: x: 2, y: 2, z: 4, core: 2. Of those that a mesh axis runs over, the one named last changes fastest.
Arguments:
- tokens: bfloat16 [8192, 2048], P(('grp', 'ep')), parts along dimension 0, may hold values from -6 to 6
- norm_gain: float32 [2048], replicated, may hold values from 0.1 to 1.9
- routes: int32 [8192, 2], P(('grp', 'ep')), parts along dimension 0, may hold values from 0 to 15, all different within a row; in each aligned block of 256 rows (0 to 255, 256 to 511, ...) at most 40 rows name the same one
- route_weights: float32 [8192, 2], P(('grp', 'ep')), parts along dimension 0, may hold values from 0.2 to 1.5
- expert_gate: bfloat16 [16, 2048, 256], P('ep'), may hold values from -0.125 to 0.125
- expert_up: bfloat16 [16, 2048, 256], P('ep'), may hold values from -0.125 to 0.125
- expert_down: bfloat16 [16, 256, 2048], P('ep'), may hold values from -0.375 to 0.375
- shared_gate: bfloat16 [2048, 256], replicated, may hold values from -0.125 to 0.125
- shared_up: bfloat16 [2048, 256], replicated, may hold values from -0.125 to 0.125
- shared_down: bfloat16 [256, 2048], replicated, may hold values from -0.375 to 0.375
Outputs:
- mixed: bfloat16 [8192, 2048], P(('grp', 'ep')), parts along dimension 0
The draws below stay inside these ranges and needn't reach their ends.
There are 2 independent parts, one for each index of `grp`. The reference program is written for one: setup_inputs(seed, part) draws one part's arguments, and reference() takes and returns one part's arrays. A program takes and returns all parts, laid end to end along the dimension named above; an argument that names none is the same for every part. Nothing has to cross between parts.
Inputs may be any that keep to these rules, and one draw needn't show every extreme that they name: `routes`: the 2 experts of a token are distinct. Among the tokens of one device, at most 40 choose any one expert; in every draw some expert is chosen by exactly 40 tokens of some device.
All inputs are finite; a program needn't handle non-finite values.
Results may differ from the reference program's by a relative error of at most 0.0075.
Values may be sent and summed in bfloat16 or wider, within the bound.
A program may use at most 64 MiB of HBM per device.

```python
import math
import jax
import jax.numpy as jnp
import numpy as np
from jax import lax

D = 2048
DE = 256
DS = 256
TOP_K = 2
TOK_DEV = 256
EXPERTS = 16
TOKENS = 4096
CAPACITY = 40
N_EP = 16


def block_levels(key, dims, cuts, least, largest):
    loudness, own = 1.0, jax.random.fold_in(key, 6)
    for dim, parts in cuts:
        draws = jnp.exp(jax.random.uniform(jax.random.fold_in(own, dim), (parts,), jnp.float32, least / len(cuts), largest / len(cuts)))
        loudness = loudness * jnp.repeat(draws, dims[dim] // parts).reshape([-1 if axis == dim else 1 for axis in range(len(dims))])
    return loudness


def routed_block(key, own, number, rows, amount, top, most, skew):
    sequence = jax.random.permutation(key, amount)
    heavy_load, common = load_shares(amount, rows * top, most, skew, True), load_shares(amount, rows * top, most, skew, False)
    places = jnp.arange(amount)

    def named(tallies, rotation):
        used = int((tallies > 0).sum())
        fixed = max(1, used // 4)
        passed = fixed + (places - fixed + rotation * (used - fixed)) % max(1, amount - fixed)
        return jnp.zeros((amount,), jnp.int32).at[sequence[jnp.where(places < fixed, places, passed)]].set(jnp.asarray(tallies, jnp.int32))

    tallies = jnp.where(number % 4 == 0, named(heavy_load, number // 4), named(common, number - number // 4 - 1))
    mixed = jax.random.permutation(jax.random.fold_in(own, 3), amount)
    source_of, taker = mixed[0:amount // 2 * 2:2], mixed[1:amount // 2 * 2:2]
    room = jnp.minimum(tallies[source_of] - 1, most - tallies[taker]) // 2
    room = jnp.where((source_of == sequence[0]) | (taker == sequence[0]) | (tallies[taker] == 0), 0, jnp.maximum(room, 0))
    passed = jax.random.randint(jax.random.fold_in(own, 4), (amount // 2,), 0, 1 << 20) % (room + 1)
    tallies = tallies.at[source_of].add(-passed).at[taker].add(passed)
    labels = jnp.searchsorted(jnp.cumsum(tallies), jnp.arange(rows * top), side="right").astype(jnp.int32)
    table = labels.reshape(top, rows).T
    table = table[jax.random.permutation(jax.random.fold_in(own, 1), rows)]
    rotation = jax.random.randint(jax.random.fold_in(own, 2), (rows, 1), 0, top)
    return jnp.take_along_axis(table, (jnp.arange(top)[None, :] + rotation) % top, axis=1)


def load_shares(number_of, total, reach, skew, full):
    weights = [(1 << 20) // math.isqrt(grade ** skew) + 1 for grade in range(1, number_of + 1)]
    largest = reach if full else min(reach, max(-(-total // number_of), total * weights[0] // sum(weights)))
    least = 1 if total - largest >= number_of - 1 else 0
    holding, rest = [largest] + [least] * (number_of - 1), total - largest - least * (number_of - 1)
    while rest > 0:
        movable = [i for i in range(1, number_of) if holding[i] < largest] or [i for i in range(1, number_of) if holding[i] < reach]
        whole, left = sum([weights[i] for i in movable]), rest
        for i in movable:
            addition = min(reach - holding[i], max(1, left * weights[i] // whole), rest)
            holding[i] = holding[i] + addition
            rest = rest - addition
    return np.array(holding)


def centred(own_key, dims, spread, limit, shards=(), kind=jnp.bfloat16):
    values = spread * jax.random.normal(own_key, dims, jnp.float32)
    if shards:
        values = values * block_levels(own_key, dims, shards, -0.22, 0.18)
    return jnp.clip(values, -limit, limit).astype(kind)


def setup_inputs(seed: int = 0, part: int = 0) -> dict:
    key_of = jax.random.split(jax.random.key(seed), 11)
    own_keys = jax.random.split(jax.random.fold_in(key_of[10], part), 11)
    tokens = centred(own_keys[0], (TOKENS, D), 1.0, 6.0, ((0, 16),))
    norm_gain = jnp.clip(1.0 + 0.18 * jax.random.normal(key_of[1], (D,), jnp.float32), 0.1, 1.9)
    routes_keys = jax.random.split(jax.random.fold_in(own_keys[2], 1), TOKENS // TOK_DEV)
    routes_turns = jax.random.permutation(jax.random.fold_in(own_keys[2], 3), TOKENS // TOK_DEV)
    routes = jax.vmap(lambda own, number: routed_block(jax.random.fold_in(own_keys[2], 2), own, number, TOK_DEV, EXPERTS, TOP_K, CAPACITY, 2))(routes_keys, routes_turns).reshape((TOKENS, TOP_K))
    route_weights = jnp.clip(0.2 + 1.3 * jax.random.uniform(own_keys[3], (TOKENS, TOP_K), jnp.float32) ** block_levels(own_keys[3], (TOKENS, TOP_K), ((0, 16),), -0.2, 0.2), 0.2, 1.5)
    expert_gate = centred(key_of[4], (EXPERTS, D, DE), D ** -0.5, 0.125, ((0, 16),))
    expert_up = centred(key_of[5], (EXPERTS, D, DE), D ** -0.5, 0.125, ((0, 16),))
    expert_down = centred(key_of[6], (EXPERTS, DE, D), DE ** -0.5, 0.375, ((0, 16),))
    shared_gate = centred(key_of[7], (D, DS), D ** -0.5, 0.125)
    shared_up = centred(key_of[8], (D, DS), D ** -0.5, 0.125)
    shared_down = centred(key_of[9], (DS, D), DS ** -0.5, 0.375)
    return dict(tokens=tokens, norm_gain=norm_gain, routes=routes, route_weights=route_weights, expert_gate=expert_gate, expert_up=expert_up, expert_down=expert_down, shared_gate=shared_gate, shared_up=shared_up, shared_down=shared_down)


def swiglu_rows(row_block, w_gate, w_up, w_down):
    gate_part = jnp.dot(row_block, w_gate, preferred_element_type=jnp.float32)
    up_part = jnp.dot(row_block, w_up, preferred_element_type=jnp.float32)
    hidden = (jax.nn.silu(gate_part) * up_part).astype(jnp.bfloat16)
    return jnp.dot(hidden, w_down, preferred_element_type=jnp.float32)

def reference(tokens, norm_gain, routes, route_weights, expert_gate, expert_up, expert_down, shared_gate, shared_up, shared_down):
    upcast = tokens.astype(jnp.float32)
    factor = lax.rsqrt(lax.optimization_barrier(jnp.mean(upcast * upcast, axis=-1, keepdims=True)) + 1e-06)
    normed = (upcast * factor * norm_gain.astype(jnp.float32)).astype(jnp.bfloat16)
    pair_count = TOKENS * TOP_K
    flat_expert = routes.reshape(-1).astype(jnp.int32)
    onehot = (flat_expert[:, None] == jnp.arange(EXPERTS, dtype=jnp.int32)[None, :]).astype(jnp.int32)
    position = (lax.optimization_barrier(jnp.sum(jnp.cumsum(onehot, axis=0) * onehot, axis=1)) - 1).astype(jnp.int32)
    per_expert = N_EP * CAPACITY
    slot_index = (flat_expert * per_expert + position).astype(jnp.int32)
    pair_token = (jnp.arange(pair_count, dtype=jnp.int32) // TOP_K).astype(jnp.int32)
    slot_token = jnp.full((EXPERTS * per_expert,), TOKENS, jnp.int32).at[slot_index].set(pair_token)
    padded = jnp.concatenate([normed, jnp.zeros((1, D), jnp.bfloat16)], axis=0)

    def one_expert(args):
        table, w_gate, w_up, w_down = args
        return swiglu_rows(padded[table], w_gate, w_up, w_down).astype(jnp.bfloat16)
    outputs = lax.map(one_expert, (slot_token.reshape(EXPERTS, per_expert), expert_gate, expert_up, expert_down))
    pair_out = outputs.reshape(EXPERTS * per_expert, D)[slot_index].astype(jnp.float32).reshape(TOKENS, TOP_K, D)
    routed = lax.optimization_barrier(jnp.sum(pair_out * route_weights[:, :, None], axis=1))
    shared = swiglu_rows(normed, shared_gate, shared_up, shared_down)
    return (routed + shared).astype(jnp.bfloat16)
```

```python
import functools

import jax
import jax.numpy as jnp
from jax import lax
from jax.experimental import pallas as pl
from jax.experimental.pallas import tpu as pltpu
from jax.sharding import PartitionSpec as P

BF16 = jnp.bfloat16
F32 = jnp.float32
PIECES = 2
SLABS = 4


def dot(a, b, dims=((1,), (0,))):
    return lax.dot_general(a, b, (dims, ((), ())), preferred_element_type=F32)


def hidden_rows(rows, w_gate, w_up):
    gate_part = dot(rows, w_gate)
    up_part = dot(rows, w_up)
    return (gate_part / (1.0 + jnp.exp(-gate_part)) * up_part).astype(BF16)


def halves_kernel(
    n, groups, cap,
    tokens_hbm, gain_ref, routes_ref, rw_ref, eg_hbm, eu_hbm, ed_hbm, sg_hbm, su_hbm, sd_hbm,
    out_ref,
    tok, normed, place, scale, wg, wu, wd, fg, fu, fd, sg, su, sd, obuf, arr, ybuf, ret, acc, hid, pick,
    load_sem, wsend, wrecv, xsend, xrecv, dsend, drecv, rsend, rrecv,
):
    half = n // 2
    me = lax.axis_index("ep")
    grp = lax.axis_index("grp")
    base = (me // half) * half
    mine = me % half
    far = (base + half) % n + (mine + half // 2) % half
    rows = tok.shape[0]
    width = tok.shape[1]

    def peer(j):
        total, bit = 0, 1
        while bit < half:
            total = total + bit * (((mine // bit) % 2 + (j // bit) % 2) % 2)
            bit *= 2
        return total

    capp = ret.shape[2]
    if capp > cap:
        low = cap // 16 * 16
        ret[:, :, low:, :] = jnp.zeros((2, half, capp - low, width), BF16)
    barrier = pltpu.get_barrier_semaphore()

    def greet(i, c):
        pl.semaphore_signal(barrier, inc=1, device_id={"ep": base + peer(i)})
        return c

    lax.fori_loop(1, half, greet, 0)
    pl.semaphore_signal(barrier, inc=1, device_id={"ep": far})
    for k in range(1, groups):
        pl.semaphore_signal(barrier, inc=1, device_id={"grp": (grp + k) % groups})

    loads = [(tokens_hbm, tok), (eg_hbm.at[0], wg), (eu_hbm.at[0], wu), (ed_hbm.at[0], wd),
             (sg_hbm, sg), (su_hbm, su), (sd_hbm, sd)]
    loads = [pltpu.make_async_copy(a, b, load_sem.at[i]) for i, (a, b) in enumerate(loads)]
    loads[0].start()

    slab = width // SLABS

    def region(group, a, piece):
        depth = (fg, fu, fd)[a].shape[0] // groups
        if a == 2:
            return pl.ds(pl.multiple_of(group * depth, depth), depth), pl.ds(piece * slab, slab)
        depth = depth // PIECES
        start = (group * PIECES + piece) * depth
        return pl.ds(pl.multiple_of(start, depth), depth), pl.ds(0, fg.shape[1])

    chunks = [(a, piece) for piece in range(PIECES) for a in range(2)]
    chunks += [(2, piece) for piece in range(SLABS)]

    def weight_copy(a, piece):
        src, dst = ((eg_hbm, fg), (eu_hbm, fu), (ed_hbm, fd))[a]
        at, i = region(grp, a, piece), chunks.index((a, piece))
        return pltpu.make_async_remote_copy(
            src_ref=src.at[0, at[0], at[1]], dst_ref=dst.at[at[0], at[1]],
            send_sem=wsend.at[i], recv_sem=wrecv.at[i], device_id={"ep": far})

    def forward_copy(a, piece, k):
        dst = (fg, fu, fd)[a]
        at = region(grp, a, piece)
        i = chunks.index((a, piece)) * max(1, groups - 1) + k - 1
        return pltpu.make_async_remote_copy(
            src_ref=dst.at[at[0], at[1]], dst_ref=dst.at[at[0], at[1]],
            send_sem=xsend.at[i], recv_sem=xrecv.at[i],
            device_id={"grp": (grp + k) % groups})

    pl.semaphore_wait(barrier, half - 1 + 1 + groups - 1)
    weight_copy(*chunks[0]).start()

    lane = lax.broadcasted_iota(jnp.int32, (rows, 128), 1)
    chosen = jnp.zeros((rows, 128), F32)
    weight = jnp.zeros((rows, 128), F32)
    for k in range(routes_ref.shape[1]):
        hit = lane == routes_ref[:, k:k + 1]
        chosen = chosen + jnp.where(hit, 1.0, 0.0)
        weight = weight + jnp.where(hit, rw_ref[:, k:k + 1], 0.0)
    chosen_t = chosen.T
    earlier = (lax.broadcasted_iota(jnp.int32, (rows, rows), 0)
               < lax.broadcasted_iota(jnp.int32, (rows, rows), 1))
    before = dot(chosen_t.astype(BF16), jnp.where(earlier, 1.0, 0.0).astype(BF16))
    place[...] = jnp.where(chosen_t > 0.5, before, -1.0)
    scale[...] = weight.T

    loads[0].wait()
    for copy in loads[1:]:
        copy.start()

    def norm_step(i, c):
        at = pl.ds(pl.multiple_of(i * 32, 32), 32)
        x = tok[at, :].astype(F32)
        factor = lax.rsqrt(jnp.mean(x * x, axis=-1, keepdims=True) + 1e-06)
        normed[at, :] = (x * factor * gain_ref[...]).astype(BF16)
        return c

    lax.fori_loop(0, rows // 32, norm_step, 0)
    slot = lax.broadcasted_iota(jnp.int32, (capp, rows), 0).astype(F32)
    slot = jnp.where(slot < cap, slot, -2.0)

    def gather(p):
        ours = slot == place[pl.ds(base + p, 1), :]
        theirs = slot == place[pl.ds((base + half) % n + (p + half // 2) % half, 1), :]
        want = jnp.concatenate([jnp.where(ours, 1.0, 0.0), jnp.where(theirs, 1.0, 0.0)], axis=0)
        got = dot(want.astype(BF16), normed[...])
        return got[:capp].astype(BF16), got[capp:].astype(BF16)

    used = pl.ds(0, cap)

    def dispatch_copy(p):
        return pltpu.make_async_remote_copy(
            src_ref=obuf.at[:, p, used], dst_ref=arr.at[:, mine, used],
            send_sem=dsend.at[p], recv_sem=drecv.at[mine], device_id={"ep": base + p})

    def dispatch_wait(p):
        pltpu.make_async_remote_copy(
            src_ref=obuf.at[:, p, used], dst_ref=arr.at[:, p, used],
            send_sem=dsend.at[p], recv_sem=drecv.at[p], device_id={"ep": base + p}).wait_recv()

    def message(ref, p, m):
        if m == 0:
            return ref.at[0, p, used]
        return ref.at[1, p, used, pl.ds((m - 1) * slab, slab)]

    def return_copy(p, m):
        return pltpu.make_async_remote_copy(
            src_ref=message(ybuf, p, m), dst_ref=message(ret, mine, m),
            send_sem=rsend.at[p, m], recv_sem=rrecv.at[mine, m], device_id={"ep": base + p})

    def return_wait(p, m):
        pltpu.make_async_remote_copy(
            src_ref=message(ybuf, p, m), dst_ref=message(ret, p, m),
            send_sem=rsend.at[p, m], recv_sem=rrecv.at[p, m],
            device_id={"ep": base + p}).wait_recv()

    def dispatch_step(i, c):
        p = peer(half - 1 - i)
        first, second = gather(p)
        obuf[0, p] = first
        obuf[1, p] = second
        dispatch_copy(p).start()
        return c

    lax.fori_loop(0, half - 1, dispatch_step, 0)
    for a, piece in chunks[1:-SLABS]:
        weight_copy(a, piece).start()
    first, second = gather(mine)
    arr[0, mine] = first
    arr[1, mine] = second

    for copy in loads[4:]:
        copy.wait()
    acc[...] = dot(hidden_rows(normed[...], sg[...], su[...]), sd[...])
    for copy in loads[1:4]:
        copy.wait()

    for b in range(2):
        for p in range(half):
            at = pl.ds((base + b * half) % n + (p + b * (half // 2)) % half, 1)
            want = jnp.where(slot == place[at, :], scale[at, :], 0.0)
            pick[b, p * capp:(p + 1) * capp, :] = want.astype(BF16)

    def own_step(i, c):
        p = peer((i + half // 2 - 1) % (half - 1) + 1)
        dispatch_wait(p)
        ybuf[0, p] = dot(hidden_rows(arr[0, p], wg[...], wu[...]), wd[...]).astype(BF16)
        return_copy(p, 0).start()
        return c

    def forward(a, piece):
        weight_copy(a, piece).wait_recv()
        for k in range(1, groups):
            forward_copy(a, piece, k).start()

    def forwarded(a, piece):
        for k in range(1, groups):
            forward_copy(a, piece, k).wait_recv()

    early = chunks[:-SLABS]
    done = 0
    for i, (a, piece) in enumerate(early):
        until = (half - 1) * (i + 1) // len(early)
        lax.fori_loop(done, until, own_step, 0)
        done = until
        forward(a, piece)
        weight_copy(*chunks[len(early) + i]).start()
    own = dot(hidden_rows(arr[0, mine], wg[...], wu[...]), wd[...]).astype(BF16)
    ret[0, mine] = own

    for a, piece in early:
        forwarded(a, piece)
    hid[...] = hidden_rows(arr[1].reshape(half * capp, width), fg[...], fu[...])

    def far_slab(c):
        forwarded(2, c)
        cols = pl.ds(c * slab, slab)
        got = dot(hid[...], fd[:, cols]).astype(BF16)
        ybuf[1, :, :, cols] = got.reshape(half, capp, slab)

        def send(i, k):
            return_copy(peer(half - 1 - i), 1 + c).start()
            return k

        lax.fori_loop(0, half - 1, send, 0)
        ret[1, mine, :, cols] = ybuf[1, mine, :, cols]

    for c in range(SLABS):
        forward(2, c)
        if c > 0:
            far_slab(c - 1)
    far_slab(SLABS - 1)

    def arrive(m):
        def step(i, k):
            return_wait(peer(i + 1), m)
            return k

        lax.fori_loop(0, half - 1, step, 0)

    arrive(0)
    acc[...] += dot(pick[0], ret[0].reshape(half * capp, width), ((0,), (0,)))
    for c in range(SLABS):
        arrive(1 + c)
        cols = pl.ds(c * slab, slab)
        total = acc[:, cols] + dot(
            pick[1], ret[1, :, :, cols].reshape(half * capp, slab), ((0,), (0,)))
        out_ref[:, cols] = total.astype(BF16)

    def drain(i, c):
        p = peer(half - 1 - i)
        dispatch_copy(p).wait_send()
        for m in range(1 + SLABS):
            return_copy(p, m).wait_send()
        return c

    lax.fori_loop(0, half - 1, drain, 0)
    for a, piece in chunks:
        weight_copy(a, piece).wait_send()
        for k in range(1, groups):
            forward_copy(a, piece, k).wait_send()


def on_halves(tokens, norm_gain, routes, route_weights, expert_gate, expert_up, expert_down,
              shared_gate, shared_up, shared_down):
    rows, width = tokens.shape
    n, groups = lax.axis_size("ep"), lax.axis_size("grp")
    half = n // 2
    cap = -(-(5 * rows * routes.shape[1] // (4 * n)) // 8) * 8
    nchunk = 2 * PIECES + SLABS
    nfwd = nchunk * max(1, groups - 1)
    vmem = lambda shape, kind=BF16: pltpu.VMEM(shape, kind)
    anyspec = pl.BlockSpec(memory_space=pl.ANY)
    vspec = pl.BlockSpec(memory_space=pltpu.VMEM)
    capp = cap
    block = (2, half, capp, width)
    return pl.pallas_call(
        functools.partial(halves_kernel, n, groups, cap),
        out_shape=jax.ShapeDtypeStruct((rows, width), BF16),
        in_specs=[anyspec, vspec, vspec, vspec] + [anyspec] * 6,
        out_specs=vspec,
        scratch_shapes=[
            vmem((rows, width)), vmem((rows, width)), vmem((128, rows), F32), vmem((128, rows), F32),
            vmem(expert_gate.shape[1:]), vmem(expert_up.shape[1:]), vmem(expert_down.shape[1:]),
            vmem(expert_gate.shape[1:]), vmem(expert_up.shape[1:]), vmem(expert_down.shape[1:]),
            vmem(shared_gate.shape), vmem(shared_up.shape), vmem(shared_down.shape),
            vmem(block), vmem(block), vmem(block), vmem(block), vmem((rows, width), F32),
            vmem((half * capp, expert_gate.shape[2])), vmem((2, half * capp, rows)),
            pltpu.SemaphoreType.DMA((7,)),
            pltpu.SemaphoreType.DMA((nchunk,)), pltpu.SemaphoreType.DMA((nchunk,)),
            pltpu.SemaphoreType.DMA((nfwd,)), pltpu.SemaphoreType.DMA((nfwd,)),
            pltpu.SemaphoreType.DMA((half,)), pltpu.SemaphoreType.DMA((half,)),
            pltpu.SemaphoreType.DMA((half, 1 + SLABS)), pltpu.SemaphoreType.DMA((half, 1 + SLABS)),
        ],
        compiler_params=pltpu.CompilerParams(
            collective_id=0, has_side_effects=True, vmem_limit_bytes=60 * 1024 * 1024),
    )(tokens, norm_gain.reshape(1, width), routes, route_weights, expert_gate, expert_up,
      expert_down, shared_gate, shared_up, shared_down)


def layers_kernel(
    n, cap,
    tokens_hbm, gain_ref, routes_ref, rw_ref, eg_hbm, eu_hbm, ed_hbm, sg_hbm, su_hbm, sd_hbm,
    out_ref,
    tok, normed, place, scale, wg, wu, wd, fg, fu, fd, sg, su, sd, obuf, arr, ybuf, ret, acc, hid, pick,
    load_sem, wsend, wrecv, xsend, dsend, drecv, nsend, nrecv, fsend, frecv, osend, orecv,
):
    q = n // 4
    me = lax.axis_index("ep")
    grp = lax.axis_index("grp")
    layer, s = me // q, me % q
    side = layer // 2
    inner = (layer % 3 + 1) // 2
    outer = 1 - inner
    inner_l, outer_l = 1 + side, 3 * side
    other_l = inner_l + outer_l - layer
    far_in, far_out = 2 - side, 3 - 3 * side
    par = (grp + s) % 2
    rows, width = tok.shape
    is_a = (inner == 1) & (par == 0)
    is_b = (inner == 1) & (par == 1)
    is_d = (inner == 0) & (par == 1)

    barrier = pltpu.get_barrier_semaphore()

    def greet(i, c):
        k = (grp * n + me + i) % (2 * n)
        pl.semaphore_signal(barrier, inc=1, device_id={"grp": k // n, "ep": k % n})
        return c

    lax.fori_loop(1, 2 * n, greet, 0)

    loads = [(tokens_hbm, tok), (eg_hbm.at[0], wg), (eu_hbm.at[0], wu), (ed_hbm.at[0], wd),
             (sg_hbm, sg), (su_hbm, su), (sd_hbm, sd)]
    loads = [pltpu.make_async_copy(a, b, load_sem.at[i]) for i, (a, b) in enumerate(loads)]
    for copy in loads:
        copy.start()

    slab = width // SLABS
    depth = fg.shape[0] // PIECES
    chunks = [(a, piece) for piece in range(PIECES) for a in range(2)]
    ngu = len(chunks)
    chunks += [(2, piece) for piece in range(SLABS)]
    far = (fg, fu, fd)

    def region(a, piece):
        if a == 2:
            return pl.ds(0, fd.shape[0]), pl.ds(piece * slab, slab)
        return pl.ds(piece * depth, depth), pl.ds(0, fg.shape[1])

    def weight_copy(i):
        a, piece = chunks[i]
        at = region(a, piece)
        src = (eg_hbm, eu_hbm, ed_hbm)[a]
        return pltpu.make_async_remote_copy(
            src_ref=src.at[0, at[0], at[1]], dst_ref=far[a].at[at[0], at[1]],
            send_sem=wsend.at[i], recv_sem=wrecv.at[i], device_id={"ep": far_in * q + s})

    def relay_copy(i):
        a, piece = chunks[i]
        at = region(a, piece)
        return pltpu.make_async_remote_copy(
            src_ref=far[a].at[at[0], at[1]], dst_ref=far[a].at[at[0], at[1]],
            send_sem=xsend.at[i], recv_sem=wrecv.at[i], device_id={"ep": outer_l * q + s})

    pl.semaphore_wait(barrier, 2 * n - 1)

    @pl.when(is_a)
    def _():
        for i in range(len(chunks)):
            weight_copy(i).start()

    expert = lax.broadcasted_iota(jnp.int32, (128, rows), 0)
    chosen = jnp.zeros((128, rows), F32)
    weight = jnp.zeros((128, rows), F32)
    for k in range(routes_ref.shape[0]):
        hit = expert == routes_ref[k:k + 1, :]
        chosen = chosen + jnp.where(hit, 1.0, 0.0)
        weight = weight + jnp.where(hit, rw_ref[k:k + 1, :], 0.0)
    earlier = (lax.broadcasted_iota(jnp.int32, (rows, rows), 0)
               < lax.broadcasted_iota(jnp.int32, (rows, rows), 1))
    before = dot(chosen.astype(BF16), jnp.where(earlier, 1.0, 0.0).astype(BF16))
    place[...] = jnp.where(chosen > 0.5, before, -1.0)
    scale[...] = weight

    loads[0].wait()

    def norm_step(i, c):
        at = pl.ds(pl.multiple_of(i * 32, 32), 32)
        x = tok[at, :].astype(F32)
        factor = lax.rsqrt(jnp.mean(x * x, axis=-1, keepdims=True) + 1e-06)
        normed[at, :] = (x * factor * gain_ref[...]).astype(BF16)
        return c

    lax.fori_loop(0, rows // 32, norm_step, 0)
    slot = lax.broadcasted_iota(jnp.int32, (cap, rows), 0).astype(F32)

    class_layer = (other_l, layer, far_out, far_in)
    near_at = outer * q + s
    land_at = (near_at, near_at, 2 * q + outer * 2 * q + grp * q + s, 2 * q + grp * q + s)

    def host(cls, t):
        if cls == 0:
            return grp, other_l * q + t
        if cls == 1:
            return grp, layer * q + t
        if cls == 2:
            return (t + 1) % 2, inner_l * q + t
        return t % 2, layer * q + t

    at_home = (None, inner < 2, is_b, par == 0)

    def dispatch_copy(cls, t):
        hg, he = host(cls, t)
        return pltpu.make_async_remote_copy(
            src_ref=obuf.at[cls * q + t], dst_ref=arr.at[land_at[cls]],
            send_sem=dsend.at[cls * q + t], recv_sem=drecv.at[land_at[cls]],
            device_id={"grp": hg, "ep": he})

    def one_hot(cls, values):
        at = [pl.ds(class_layer[cls] * q + t, 1) for t in range(q)]
        return jnp.concatenate([jnp.where(slot == place[a, :], values(a), 0.0) for a in at], axis=0).astype(BF16)

    def dispatch(cls):
        got = dot(one_hot(cls, lambda a: 1.0), normed[...]).astype(BF16)
        obuf[cls * q:(cls + 1) * q] = got.reshape(q, cap, width)

        def send(i, c):
            dispatch_copy(cls, (s + 1 + i) % q).start()
            return c

        lax.fori_loop(0, q - 1, send, 0)
        if cls == 0:
            dispatch_copy(cls, s).start()
            return

        @pl.when(at_home[cls])
        def _():
            arr[land_at[cls]] = obuf[cls * q + s]

        if cls > 1:
            @pl.when(jnp.logical_not(at_home[cls]))
            def _():
                dispatch_copy(cls, s).start()

    for cls in range(4):
        dispatch(cls)

    @pl.when(is_d)
    def _():
        for i in range(len(chunks)):
            weight_copy(i).start()

    for cls in range(4):
        pick[cls] = one_hot(cls, lambda a: scale[a, :])
    for copy in loads[4:]:
        copy.wait()
    acc[...] = dot(hidden_rows(normed[...], sg[...], su[...]), sd[...])
    for copy in loads[1:4]:
        copy.wait()

    def arrived(slot_at):
        pltpu.make_async_remote_copy(
            src_ref=obuf.at[0], dst_ref=arr.at[slot_at], send_sem=dsend.at[0], recv_sem=drecv.at[slot_at],
            device_id={"grp": grp, "ep": other_l * q + s}).wait_recv()

    def near_return(base, cls, t):
        to = (other_l, layer)[cls]
        return pltpu.make_async_remote_copy(
            src_ref=ybuf.at[base + t], dst_ref=ret.at[cls * q + s],
            send_sem=nsend.at[base + t], recv_sem=nrecv.at[cls * q + s], device_id={"ep": to * q + t})

    def near(cls):
        base = (inner * q, outer * q)[cls]

        def wait(i, c):
            arrived(base + (s + 1 + i) % q)
            return c

        lax.fori_loop(0, q - cls, wait, 0)
        block = pl.ds(base, q)
        got = hidden_rows(arr[block].reshape(q * cap, width), wg[...], wu[...])
        ybuf[block] = dot(got, wd[...]).astype(BF16).reshape(q, cap, width)

        def send(i, c):
            near_return(base, cls, (s + 1 + i) % q).start()
            return c

        lax.fori_loop(0, q - cls, send, 0)
        if cls == 1:
            ret[q + s] = ybuf[base + s]

    def far_peer(i):
        k = (grp * q + s + i) % (2 * q)
        return k // q, k % q

    def inner_return(i):
        g, t = far_peer(i)
        return pltpu.make_async_remote_copy(
            src_ref=ybuf.at[2 * q + g * q + t], dst_ref=ret.at[3 * q + s],
            send_sem=fsend.at[g * q + t], recv_sem=frecv.at[s], device_id={"grp": g, "ep": layer * q + t})

    def outer_return(i, m):
        sel, g, t = i // (2 * q), *far_peer(i % (2 * q))
        cols = pl.ds(m * slab, slab)
        k = sel * 2 * q + g * q + t
        return pltpu.make_async_remote_copy(
            src_ref=ybuf.at[2 * q + k, :, cols], dst_ref=ret.at[2 * q + s, :, cols],
            send_sem=osend.at[k, m], recv_sem=orecv.at[s, m],
            device_id={"grp": g, "ep": (inner_l + sel * (outer_l - inner_l)) * q + t})

    def far_arrived(count):
        def wait(i, c):
            g, t = far_peer(i % (2 * q))
            arrived(2 * q + (i // (2 * q)) * 2 * q + g * q + t)
            return c

        lax.fori_loop(1, count, wait, 0)

    def take(i):
        weight_copy(i).wait_recv()

        @pl.when(inner == 1)
        def _():
            relay_copy(i).start()

    @pl.when(is_a)
    def _():
        for i in range(2):
            take(i)

    near(1)

    @pl.when(is_a)
    def _():
        for i in range(2, ngu):
            take(i)

    near(0)

    @pl.when(par == 0)
    def _():
        @pl.when(inner == 0)
        def _():
            for i in range(ngu):
                weight_copy(i).wait_recv()

        far_arrived(2 * q)
        hid[:2 * q * cap] = hidden_rows(
            arr[2 * q:4 * q].reshape(2 * q * cap, width), fg[...], fu[...])
        for i in range(ngu, len(chunks)):
            take(i)
        got = dot(hid[:2 * q * cap], fd[...]).astype(BF16)
        ybuf[2 * q:4 * q] = got.reshape(2 * q, cap, width)

        def send(i, c):
            inner_return(i).start()
            return c

        lax.fori_loop(1, 2 * q, send, 0)
        ret[3 * q + s] = ybuf[2 * q + grp * q + s]

    @pl.when(is_b)
    def _():
        for i in range(ngu):
            weight_copy(i).wait_recv()
        far_arrived(4 * q)
        hid[...] = hidden_rows(arr[2 * q:].reshape(4 * q * cap, width), fg[...], fu[...])
        for m in range(SLABS):
            weight_copy(ngu + m).wait_recv()
            cols = pl.ds(m * slab, slab)
            got = dot(hid[...], fd[:, cols]).astype(BF16)
            ybuf[2 * q:, :, cols] = got.reshape(4 * q, cap, slab)

            def send(i, c):
                outer_return(i, m).start()
                return c

            lax.fori_loop(1, 4 * q, send, 0)
            ret[2 * q + s, :, cols] = ybuf[2 * q + grp * q + s, :, cols]

    def near_back(cls):
        def wait(i, c):
            k = cls * q + (s + 1 + i) % q
            pltpu.make_async_remote_copy(
                src_ref=ybuf.at[0], dst_ref=ret.at[k], send_sem=nsend.at[0], recv_sem=nrecv.at[k],
                device_id={"ep": other_l * q + s}).wait_recv()
            return c

        lax.fori_loop(0, q - cls, wait, 0)

    def inner_back(i, c):
        t = (s + i) % q
        pltpu.make_async_remote_copy(
            src_ref=ybuf.at[0], dst_ref=ret.at[3 * q + t], send_sem=fsend.at[0], recv_sem=frecv.at[t],
            device_id={"ep": other_l * q + s}).wait_recv()
        return c

    def outer_back(m):
        cols = pl.ds(m * slab, slab)

        def wait(i, c):
            t = (s + i) % q
            pltpu.make_async_remote_copy(
                src_ref=ybuf.at[0, :, cols], dst_ref=ret.at[2 * q + t, :, cols], send_sem=osend.at[0, m],
                recv_sem=orecv.at[t, m], device_id={"ep": other_l * q + s}).wait_recv()
            return c

        lax.fori_loop(1, q, wait, 0)

        @pl.when(jnp.logical_not(is_b))
        def _():
            wait(0, 0)

    def weighted(cls, cols):
        return dot(pick[cls], ret[cls * q:(cls + 1) * q, :, cols].reshape(q * cap, -1), ((0,), (0,)))

    near_back(1)
    acc[...] += weighted(1, slice(None))
    lax.fori_loop(1, q, inner_back, 0)

    @pl.when(par == 1)
    def _():
        inner_back(0, 0)

    acc[...] += weighted(3, slice(None))
    near_back(0)
    acc[...] += weighted(0, slice(None))
    for m in range(SLABS):
        outer_back(m)
        cols = slice(m * slab, (m + 1) * slab)
        out_ref[:, cols] = (acc[:, cols] + weighted(2, cols)).astype(BF16)

    for cls in range(4):
        def drain(i, c):
            dispatch_copy(cls, (s + 1 + i) % q).wait_send()
            return c

        lax.fori_loop(0, q - 1, drain, 0)
        if cls == 0:
            dispatch_copy(cls, s).wait_send()
        elif cls > 1:
            @pl.when(jnp.logical_not(at_home[cls]))
            def _():
                dispatch_copy(cls, s).wait_send()

    for cls in range(2):
        base = (inner * q, outer * q)[cls]

        def drain_near(i, c):
            near_return(base, cls, (s + 1 + i) % q).wait_send()
            return c

        lax.fori_loop(0, q - cls, drain_near, 0)

    @pl.when(par == outer)
    def _():
        for i in range(len(chunks)):
            weight_copy(i).wait_send()

    @pl.when(is_a)
    def _():
        for i in range(len(chunks)):
            relay_copy(i).wait_send()

    @pl.when(par == 0)
    def _():
        def drain_inner(i, c):
            inner_return(i).wait_send()
            return c

        lax.fori_loop(1, 2 * q, drain_inner, 0)

    @pl.when(is_b)
    def _():
        def drain_outer(i, c):
            for m in range(SLABS):
                outer_return(i, m).wait_send()
            return c

        lax.fori_loop(1, 4 * q, drain_outer, 0)


def on_layers(tokens, norm_gain, routes, route_weights, expert_gate, expert_up, expert_down,
              shared_gate, shared_up, shared_down):
    rows, width = tokens.shape
    n = lax.axis_size("ep")
    q = n // 4
    cap = -(-(5 * rows * routes.shape[1] // (4 * n)) // 8) * 8
    nchunk = 2 * PIECES + SLABS
    vmem = lambda shape, kind=BF16: pltpu.VMEM(shape, kind)
    sems = lambda *shape: pltpu.SemaphoreType.DMA(shape)
    anyspec = pl.BlockSpec(memory_space=pl.ANY)
    vspec = pl.BlockSpec(memory_space=pltpu.VMEM)
    ff = expert_gate.shape[2]
    return pl.pallas_call(
        functools.partial(layers_kernel, n, cap),
        out_shape=jax.ShapeDtypeStruct((rows, width), BF16),
        in_specs=[anyspec, vspec, vspec, vspec] + [anyspec] * 6,
        out_specs=vspec,
        scratch_shapes=[
            vmem((rows, width)), vmem((rows, width)), vmem((128, rows), F32), vmem((128, rows), F32),
            vmem(expert_gate.shape[1:]), vmem(expert_up.shape[1:]), vmem(expert_down.shape[1:]),
            vmem(expert_gate.shape[1:]), vmem(expert_up.shape[1:]), vmem(expert_down.shape[1:]),
            vmem(shared_gate.shape), vmem(shared_up.shape), vmem(shared_down.shape),
            vmem((n, cap, width)), vmem((6 * q, cap, width)), vmem((6 * q, cap, width)), vmem((n, cap, width)),
            vmem((rows, width), F32), vmem((4 * q * cap, ff)), vmem((4, q * cap, rows)),
            sems(7), sems(nchunk), sems(nchunk), sems(nchunk), sems(n), sems(6 * q),
            sems(2 * q), sems(2 * q), sems(2 * q), sems(q), sems(4 * q, SLABS), sems(q, SLABS),
        ],
        compiler_params=pltpu.CompilerParams(
            collective_id=0, has_side_effects=True, vmem_limit_bytes=60 * 1024 * 1024),
    )(tokens, norm_gain.reshape(1, width), routes.T, route_weights.T, expert_gate, expert_up,
      expert_down, shared_gate, shared_up, shared_down)


def on_device(*args):
    n, groups = lax.axis_size("ep"), lax.axis_size("grp")
    if groups == 2 and n % 8 == 0 and n <= 32:
        return on_layers(*args)
    return on_halves(*args)


def solution(mesh):
    return jax.shard_map(
        on_device,
        mesh=mesh,
        in_specs=(
            P(("grp", "ep"), None),
            P(),
            P(("grp", "ep"), None),
            P(("grp", "ep"), None),
            P("ep", None, None),
            P("ep", None, None),
            P("ep", None, None),
            P(),
            P(),
            P(),
        ),
        out_specs=P(("grp", "ep"), None),
        check_vma=False,
    )
```

```python
import functools

import jax
import jax.numpy as jnp
from jax import lax
from jax.experimental import pallas as pl
from jax.experimental.pallas import tpu as pltpu
from jax.sharding import PartitionSpec as P

BF16 = jnp.bfloat16
F32 = jnp.float32
PIECES = 2
SLABS = 4
PARTS = 4


def dot(a, b, dims=((1,), (0,))):
    return lax.dot_general(a, b, (dims, ((), ())), preferred_element_type=F32)


def hidden_rows(rows, w_gate, w_up):
    gate_part = dot(rows, w_gate)
    up_part = dot(rows, w_up)
    return (gate_part / (1.0 + jnp.exp(-gate_part)) * up_part).astype(BF16)


def halves_kernel(
    n, groups, cap,
    tokens_hbm, gain_ref, routes_ref, rw_ref, eg_hbm, eu_hbm, ed_hbm, sg_hbm, su_hbm, sd_hbm,
    out_ref,
    tok, normed, place, scale, wg, wu, wd, fg, fu, fd, sg, su, sd, obuf, arr, ybuf, ret, acc, hid, pick,
    load_sem, wsend, wrecv, xsend, xrecv, dsend, drecv, rsend, rrecv,
):
    half = n // 2
    me = lax.axis_index("ep")
    grp = lax.axis_index("grp")
    base = (me // half) * half
    mine = me % half
    far = (base + half) % n + (mine + half // 2) % half
    rows = tok.shape[0]
    width = tok.shape[1]

    def peer(j):
        total, bit = 0, 1
        while bit < half:
            total = total + bit * (((mine // bit) % 2 + (j // bit) % 2) % 2)
            bit *= 2
        return total

    capp = ret.shape[2]
    if capp > cap:
        low = cap // 16 * 16
        ret[:, :, low:, :] = jnp.zeros((2, half, capp - low, width), BF16)
    barrier = pltpu.get_barrier_semaphore()

    def greet(i, c):
        pl.semaphore_signal(barrier, inc=1, device_id={"ep": base + peer(i)})
        return c

    lax.fori_loop(1, half, greet, 0)
    pl.semaphore_signal(barrier, inc=1, device_id={"ep": far})
    for k in range(1, groups):
        pl.semaphore_signal(barrier, inc=1, device_id={"grp": (grp + k) % groups})

    loads = [(tokens_hbm, tok), (eg_hbm.at[0], wg), (eu_hbm.at[0], wu), (ed_hbm.at[0], wd),
             (sg_hbm, sg), (su_hbm, su), (sd_hbm, sd)]
    loads = [pltpu.make_async_copy(a, b, load_sem.at[i]) for i, (a, b) in enumerate(loads)]
    loads[0].start()

    slab = width // SLABS

    def region(group, a, piece):
        depth = (fg, fu, fd)[a].shape[0] // groups
        if a == 2:
            return pl.ds(pl.multiple_of(group * depth, depth), depth), pl.ds(piece * slab, slab)
        depth = depth // PIECES
        start = (group * PIECES + piece) * depth
        return pl.ds(pl.multiple_of(start, depth), depth), pl.ds(0, fg.shape[1])

    chunks = [(a, piece) for piece in range(PIECES) for a in range(2)]
    chunks += [(2, piece) for piece in range(SLABS)]

    def weight_copy(a, piece):
        src, dst = ((eg_hbm, fg), (eu_hbm, fu), (ed_hbm, fd))[a]
        at, i = region(grp, a, piece), chunks.index((a, piece))
        return pltpu.make_async_remote_copy(
            src_ref=src.at[0, at[0], at[1]], dst_ref=dst.at[at[0], at[1]],
            send_sem=wsend.at[i], recv_sem=wrecv.at[i], device_id={"ep": far})

    def forward_copy(a, piece, k):
        dst = (fg, fu, fd)[a]
        at = region(grp, a, piece)
        i = chunks.index((a, piece)) * max(1, groups - 1) + k - 1
        return pltpu.make_async_remote_copy(
            src_ref=dst.at[at[0], at[1]], dst_ref=dst.at[at[0], at[1]],
            send_sem=xsend.at[i], recv_sem=xrecv.at[i],
            device_id={"grp": (grp + k) % groups})

    pl.semaphore_wait(barrier, half - 1 + 1 + groups - 1)
    weight_copy(*chunks[0]).start()

    lane = lax.broadcasted_iota(jnp.int32, (rows, 128), 1)
    chosen = jnp.zeros((rows, 128), F32)
    weight = jnp.zeros((rows, 128), F32)
    for k in range(routes_ref.shape[1]):
        hit = lane == routes_ref[:, k:k + 1]
        chosen = chosen + jnp.where(hit, 1.0, 0.0)
        weight = weight + jnp.where(hit, rw_ref[:, k:k + 1], 0.0)
    chosen_t = chosen.T
    earlier = (lax.broadcasted_iota(jnp.int32, (rows, rows), 0)
               < lax.broadcasted_iota(jnp.int32, (rows, rows), 1))
    before = dot(chosen_t.astype(BF16), jnp.where(earlier, 1.0, 0.0).astype(BF16))
    place[...] = jnp.where(chosen_t > 0.5, before, -1.0)
    scale[...] = weight.T

    loads[0].wait()
    for copy in loads[1:]:
        copy.start()

    def norm_step(i, c):
        at = pl.ds(pl.multiple_of(i * 32, 32), 32)
        x = tok[at, :].astype(F32)
        factor = lax.rsqrt(jnp.mean(x * x, axis=-1, keepdims=True) + 1e-06)
        normed[at, :] = (x * factor * gain_ref[...]).astype(BF16)
        return c

    lax.fori_loop(0, rows // 32, norm_step, 0)
    slot = lax.broadcasted_iota(jnp.int32, (capp, rows), 0).astype(F32)
    slot = jnp.where(slot < cap, slot, -2.0)

    def gather(p):
        ours = slot == place[pl.ds(base + p, 1), :]
        theirs = slot == place[pl.ds((base + half) % n + (p + half // 2) % half, 1), :]
        want = jnp.concatenate([jnp.where(ours, 1.0, 0.0), jnp.where(theirs, 1.0, 0.0)], axis=0)
        got = dot(want.astype(BF16), normed[...])
        return got[:capp].astype(BF16), got[capp:].astype(BF16)

    used = pl.ds(0, cap)

    def dispatch_copy(p):
        return pltpu.make_async_remote_copy(
            src_ref=obuf.at[:, p, used], dst_ref=arr.at[:, mine, used],
            send_sem=dsend.at[p], recv_sem=drecv.at[mine], device_id={"ep": base + p})

    def dispatch_wait(p):
        pltpu.make_async_remote_copy(
            src_ref=obuf.at[:, p, used], dst_ref=arr.at[:, p, used],
            send_sem=dsend.at[p], recv_sem=drecv.at[p], device_id={"ep": base + p}).wait_recv()

    def message(ref, p, m):
        if m == 0:
            return ref.at[0, p, used]
        return ref.at[1, p, used, pl.ds((m - 1) * slab, slab)]

    def return_copy(p, m):
        return pltpu.make_async_remote_copy(
            src_ref=message(ybuf, p, m), dst_ref=message(ret, mine, m),
            send_sem=rsend.at[p, m], recv_sem=rrecv.at[mine, m], device_id={"ep": base + p})

    def return_wait(p, m):
        pltpu.make_async_remote_copy(
            src_ref=message(ybuf, p, m), dst_ref=message(ret, p, m),
            send_sem=rsend.at[p, m], recv_sem=rrecv.at[p, m],
            device_id={"ep": base + p}).wait_recv()

    def dispatch_step(i, c):
        p = peer(half - 1 - i)
        first, second = gather(p)
        obuf[0, p] = first
        obuf[1, p] = second
        dispatch_copy(p).start()
        return c

    lax.fori_loop(0, half - 1, dispatch_step, 0)
    for a, piece in chunks[1:-SLABS]:
        weight_copy(a, piece).start()
    first, second = gather(mine)
    arr[0, mine] = first
    arr[1, mine] = second

    for copy in loads[4:]:
        copy.wait()
    acc[...] = dot(hidden_rows(normed[...], sg[...], su[...]), sd[...])
    for copy in loads[1:4]:
        copy.wait()

    for b in range(2):
        for p in range(half):
            at = pl.ds((base + b * half) % n + (p + b * (half // 2)) % half, 1)
            want = jnp.where(slot == place[at, :], scale[at, :], 0.0)
            pick[b, p * capp:(p + 1) * capp, :] = want.astype(BF16)

    def own_step(i, c):
        p = peer((i + half // 2 - 1) % (half - 1) + 1)
        dispatch_wait(p)
        ybuf[0, p] = dot(hidden_rows(arr[0, p], wg[...], wu[...]), wd[...]).astype(BF16)
        return_copy(p, 0).start()
        return c

    def forward(a, piece):
        weight_copy(a, piece).wait_recv()
        for k in range(1, groups):
            forward_copy(a, piece, k).start()

    def forwarded(a, piece):
        for k in range(1, groups):
            forward_copy(a, piece, k).wait_recv()

    early = chunks[:-SLABS]
    done = 0
    for i, (a, piece) in enumerate(early):
        until = (half - 1) * (i + 1) // len(early)
        lax.fori_loop(done, until, own_step, 0)
        done = until
        forward(a, piece)
        weight_copy(*chunks[len(early) + i]).start()
    own = dot(hidden_rows(arr[0, mine], wg[...], wu[...]), wd[...]).astype(BF16)
    ret[0, mine] = own

    for a, piece in early:
        forwarded(a, piece)
    hid[...] = hidden_rows(arr[1].reshape(half * capp, width), fg[...], fu[...])

    def far_slab(c):
        forwarded(2, c)
        cols = pl.ds(c * slab, slab)
        got = dot(hid[...], fd[:, cols]).astype(BF16)
        ybuf[1, :, :, cols] = got.reshape(half, capp, slab)

        def send(i, k):
            return_copy(peer(half - 1 - i), 1 + c).start()
            return k

        lax.fori_loop(0, half - 1, send, 0)
        ret[1, mine, :, cols] = ybuf[1, mine, :, cols]

    for c in range(SLABS):
        forward(2, c)
        if c > 0:
            far_slab(c - 1)
    far_slab(SLABS - 1)

    def arrive(m):
        def step(i, k):
            return_wait(peer(i + 1), m)
            return k

        lax.fori_loop(0, half - 1, step, 0)

    arrive(0)
    acc[...] += dot(pick[0], ret[0].reshape(half * capp, width), ((0,), (0,)))
    for c in range(SLABS):
        arrive(1 + c)
        cols = pl.ds(c * slab, slab)
        total = acc[:, cols] + dot(
            pick[1], ret[1, :, :, cols].reshape(half * capp, slab), ((0,), (0,)))
        out_ref[:, cols] = total.astype(BF16)

    def drain(i, c):
        p = peer(half - 1 - i)
        dispatch_copy(p).wait_send()
        for m in range(1 + SLABS):
            return_copy(p, m).wait_send()
        return c

    lax.fori_loop(0, half - 1, drain, 0)
    for a, piece in chunks:
        weight_copy(a, piece).wait_send()
        for k in range(1, groups):
            forward_copy(a, piece, k).wait_send()


def on_halves(tokens, norm_gain, routes, route_weights, expert_gate, expert_up, expert_down,
              shared_gate, shared_up, shared_down):
    rows, width = tokens.shape
    n, groups = lax.axis_size("ep"), lax.axis_size("grp")
    half = n // 2
    cap = -(-(5 * rows * routes.shape[1] // (4 * n)) // 8) * 8
    nchunk = 2 * PIECES + SLABS
    nfwd = nchunk * max(1, groups - 1)
    vmem = lambda shape, kind=BF16: pltpu.VMEM(shape, kind)
    anyspec = pl.BlockSpec(memory_space=pl.ANY)
    vspec = pl.BlockSpec(memory_space=pltpu.VMEM)
    capp = cap
    block = (2, half, capp, width)
    return pl.pallas_call(
        functools.partial(halves_kernel, n, groups, cap),
        out_shape=jax.ShapeDtypeStruct((rows, width), BF16),
        in_specs=[anyspec, vspec, vspec, vspec] + [anyspec] * 6,
        out_specs=vspec,
        scratch_shapes=[
            vmem((rows, width)), vmem((rows, width)), vmem((128, rows), F32), vmem((128, rows), F32),
            vmem(expert_gate.shape[1:]), vmem(expert_up.shape[1:]), vmem(expert_down.shape[1:]),
            vmem(expert_gate.shape[1:]), vmem(expert_up.shape[1:]), vmem(expert_down.shape[1:]),
            vmem(shared_gate.shape), vmem(shared_up.shape), vmem(shared_down.shape),
            vmem(block), vmem(block), vmem(block), vmem(block), vmem((rows, width), F32),
            vmem((half * capp, expert_gate.shape[2])), vmem((2, half * capp, rows)),
            pltpu.SemaphoreType.DMA((7,)),
            pltpu.SemaphoreType.DMA((nchunk,)), pltpu.SemaphoreType.DMA((nchunk,)),
            pltpu.SemaphoreType.DMA((nfwd,)), pltpu.SemaphoreType.DMA((nfwd,)),
            pltpu.SemaphoreType.DMA((half,)), pltpu.SemaphoreType.DMA((half,)),
            pltpu.SemaphoreType.DMA((half, 1 + SLABS)), pltpu.SemaphoreType.DMA((half, 1 + SLABS)),
        ],
        compiler_params=pltpu.CompilerParams(
            collective_id=0, has_side_effects=True, vmem_limit_bytes=60 * 1024 * 1024),
    )(tokens, norm_gain.reshape(1, width), routes, route_weights, expert_gate, expert_up,
      expert_down, shared_gate, shared_up, shared_down)


def layers_kernel(
    n, cap,
    tokens_hbm, gain_ref, routes_ref, rw_ref, eg_hbm, eu_hbm, ed_hbm, sg_hbm, su_hbm, sd_hbm,
    out_ref,
    tok, normed, place, scale, wg, wu, wd, fg, fu, fd, ng, nu, nd, sg, su, sd, obuf, arr, ybuf, ret, acc, hid, nhid, pick,
    load_sem, wsend, wrecv, xsend, xrecv, dsend, drecv, nsend, nrecv, fsend, frecv, osend, orecv, msend, mrecv,
):
    q = n // 4
    me = lax.axis_index("ep")
    grp = lax.axis_index("grp")
    layer, s = me // q, me % q
    side = layer // 2
    inner = (layer % 3 + 1) // 2
    outer = 1 - inner
    inner_l, outer_l = 1 + side, 3 * side
    other_l = inner_l + outer_l - layer
    far_in, far_out = 2 - side, 3 - 3 * side
    par = (grp + s) % 2
    rows, width = tok.shape
    is_a = (inner == 1) & (par == 0)
    is_b = (inner == 1) & (par == 1)
    is_d = (inner == 0) & (par == 1)

    barrier = pltpu.get_barrier_semaphore()

    def greet(i, c):
        k = (grp * n + me + i) % (2 * n)
        pl.semaphore_signal(barrier, inc=1, device_id={"grp": k // n, "ep": k % n})
        return c

    lax.fori_loop(1, 2 * n, greet, 0)

    loads = [(tokens_hbm, tok), (eg_hbm.at[0], wg), (eu_hbm.at[0], wu), (ed_hbm.at[0], wd),
             (sg_hbm, sg), (su_hbm, su), (sd_hbm, sd)]
    loads = [pltpu.make_async_copy(a, b, load_sem.at[i]) for i, (a, b) in enumerate(loads)]
    for copy in loads:
        copy.start()

    slab = width // SLABS
    depth = fg.shape[0] // PARTS
    chunks = [(a, piece) for piece in range(PARTS) for a in range(2)]
    ngu = len(chunks)
    chunks += [(2, piece) for piece in range(SLABS)]
    far, passed = (fg, fu, fd), (ng, nu, nd)

    def region(a, piece):
        if a == 2:
            return pl.ds(0, fd.shape[0]), pl.ds(piece * slab, slab)
        return pl.ds(piece * depth, depth), pl.ds(0, fg.shape[1])

    def chunk_copy(i, srcs, dsts, send_sem, recv_sem, to):
        a, piece = chunks[i]
        at = region(a, piece)
        src = srcs[a].at[0] if srcs[a].shape[0] == 1 else srcs[a]
        return pltpu.make_async_remote_copy(
            src_ref=src.at[at[0], at[1]], dst_ref=dsts[a].at[at[0], at[1]],
            send_sem=send_sem.at[i], recv_sem=recv_sem.at[i], device_id={"ep": to * q + s})

    own = (eg_hbm, eu_hbm, ed_hbm)

    def cross_copy(i):
        return chunk_copy(i, own, far, wsend, wrecv, far_in)

    def relay_copy(i):
        return chunk_copy(i, far, far, xsend, wrecv, outer_l)

    def inward_copy(i):
        return chunk_copy(i, own, passed, wsend, xrecv, inner_l)

    def onward_copy(i):
        return chunk_copy(i, passed, far, xsend, wrecv, far_in)

    pl.semaphore_wait(barrier, 2 * n - 1)

    @pl.when(is_a)
    def _():
        for i in range(len(chunks)):
            cross_copy(i).start()

    expert = lax.broadcasted_iota(jnp.int32, (128, rows), 0)
    chosen = jnp.zeros((128, rows), F32)
    weight = jnp.zeros((128, rows), F32)
    for k in range(routes_ref.shape[0]):
        hit = expert == routes_ref[k:k + 1, :]
        chosen = chosen + jnp.where(hit, 1.0, 0.0)
        weight = weight + jnp.where(hit, rw_ref[k:k + 1, :], 0.0)
    earlier = (lax.broadcasted_iota(jnp.int32, (rows, rows), 0)
               < lax.broadcasted_iota(jnp.int32, (rows, rows), 1))
    before = dot(chosen.astype(BF16), jnp.where(earlier, 1.0, 0.0).astype(BF16))
    place[...] = jnp.where(chosen > 0.5, before, -1.0)
    scale[...] = weight

    loads[0].wait()

    def norm_step(i, c):
        at = pl.ds(pl.multiple_of(i * 32, 32), 32)
        x = tok[at, :].astype(F32)
        factor = lax.rsqrt(jnp.mean(x * x, axis=-1, keepdims=True) + 1e-06)
        normed[at, :] = (x * factor * gain_ref[...]).astype(BF16)
        return c

    lax.fori_loop(0, rows // 32, norm_step, 0)
    slot = lax.broadcasted_iota(jnp.int32, (cap, rows), 0).astype(F32)

    class_layer = (other_l, layer, far_out, far_in)
    near_at = outer * q + s
    land_at = (outer * near_at + inner * (6 * q + grp * q + s), near_at, 2 * q + outer * 2 * q + grp * q + s, 2 * q + grp * q + s)

    def host(cls, t):
        if cls == 0:
            return outer * grp + inner * ((t + 1) % 2), inner_l * q + t
        if cls == 1:
            return grp, layer * q + t
        if cls == 2:
            return (t + 1) % 2, inner_l * q + t
        return t % 2, layer * q + t

    at_home = (is_b, inner < 2, is_b, par == 0)

    def dispatch_copy(cls, t):
        hg, he = host(cls, t)
        return pltpu.make_async_remote_copy(
            src_ref=obuf.at[cls * q + t], dst_ref=arr.at[land_at[cls]],
            send_sem=dsend.at[cls * q + t], recv_sem=drecv.at[land_at[cls]],
            device_id={"grp": hg, "ep": he})

    def one_hot(cls, values):
        at = [pl.ds(class_layer[cls] * q + t, 1) for t in range(q)]
        return jnp.concatenate([jnp.where(slot == place[a, :], values(a), 0.0) for a in at], axis=0).astype(BF16)

    def dispatch(cls):
        got = dot(one_hot(cls, lambda a: 1.0), normed[...]).astype(BF16)
        obuf[cls * q:(cls + 1) * q] = got.reshape(q, cap, width)

        def send(i, c):
            dispatch_copy(cls, (s + 1 + i) % q).start()
            return c

        lax.fori_loop(0, q - 1, send, 0)

        @pl.when(at_home[cls])
        def _():
            arr[land_at[cls]] = obuf[cls * q + s]

        if cls != 1:
            @pl.when(jnp.logical_not(at_home[cls]))
            def _():
                dispatch_copy(cls, s).start()

    for cls in (1, 0, 3):
        dispatch(cls)

    @pl.when(is_d)
    def _():
        for i in range(ngu):
            inward_copy(i).start()

    dispatch(2)

    @pl.when(is_d)
    def _():
        for i in range(ngu, len(chunks)):
            inward_copy(i).start()

    for cls in range(4):
        pick[cls] = one_hot(cls, lambda a: scale[a, :])
    for copy in loads[4:]:
        copy.wait()
    acc[...] = dot(hidden_rows(normed[...], sg[...], su[...]), sd[...])
    for copy in loads[1:4]:
        copy.wait()

    def arrived(slot_at):
        pltpu.make_async_remote_copy(
            src_ref=obuf.at[0], dst_ref=arr.at[slot_at], send_sem=dsend.at[0], recv_sem=drecv.at[slot_at],
            device_id={"grp": grp, "ep": other_l * q + s}).wait_recv()

    def near_return(base, cls, t):
        to = (other_l, layer)[cls]
        return pltpu.make_async_remote_copy(
            src_ref=ybuf.at[base + t], dst_ref=ret.at[cls * q + s],
            send_sem=nsend.at[base + t], recv_sem=nrecv.at[cls * q + s], device_id={"ep": to * q + t})

    def near(cls):
        base = (inner * q, outer * q)[cls]

        def wait(i, c):
            arrived(base + (s + 1 + i) % q)
            return c

        lax.fori_loop(0, q - cls, wait, 0)
        block = pl.ds(base, q)
        got = hidden_rows(arr[block].reshape(q * cap, width), wg[...], wu[...])
        ybuf[block] = dot(got, wd[...]).astype(BF16).reshape(q, cap, width)
        if cls == 1:
            ret[q + s] = ybuf[base + s]
            near_send(1)

    def near_send(cls):
        base = (inner * q, outer * q)[cls]

        def send(i, c):
            near_return(base, cls, (s + 1 + i) % q).start()
            return c

        lax.fori_loop(0, q - cls, send, 0)

    def far_peer(i):
        k = (grp * q + s + i) % (2 * q)
        return k // q, k % q

    def inner_return(i):
        g, t = far_peer(i)
        return pltpu.make_async_remote_copy(
            src_ref=ybuf.at[2 * q + g * q + t], dst_ref=ret.at[3 * q + s],
            send_sem=fsend.at[g * q + t], recv_sem=frecv.at[s], device_id={"grp": g, "ep": layer * q + t})

    def outer_return(i, m):
        sel, g, t = i // (2 * q), *far_peer(i % (2 * q))
        cols = pl.ds(m * slab, slab)
        k = sel * 2 * q + g * q + t
        return pltpu.make_async_remote_copy(
            src_ref=ybuf.at[2 * q + k, :, cols], dst_ref=ret.at[2 * q + s, :, cols],
            send_sem=osend.at[k, m], recv_sem=orecv.at[s, m],
            device_id={"grp": g, "ep": (inner_l + sel * (outer_l - inner_l)) * q + t})

    def passed_return(i, m):
        g, t = far_peer(i)
        cols = pl.ds(m * slab, slab)
        return pltpu.make_async_remote_copy(
            src_ref=ybuf.at[6 * q + g * q + t, :, cols], dst_ref=ret.at[s, :, cols],
            send_sem=msend.at[g * q + t, m], recv_sem=mrecv.at[s, m],
            device_id={"grp": g, "ep": layer * q + t})

    def far_arrived(first, count):
        def wait(i, c):
            g, t = far_peer(i % (2 * q))
            arrived(first + (i // (2 * q)) * 2 * q + g * q + t)
            return c

        lax.fori_loop(1, count, wait, 0)

    def take(i):
        cross_copy(i).wait_recv()

        @pl.when(inner == 1)
        def _():
            relay_copy(i).start()

    @pl.when(is_a)
    def _():
        for i in range(len(chunks)):
            take(i)

    near(1)

    @pl.when(inner == 1)
    def _():
        near(0)

    @pl.when(par == 0)
    def _():
        @pl.when(inner == 0)
        def _():
            for i in range(len(chunks)):
                cross_copy(i).wait_recv()

        @pl.when(inner == 1)
        def _():
            near_send(0)

        far_arrived(2 * q, 2 * q)
        hid[:2 * q * cap] = hidden_rows(
            arr[2 * q:4 * q].reshape(2 * q * cap, width), fg[...], fu[...])
        got = dot(hid[:2 * q * cap], fd[...]).astype(BF16)
        ybuf[2 * q:4 * q] = got.reshape(2 * q, cap, width)

        def send(i, c):
            inner_return(i).start()
            return c

        lax.fori_loop(1, 2 * q, send, 0)
        ret[3 * q + s] = ybuf[2 * q + grp * q + s]

    def hand_on(i):
        inward_copy(i).wait_recv()
        onward_copy(i).start()

    @pl.when(is_b)
    def _():
        for i in range(ngu):
            hand_on(i)
            if i == ngu // 4:
                near_send(0)
        far_arrived(6 * q, 2 * q)
        nhid[...] = hidden_rows(arr[6 * q:].reshape(2 * q * cap, width), ng[...], nu[...])
        hand_on(ngu)
        for i in range(ngu):
            cross_copy(i).wait_recv()
        far_arrived(2 * q, 4 * q)
        hand_on(ngu + 1)
        hid[...] = hidden_rows(arr[2 * q:6 * q].reshape(4 * q * cap, width), fg[...], fu[...])
        for m in range(SLABS):
            cols = pl.ds(m * slab, slab)
            cross_copy(ngu + m).wait_recv()
            got = dot(hid[...], fd[:, cols]).astype(BF16)
            ybuf[2 * q:6 * q, :, cols] = got.reshape(4 * q, cap, slab)

            def send(i, c):
                outer_return(i, m).start()
                return c

            lax.fori_loop(1, 4 * q, send, 0)
            ret[2 * q + s, :, cols] = ybuf[2 * q + grp * q + s, :, cols]
            if m + 2 < SLABS:
                hand_on(ngu + m + 2)
            got = dot(nhid[...], nd[:, cols]).astype(BF16)
            ybuf[6 * q:, :, cols] = got.reshape(2 * q, cap, slab)

            def send_passed(i, c):
                passed_return(i, m).start()
                return c

            lax.fori_loop(1, 2 * q, send_passed, 0)
            ret[s, :, cols] = ybuf[6 * q + grp * q + s, :, cols]

    def near_back(cls):
        def wait(i, c):
            k = cls * q + (s + 1 + i) % q
            pltpu.make_async_remote_copy(
                src_ref=ybuf.at[0], dst_ref=ret.at[k], send_sem=nsend.at[0], recv_sem=nrecv.at[k],
                device_id={"ep": other_l * q + s}).wait_recv()
            return c

        lax.fori_loop(0, q - cls, wait, 0)

    def inner_back(i, c):
        t = (s + i) % q
        pltpu.make_async_remote_copy(
            src_ref=ybuf.at[0], dst_ref=ret.at[3 * q + t], send_sem=fsend.at[0], recv_sem=frecv.at[t],
            device_id={"ep": other_l * q + s}).wait_recv()
        return c

    def passed_back(m):
        cols = pl.ds(m * slab, slab)

        def wait(i, c):
            t = (s + i) % q
            pltpu.make_async_remote_copy(
                src_ref=ybuf.at[0, :, cols], dst_ref=ret.at[t, :, cols], send_sem=msend.at[0, m],
                recv_sem=mrecv.at[t, m], device_id={"ep": other_l * q + s}).wait_recv()
            return c

        lax.fori_loop(1, q, wait, 0)

        @pl.when(par == 0)
        def _():
            wait(0, 0)

    def outer_back(m):
        cols = pl.ds(m * slab, slab)

        def wait(i, c):
            t = (s + i) % q
            pltpu.make_async_remote_copy(
                src_ref=ybuf.at[0, :, cols], dst_ref=ret.at[2 * q + t, :, cols], send_sem=osend.at[0, m],
                recv_sem=orecv.at[t, m], device_id={"ep": other_l * q + s}).wait_recv()
            return c

        lax.fori_loop(1, q, wait, 0)

        @pl.when(jnp.logical_not(is_b))
        def _():
            wait(0, 0)

    def weighted(cls, cols):
        return dot(pick[cls], ret[cls * q:(cls + 1) * q, :, cols].reshape(q * cap, -1), ((0,), (0,)))

    near_back(1)
    acc[...] += weighted(1, slice(None))
    lax.fori_loop(1, q, inner_back, 0)

    @pl.when(par == 1)
    def _():
        inner_back(0, 0)

    acc[...] += weighted(3, slice(None))

    @pl.when(inner == 0)
    def _():
        near_back(0)

    for m in range(SLABS):
        @pl.when(inner == 1)
        def _():
            passed_back(m)

        outer_back(m)
        cols = slice(m * slab, (m + 1) * slab)
        out_ref[:, cols] = (acc[:, cols] + weighted(0, cols) + weighted(2, cols)).astype(BF16)

    for cls in range(4):
        def drain(i, c):
            dispatch_copy(cls, (s + 1 + i) % q).wait_send()
            return c

        lax.fori_loop(0, q - 1, drain, 0)
        if cls != 1:
            @pl.when(jnp.logical_not(at_home[cls]))
            def _():
                dispatch_copy(cls, s).wait_send()

    def drain_near(cls):
        base = (inner * q, outer * q)[cls]

        def drain(i, c):
            near_return(base, cls, (s + 1 + i) % q).wait_send()
            return c

        lax.fori_loop(0, q - cls, drain, 0)

    drain_near(1)

    @pl.when(inner == 1)
    def _():
        drain_near(0)

    @pl.when(is_a)
    def _():
        for i in range(len(chunks)):
            cross_copy(i).wait_send()
            relay_copy(i).wait_send()

    @pl.when(is_d)
    def _():
        for i in range(len(chunks)):
            inward_copy(i).wait_send()

    @pl.when(par == 0)
    def _():
        def drain_inner(i, c):
            inner_return(i).wait_send()
            return c

        lax.fori_loop(1, 2 * q, drain_inner, 0)

    @pl.when(is_b)
    def _():
        def drain_outer(i, c):
            for m in range(SLABS):
                outer_return(i, m).wait_send()
            return c

        def drain_passed(i, c):
            for m in range(SLABS):
                passed_return(i, m).wait_send()
            return c

        for i in range(len(chunks)):
            onward_copy(i).wait_send()
        lax.fori_loop(1, 2 * q, drain_passed, 0)

        lax.fori_loop(1, 4 * q, drain_outer, 0)


def on_layers(tokens, norm_gain, routes, route_weights, expert_gate, expert_up, expert_down,
              shared_gate, shared_up, shared_down):
    rows, width = tokens.shape
    n = lax.axis_size("ep")
    q = n // 4
    cap = -(-(5 * rows * routes.shape[1] // (4 * n)) // 8) * 8
    nchunk = 2 * PARTS + SLABS
    vmem = lambda shape, kind=BF16: pltpu.VMEM(shape, kind)
    sems = lambda *shape: pltpu.SemaphoreType.DMA(shape)
    anyspec = pl.BlockSpec(memory_space=pl.ANY)
    vspec = pl.BlockSpec(memory_space=pltpu.VMEM)
    ff = expert_gate.shape[2]
    return pl.pallas_call(
        functools.partial(layers_kernel, n, cap),
        out_shape=pltpu.VMEM((rows, width), BF16),
        in_specs=[anyspec, vspec, vspec, vspec] + [anyspec] * 6,
        out_specs=vspec,
        scratch_shapes=[
            vmem((rows, width)), vmem((rows, width)), vmem((128, rows), F32), vmem((128, rows), F32),
            vmem(expert_gate.shape[1:]), vmem(expert_up.shape[1:]), vmem(expert_down.shape[1:]),
            vmem(expert_gate.shape[1:]), vmem(expert_up.shape[1:]), vmem(expert_down.shape[1:]),
            vmem(expert_gate.shape[1:]), vmem(expert_up.shape[1:]), vmem(expert_down.shape[1:]),
            vmem(shared_gate.shape), vmem(shared_up.shape), vmem(shared_down.shape),
            vmem((n, cap, width)), vmem((8 * q, cap, width)), vmem((8 * q, cap, width)), vmem((n, cap, width)),
            vmem((rows, width), F32), vmem((4 * q * cap, ff)), vmem((2 * q * cap, ff)), vmem((4, q * cap, rows)),
            sems(7), sems(nchunk), sems(nchunk), sems(nchunk), sems(nchunk), sems(n), sems(8 * q),
            sems(2 * q), sems(2 * q), sems(2 * q), sems(q), sems(4 * q, SLABS), sems(q, SLABS),
            sems(2 * q, SLABS), sems(q, SLABS),
        ],
        compiler_params=pltpu.CompilerParams(
            collective_id=0, has_side_effects=True, vmem_limit_bytes=62 * 1024 * 1024 + 512 * 1024),
    )(tokens, norm_gain.reshape(1, width), routes.T, route_weights.T, expert_gate, expert_up,
      expert_down, shared_gate, shared_up, shared_down)


def on_device(*args):
    n, groups = lax.axis_size("ep"), lax.axis_size("grp")
    if groups == 2 and n % 8 == 0 and n <= 32:
        return on_layers(*args)
    return on_halves(*args)


def solution(mesh):
    return jax.shard_map(
        on_device,
        mesh=mesh,
        in_specs=(
            P(("grp", "ep"), None),
            P(),
            P(("grp", "ep"), None),
            P(("grp", "ep"), None),
            P("ep", None, None),
            P("ep", None, None),
            P("ep", None, None),
            P(),
            P(),
            P(),
        ),
        out_specs=P(("grp", "ep"), None),
        check_vma=False,
    )
```

```python
import functools

import jax
import jax.numpy as jnp
from jax import lax
from jax.experimental import pallas as pl
from jax.experimental.pallas import tpu as pltpu
from jax.sharding import PartitionSpec as P

BF16 = jnp.bfloat16
F32 = jnp.float32
PIECES = 2
SLABS = 4
PARTS = 8
STRIPS = 8
LAG = 3


def dot(a, b, dims=((1,), (0,))):
    return lax.dot_general(a, b, (dims, ((), ())), preferred_element_type=F32)


def hidden_rows(rows, w_gate, w_up):
    gate_part = dot(rows, w_gate)
    up_part = dot(rows, w_up)
    return (gate_part / (1.0 + jnp.exp(-gate_part)) * up_part).astype(BF16)


def halves_kernel(
    n, groups, cap,
    tokens_hbm, gain_ref, routes_ref, rw_ref, eg_hbm, eu_hbm, ed_hbm, sg_hbm, su_hbm, sd_hbm,
    out_ref,
    tok, normed, place, scale, wg, wu, wd, fg, fu, fd, sg, su, sd, obuf, arr, ybuf, ret, acc, hid, pick,
    load_sem, wsend, wrecv, xsend, xrecv, dsend, drecv, rsend, rrecv,
):
    half = n // 2
    me = lax.axis_index("ep")
    grp = lax.axis_index("grp")
    base = (me // half) * half
    mine = me % half
    far = (base + half) % n + (mine + half // 2) % half
    rows = tok.shape[0]
    width = tok.shape[1]

    def peer(j):
        total, bit = 0, 1
        while bit < half:
            total = total + bit * (((mine // bit) % 2 + (j // bit) % 2) % 2)
            bit *= 2
        return total

    capp = ret.shape[2]
    if capp > cap:
        low = cap // 16 * 16
        ret[:, :, low:, :] = jnp.zeros((2, half, capp - low, width), BF16)
    barrier = pltpu.get_barrier_semaphore()

    def greet(i, c):
        pl.semaphore_signal(barrier, inc=1, device_id={"ep": base + peer(i)})
        return c

    lax.fori_loop(1, half, greet, 0)
    pl.semaphore_signal(barrier, inc=1, device_id={"ep": far})
    for k in range(1, groups):
        pl.semaphore_signal(barrier, inc=1, device_id={"grp": (grp + k) % groups})

    loads = [(tokens_hbm, tok), (eg_hbm.at[0], wg), (eu_hbm.at[0], wu), (ed_hbm.at[0], wd),
             (sg_hbm, sg), (su_hbm, su), (sd_hbm, sd)]
    loads = [pltpu.make_async_copy(a, b, load_sem.at[i]) for i, (a, b) in enumerate(loads)]
    loads[0].start()

    slab = width // SLABS

    def region(group, a, piece):
        depth = (fg, fu, fd)[a].shape[0] // groups
        if a == 2:
            return pl.ds(pl.multiple_of(group * depth, depth), depth), pl.ds(piece * slab, slab)
        depth = depth // PIECES
        start = (group * PIECES + piece) * depth
        return pl.ds(pl.multiple_of(start, depth), depth), pl.ds(0, fg.shape[1])

    chunks = [(a, piece) for piece in range(PIECES) for a in range(2)]
    chunks += [(2, piece) for piece in range(SLABS)]

    def weight_copy(a, piece):
        src, dst = ((eg_hbm, fg), (eu_hbm, fu), (ed_hbm, fd))[a]
        at, i = region(grp, a, piece), chunks.index((a, piece))
        return pltpu.make_async_remote_copy(
            src_ref=src.at[0, at[0], at[1]], dst_ref=dst.at[at[0], at[1]],
            send_sem=wsend.at[i], recv_sem=wrecv.at[i], device_id={"ep": far})

    def forward_copy(a, piece, k):
        dst = (fg, fu, fd)[a]
        at = region(grp, a, piece)
        i = chunks.index((a, piece)) * max(1, groups - 1) + k - 1
        return pltpu.make_async_remote_copy(
            src_ref=dst.at[at[0], at[1]], dst_ref=dst.at[at[0], at[1]],
            send_sem=xsend.at[i], recv_sem=xrecv.at[i],
            device_id={"grp": (grp + k) % groups})

    pl.semaphore_wait(barrier, half - 1 + 1 + groups - 1)
    weight_copy(*chunks[0]).start()

    lane = lax.broadcasted_iota(jnp.int32, (rows, 128), 1)
    chosen = jnp.zeros((rows, 128), F32)
    weight = jnp.zeros((rows, 128), F32)
    for k in range(routes_ref.shape[1]):
        hit = lane == routes_ref[:, k:k + 1]
        chosen = chosen + jnp.where(hit, 1.0, 0.0)
        weight = weight + jnp.where(hit, rw_ref[:, k:k + 1], 0.0)
    chosen_t = chosen.T
    earlier = (lax.broadcasted_iota(jnp.int32, (rows, rows), 0)
               < lax.broadcasted_iota(jnp.int32, (rows, rows), 1))
    before = dot(chosen_t.astype(BF16), jnp.where(earlier, 1.0, 0.0).astype(BF16))
    place[...] = jnp.where(chosen_t > 0.5, before, -1.0)
    scale[...] = weight.T

    loads[0].wait()
    for copy in loads[1:]:
        copy.start()

    def norm_step(i, c):
        at = pl.ds(pl.multiple_of(i * 32, 32), 32)
        x = tok[at, :].astype(F32)
        factor = lax.rsqrt(jnp.mean(x * x, axis=-1, keepdims=True) + 1e-06)
        normed[at, :] = (x * factor * gain_ref[...]).astype(BF16)
        return c

    lax.fori_loop(0, rows // 32, norm_step, 0)
    slot = lax.broadcasted_iota(jnp.int32, (capp, rows), 0).astype(F32)
    slot = jnp.where(slot < cap, slot, -2.0)

    def gather(p):
        ours = slot == place[pl.ds(base + p, 1), :]
        theirs = slot == place[pl.ds((base + half) % n + (p + half // 2) % half, 1), :]
        want = jnp.concatenate([jnp.where(ours, 1.0, 0.0), jnp.where(theirs, 1.0, 0.0)], axis=0)
        got = dot(want.astype(BF16), normed[...])
        return got[:capp].astype(BF16), got[capp:].astype(BF16)

    used = pl.ds(0, cap)

    def dispatch_copy(p):
        return pltpu.make_async_remote_copy(
            src_ref=obuf.at[:, p, used], dst_ref=arr.at[:, mine, used],
            send_sem=dsend.at[p], recv_sem=drecv.at[mine], device_id={"ep": base + p})

    def dispatch_wait(p):
        pltpu.make_async_remote_copy(
            src_ref=obuf.at[:, p, used], dst_ref=arr.at[:, p, used],
            send_sem=dsend.at[p], recv_sem=drecv.at[p], device_id={"ep": base + p}).wait_recv()

    def message(ref, p, m):
        if m == 0:
            return ref.at[0, p, used]
        return ref.at[1, p, used, pl.ds((m - 1) * slab, slab)]

    def return_copy(p, m):
        return pltpu.make_async_remote_copy(
            src_ref=message(ybuf, p, m), dst_ref=message(ret, mine, m),
            send_sem=rsend.at[p, m], recv_sem=rrecv.at[mine, m], device_id={"ep": base + p})

    def return_wait(p, m):
        pltpu.make_async_remote_copy(
            src_ref=message(ybuf, p, m), dst_ref=message(ret, p, m),
            send_sem=rsend.at[p, m], recv_sem=rrecv.at[p, m],
            device_id={"ep": base + p}).wait_recv()

    def dispatch_step(i, c):
        p = peer(half - 1 - i)
        first, second = gather(p)
        obuf[0, p] = first
        obuf[1, p] = second
        dispatch_copy(p).start()
        return c

    lax.fori_loop(0, half - 1, dispatch_step, 0)
    for a, piece in chunks[1:-SLABS]:
        weight_copy(a, piece).start()
    first, second = gather(mine)
    arr[0, mine] = first
    arr[1, mine] = second

    for copy in loads[4:]:
        copy.wait()
    acc[...] = dot(hidden_rows(normed[...], sg[...], su[...]), sd[...])
    for copy in loads[1:4]:
        copy.wait()

    for b in range(2):
        for p in range(half):
            at = pl.ds((base + b * half) % n + (p + b * (half // 2)) % half, 1)
            want = jnp.where(slot == place[at, :], scale[at, :], 0.0)
            pick[b, p * capp:(p + 1) * capp, :] = want.astype(BF16)

    def own_step(i, c):
        p = peer((i + half // 2 - 1) % (half - 1) + 1)
        dispatch_wait(p)
        ybuf[0, p] = dot(hidden_rows(arr[0, p], wg[...], wu[...]), wd[...]).astype(BF16)
        return_copy(p, 0).start()
        return c

    def forward(a, piece):
        weight_copy(a, piece).wait_recv()
        for k in range(1, groups):
            forward_copy(a, piece, k).start()

    def forwarded(a, piece):
        for k in range(1, groups):
            forward_copy(a, piece, k).wait_recv()

    early = chunks[:-SLABS]
    done = 0
    for i, (a, piece) in enumerate(early):
        until = (half - 1) * (i + 1) // len(early)
        lax.fori_loop(done, until, own_step, 0)
        done = until
        forward(a, piece)
        weight_copy(*chunks[len(early) + i]).start()
    own = dot(hidden_rows(arr[0, mine], wg[...], wu[...]), wd[...]).astype(BF16)
    ret[0, mine] = own

    for a, piece in early:
        forwarded(a, piece)
    hid[...] = hidden_rows(arr[1].reshape(half * capp, width), fg[...], fu[...])

    def far_slab(c):
        forwarded(2, c)
        cols = pl.ds(c * slab, slab)
        got = dot(hid[...], fd[:, cols]).astype(BF16)
        ybuf[1, :, :, cols] = got.reshape(half, capp, slab)

        def send(i, k):
            return_copy(peer(half - 1 - i), 1 + c).start()
            return k

        lax.fori_loop(0, half - 1, send, 0)
        ret[1, mine, :, cols] = ybuf[1, mine, :, cols]

    for c in range(SLABS):
        forward(2, c)
        if c > 0:
            far_slab(c - 1)
    far_slab(SLABS - 1)

    def arrive(m):
        def step(i, k):
            return_wait(peer(i + 1), m)
            return k

        lax.fori_loop(0, half - 1, step, 0)

    arrive(0)
    acc[...] += dot(pick[0], ret[0].reshape(half * capp, width), ((0,), (0,)))
    for c in range(SLABS):
        arrive(1 + c)
        cols = pl.ds(c * slab, slab)
        total = acc[:, cols] + dot(
            pick[1], ret[1, :, :, cols].reshape(half * capp, slab), ((0,), (0,)))
        out_ref[:, cols] = total.astype(BF16)

    def drain(i, c):
        p = peer(half - 1 - i)
        dispatch_copy(p).wait_send()
        for m in range(1 + SLABS):
            return_copy(p, m).wait_send()
        return c

    lax.fori_loop(0, half - 1, drain, 0)
    for a, piece in chunks:
        weight_copy(a, piece).wait_send()
        for k in range(1, groups):
            forward_copy(a, piece, k).wait_send()


def on_halves(tokens, norm_gain, routes, route_weights, expert_gate, expert_up, expert_down,
              shared_gate, shared_up, shared_down):
    rows, width = tokens.shape
    n, groups = lax.axis_size("ep"), lax.axis_size("grp")
    half = n // 2
    cap = -(-(5 * rows * routes.shape[1] // (4 * n)) // 8) * 8
    nchunk = 2 * PIECES + SLABS
    nfwd = nchunk * max(1, groups - 1)
    vmem = lambda shape, kind=BF16: pltpu.VMEM(shape, kind)
    anyspec = pl.BlockSpec(memory_space=pl.ANY)
    vspec = pl.BlockSpec(memory_space=pltpu.VMEM)
    capp = cap
    block = (2, half, capp, width)
    return pl.pallas_call(
        functools.partial(halves_kernel, n, groups, cap),
        out_shape=jax.ShapeDtypeStruct((rows, width), BF16),
        in_specs=[anyspec, vspec, vspec, vspec] + [anyspec] * 6,
        out_specs=vspec,
        scratch_shapes=[
            vmem((rows, width)), vmem((rows, width)), vmem((128, rows), F32), vmem((128, rows), F32),
            vmem(expert_gate.shape[1:]), vmem(expert_up.shape[1:]), vmem(expert_down.shape[1:]),
            vmem(expert_gate.shape[1:]), vmem(expert_up.shape[1:]), vmem(expert_down.shape[1:]),
            vmem(shared_gate.shape), vmem(shared_up.shape), vmem(shared_down.shape),
            vmem(block), vmem(block), vmem(block), vmem(block), vmem((rows, width), F32),
            vmem((half * capp, expert_gate.shape[2])), vmem((2, half * capp, rows)),
            pltpu.SemaphoreType.DMA((7,)),
            pltpu.SemaphoreType.DMA((nchunk,)), pltpu.SemaphoreType.DMA((nchunk,)),
            pltpu.SemaphoreType.DMA((nfwd,)), pltpu.SemaphoreType.DMA((nfwd,)),
            pltpu.SemaphoreType.DMA((half,)), pltpu.SemaphoreType.DMA((half,)),
            pltpu.SemaphoreType.DMA((half, 1 + SLABS)), pltpu.SemaphoreType.DMA((half, 1 + SLABS)),
        ],
        compiler_params=pltpu.CompilerParams(
            collective_id=0, has_side_effects=True, vmem_limit_bytes=60 * 1024 * 1024),
    )(tokens, norm_gain.reshape(1, width), routes, route_weights, expert_gate, expert_up,
      expert_down, shared_gate, shared_up, shared_down)


def layers_kernel(
    n, cap,
    tokens_hbm, gain_ref, routes_ref, rw_ref, eg_hbm, eu_hbm, ed_hbm, sg_hbm, su_hbm, sd_hbm,
    out_ref,
    tok, normed, place, scale, wg, wu, wd, fgu, fd, pgu, pd, sg, su, sd, obuf, arr, ybuf, ret, acc, hid, phid, pick,
    load_sem, sent, wsent, landed, wrecv, precv, orecv, mrecv,
):
    q = n // 4
    me = lax.axis_index("ep")
    grp = lax.axis_index("grp")
    layer, s = me // q, me % q
    side = layer // 2
    inner = (layer % 3 + 1) // 2
    outer = 1 - inner
    inner_l, outer_l = 1 + side, 3 * side
    other_l = inner_l + outer_l - layer
    far_in, far_out = 2 - side, 3 - 3 * side
    par = (grp + s) % 2
    rows, width = tok.shape
    is_a = (inner == 1) & (par == 0)
    is_b = (inner == 1) & (par == 1)
    is_c = (inner == 0) & (par == 0)
    is_d = (inner == 0) & (par == 1)

    barrier = pltpu.get_barrier_semaphore()

    def greet(i, c):
        k = (grp * 2 * q + me % (2 * q) + i) % (4 * q)
        pl.semaphore_signal(barrier, inc=1, device_id={"grp": k // (2 * q), "ep": side * 2 * q + k % (2 * q)})
        return c

    lax.fori_loop(1, 4 * q, greet, 0)

    @pl.when(inner == 1)
    def _():
        pl.semaphore_signal(barrier, inc=1, device_id={"ep": far_in * q + s})

    loads = [(tokens_hbm, tok), (eg_hbm.at[0], wg), (eu_hbm.at[0], wu), (ed_hbm.at[0], wd),
             (sg_hbm, sg), (su_hbm, su), (sd_hbm, sd)]
    loads = [pltpu.make_async_copy(a, b, load_sem.at[i]) for i, (a, b) in enumerate(loads)]
    for copy in loads:
        copy.start()

    strip = width // STRIPS
    depth = fgu.shape[1] // PARTS

    def chunk_copies(i, srcs, dsts, sem, recv, to):
        if i < PARTS:
            at = pl.ds(i * depth, depth)
            pairs = [(srcs[a].at[at], dsts[a].at[at], sem + a) for a in range(2)]
        else:
            at = pl.ds((i - PARTS) * strip, strip)
            pairs = [(srcs[2].at[:, at], dsts[2].at[:, at], sem + 2)]
        return [pltpu.make_async_remote_copy(
            src_ref=a, dst_ref=b, send_sem=wsent.at[k], recv_sem=recv.at[i], device_id={"ep": to * q + s})
            for a, b, k in pairs]

    own = (eg_hbm.at[0], eu_hbm.at[0], ed_hbm.at[0])
    far = (fgu.at[0], fgu.at[1], fd)
    passed = (pgu.at[0], pgu.at[1], pd)
    nchunk = PARTS + STRIPS

    def cross(i):
        return chunk_copies(i, own, far, 0, wrecv, far_in)

    def relay(i):
        return chunk_copies(i, far, far, 3, wrecv, outer_l)

    def inward(i):
        return chunk_copies(i, own, passed, 0, precv, inner_l)

    def onward(i):
        return chunk_copies(i, passed, far, 3, wrecv, far_in)

    def start(copies):
        for copy in copies:
            copy.start()

    def remote(ref, sem):
        return pltpu.make_async_remote_copy(
            src_ref=ref, dst_ref=ref, send_sem=sem, recv_sem=sem, device_id={"ep": other_l * q + s})

    def chunk_landed(i, gu, down, recv):
        if i < PARTS:
            remote(gu.at[:, pl.ds(i * depth, depth)], recv.at[i]).wait_recv()
        else:
            remote(down.at[:, pl.ds((i - PARTS) * strip, strip)], recv.at[i]).wait_recv()

    def weights_sent(srcs, k):
        for a in range(3):
            remote(srcs[a], wsent.at[k + a]).wait_send()

    expert = lax.broadcasted_iota(jnp.int32, (128, rows), 0)
    chosen = jnp.zeros((128, rows), F32)
    weight = jnp.zeros((128, rows), F32)
    for k in range(routes_ref.shape[0]):
        hit = expert == routes_ref[k:k + 1, :]
        chosen = chosen + jnp.where(hit, 1.0, 0.0)
        weight = weight + jnp.where(hit, rw_ref[k:k + 1, :], 0.0)
    earlier = (lax.broadcasted_iota(jnp.int32, (rows, rows), 0)
               < lax.broadcasted_iota(jnp.int32, (rows, rows), 1))
    before = dot(chosen.astype(BF16), jnp.where(earlier, 1.0, 0.0).astype(BF16))
    place[...] = jnp.where(chosen > 0.5, before, -1.0)
    scale[...] = weight

    loads[0].wait()

    def norm_step(i, c):
        at = pl.ds(pl.multiple_of(i * 32, 32), 32)
        x = tok[at, :].astype(F32)
        factor = lax.rsqrt(jnp.mean(x * x, axis=-1, keepdims=True) + 1e-06)
        normed[at, :] = (x * factor * gain_ref[...]).astype(BF16)
        return c

    lax.fori_loop(0, rows // 32, norm_step, 0)
    slot = lax.broadcasted_iota(jnp.int32, (cap, rows), 0).astype(F32)

    class_layer = (other_l, layer, far_out, far_in)
    near_at = outer * q + s
    land_at = (outer * near_at + inner * (6 * q + grp * q + s), near_at,
               2 * q + outer * 2 * q + grp * q + s, 2 * q + grp * q + s)
    land_on = (outer + inner * 4, 0, 3, 2)
    at_home = (is_b, inner < 2, is_b, par == 0)

    def host(cls, t):
        if cls == 0:
            return outer * grp + inner * ((t + 1) % 2), inner_l * q + t
        if cls == 1:
            return grp, layer * q + t
        if cls == 2:
            return (t + 1) % 2, inner_l * q + t
        return t % 2, layer * q + t

    def dispatch_copy(cls, t):
        hg, he = host(cls, t)
        return pltpu.make_async_remote_copy(
            src_ref=obuf.at[cls * q + t], dst_ref=arr.at[land_at[cls]],
            send_sem=sent.at[0], recv_sem=landed.at[land_on[cls]], device_id={"grp": hg, "ep": he})

    def one_hot(cls, values):
        at = [pl.ds(class_layer[cls] * q + t, 1) for t in range(q)]
        return jnp.concatenate([jnp.where(slot == place[a, :], values(a), 0.0) for a in at], axis=0)

    def gather(cls):
        got = dot(one_hot(cls, lambda a: 1.0).astype(BF16), normed[...]).astype(BF16)
        obuf[cls * q:(cls + 1) * q] = got.reshape(q, cap, width)

    def dispatch(cls):
        def send(i, c):
            dispatch_copy(cls, (s + 1 + i) % q).start()
            return c

        lax.fori_loop(0, q - 1, send, 0)

        @pl.when(at_home[cls])
        def _():
            arr[land_at[cls]] = obuf[cls * q + s]

        if cls != 1:
            @pl.when(jnp.logical_not(at_home[cls]))
            def _():
                dispatch_copy(cls, s).start()

    gather(1)
    gather(0)
    pl.semaphore_wait(barrier, 4 * q - 1 + inner)

    @pl.when(is_a)
    def _():
        for i in range(nchunk):
            start(cross(i))

    @pl.when(inner == 0)
    def _():
        dispatch(0)

    dispatch(1)

    @pl.when(inner == 1)
    def _():
        dispatch(0)

    @pl.when(is_d)
    def _():
        for i in range(PARTS):
            start(inward(i))

    gather(3)
    dispatch(3)
    gather(2)
    dispatch(2)

    @pl.when(is_d)
    def _():
        for i in range(PARTS, nchunk):
            start(inward(i))

    for cls in range(4):
        pick[cls] = one_hot(cls, lambda a: scale[a, :]).T.astype(BF16)
    for copy in loads[4:]:
        copy.wait()
    acc[...] = dot(hidden_rows(normed[...], sg[...], su[...]), sd[...])
    for copy in loads[1:4]:
        copy.wait()

    def near_return(base, cls, t):
        to = (other_l, layer)[cls]
        return pltpu.make_async_remote_copy(
            src_ref=ybuf.at[base + t], dst_ref=ret.at[cls * q + s],
            send_sem=sent.at[1], recv_sem=landed.at[5 + cls], device_id={"ep": to * q + t})

    def near(cls):
        base = (inner * q, outer * q)[cls]
        remote(arr.at[pl.ds(0, q - cls)], landed.at[1 - cls]).wait_recv()
        block = pl.ds(base, q)
        got = hidden_rows(arr[block].reshape(q * cap, width), wg[...], wu[...])
        ybuf[block] = dot(got, wd[...]).astype(BF16).reshape(q, cap, width)
        if cls == 1:
            ret[q + s] = ybuf[base + s]
            near_send(1)

    def near_send(cls):
        base = (inner * q, outer * q)[cls]

        def send(i, c):
            near_return(base, cls, (s + 1 + i) % q).start()
            return c

        lax.fori_loop(0, q - cls, send, 0)

    def far_peer(i):
        k = (grp * q + s + i) % (2 * q)
        return k // q, k % q

    def inner_return(i):
        g, t = far_peer(i)
        return pltpu.make_async_remote_copy(
            src_ref=ybuf.at[2 * q + g * q + t], dst_ref=ret.at[3 * q + s],
            send_sem=sent.at[2], recv_sem=landed.at[7], device_id={"grp": g, "ep": layer * q + t})

    def outer_return(i, m):
        sel, g, t = i // (2 * q), *far_peer(i % (2 * q))
        cols = pl.ds(m * strip, strip)
        k = sel * 2 * q + g * q + t
        return pltpu.make_async_remote_copy(
            src_ref=ybuf.at[2 * q + k, :, cols], dst_ref=ret.at[2 * q + s, :, cols],
            send_sem=sent.at[3], recv_sem=orecv.at[m],
            device_id={"grp": g, "ep": (inner_l + sel * (outer_l - inner_l)) * q + t})

    def passed_return(i, m):
        g, t = far_peer(i)
        cols = pl.ds(m * strip, strip)
        return pltpu.make_async_remote_copy(
            src_ref=ybuf.at[6 * q + g * q + t, :, cols], dst_ref=ret.at[s, :, cols],
            send_sem=sent.at[4], recv_sem=mrecv.at[m], device_id={"grp": g, "ep": layer * q + t})

    def far_arrived(count, k):
        remote(arr.at[pl.ds(0, count)], landed.at[k]).wait_recv()

    def hand_on(i):
        chunk_landed(i, pgu, pd, precv)
        start(onward(i))

    @pl.when(is_a)
    def _():
        for i in range(nchunk):
            chunk_landed(i, fgu, fd, wrecv)
            start(relay(i))

    @pl.when(is_b)
    def _():
        hand_on(0)

    near(1)

    @pl.when(inner == 1)
    def _():
        near(0)

    @pl.when(par == 0)
    def _():
        @pl.when(inner == 0)
        def _():
            for i in range(nchunk):
                chunk_landed(i, fgu, fd, wrecv)

        @pl.when(inner == 1)
        def _():
            near_send(0)

        far_arrived(2 * q - 1, 2)
        hid[:2 * q * cap] = hidden_rows(
            arr[2 * q:4 * q].reshape(2 * q * cap, width), fgu[0], fgu[1])
        got = dot(hid[:2 * q * cap], fd[...]).astype(BF16)
        ybuf[2 * q:4 * q] = got.reshape(2 * q, cap, width)

        def send(i, c):
            inner_return(i).start()
            return c

        lax.fori_loop(1, 2 * q, send, 0)
        ret[3 * q + s] = ybuf[2 * q + grp * q + s]

    def passed_strip(m):
        cols = pl.ds(m * strip, strip)
        got = dot(phid[...], pd[:, cols]).astype(BF16)
        ybuf[6 * q:, :, cols] = got.reshape(2 * q, cap, strip)

        def send(i, c):
            passed_return(i, m).start()
            return c

        lax.fori_loop(1, 2 * q, send, 0)
        ret[s, :, cols] = ybuf[6 * q + grp * q + s, :, cols]

    def outer_strip(m):
        cols = pl.ds(m * strip, strip)
        chunk_landed(PARTS + m, fgu, fd, wrecv)
        got = dot(hid[...], fd[:, cols]).astype(BF16)
        ybuf[2 * q:6 * q, :, cols] = got.reshape(4 * q, cap, strip)

        def send(i, c):
            outer_return(4 * q - i, m).start()
            return c

        lax.fori_loop(1, 4 * q, send, 0)
        ret[2 * q + s, :, cols] = ybuf[2 * q + grp * q + s, :, cols]

    @pl.when(is_b)
    def _():
        for i in range(1, PARTS):
            hand_on(i)
            if i == PARTS // 2:
                near_send(0)
        far_arrived(2 * q - 1, 4)
        phid[...] = hidden_rows(arr[6 * q:].reshape(2 * q * cap, width), pgu[0], pgu[1])
        for i in range(PARTS):
            chunk_landed(i, fgu, fd, wrecv)
        far_arrived(4 * q - 1, 3)
        hid[...] = hidden_rows(arr[2 * q:6 * q].reshape(4 * q * cap, width), fgu[0], fgu[1])
        for m in range(STRIPS + LAG):
            if m < STRIPS:
                hand_on(PARTS + m)
                passed_strip(m)
            if m >= LAG:
                outer_strip(m - LAG)

    def back(k, home):
        remote(ret.at[pl.ds(0, q - home)], landed.at[k]).wait_recv()

    def strip_back(at, sem, m, home):
        remote(ret.at[pl.ds(at, q - home), :, pl.ds(m * strip, strip)], sem.at[m]).wait_recv()

    def weighted(cls, cols):
        return dot(pick[cls], ret[cls * q:(cls + 1) * q, :, cols].reshape(q * cap, -1))

    back(6, 1)
    acc[...] += weighted(1, slice(None))

    @pl.when(par == 0)
    def _():
        back(7, 1)

    @pl.when(par == 1)
    def _():
        back(7, 0)

    acc[...] += weighted(3, slice(None))

    @pl.when(inner == 0)
    def _():
        back(5, 0)

    for m in range(STRIPS):
        @pl.when(is_b)
        def _():
            strip_back(0, mrecv, m, 1)
            strip_back(2 * q, orecv, m, 1)

        @pl.when(is_a)
        def _():
            strip_back(0, mrecv, m, 0)

        @pl.when(jnp.logical_not(is_b))
        def _():
            strip_back(2 * q, orecv, m, 0)

        cols = slice(m * strip, (m + 1) * strip)
        out_ref[:, cols] = (acc[:, cols] + weighted(0, cols) + weighted(2, cols)).astype(BF16)

    def drain(ref, count, k):
        remote(ref.at[pl.ds(0, count)], sent.at[k]).wait_send()

    @pl.when(is_a)
    def _():
        drain(obuf, 4 * q - 2, 0)
        drain(ybuf, 2 * q - 1, 1)
        drain(ybuf, 2 * q - 1, 2)
        weights_sent(own, 0)
        weights_sent(far, 3)

    @pl.when(is_b)
    def _():
        drain(obuf, 4 * q - 3, 0)
        drain(ybuf, 2 * q - 1, 1)
        drain(ybuf, 4 * q - 1, 3)
        drain(ybuf, 2 * q - 1, 4)
        weights_sent(passed, 3)

    @pl.when(is_c)
    def _():
        drain(obuf, 4 * q - 2, 0)
        drain(ybuf, q - 1, 1)
        drain(ybuf, 2 * q - 1, 2)

    @pl.when(is_d)
    def _():
        drain(obuf, 4 * q - 1, 0)
        drain(ybuf, q - 1, 1)
        weights_sent(own, 0)


def on_layers(tokens, norm_gain, routes, route_weights, expert_gate, expert_up, expert_down,
              shared_gate, shared_up, shared_down):
    rows, width = tokens.shape
    n = lax.axis_size("ep")
    q = n // 4
    cap = -(-(5 * rows * routes.shape[1] // (4 * n)) // 8) * 8
    vmem = lambda shape, kind=BF16: pltpu.VMEM(shape, kind)
    sems = lambda *shape: pltpu.SemaphoreType.DMA(shape)
    anyspec = pl.BlockSpec(memory_space=pl.ANY)
    vspec = pl.BlockSpec(memory_space=pltpu.VMEM)
    ff = expert_gate.shape[2]
    both = (2,) + expert_gate.shape[1:]
    return pl.pallas_call(
        functools.partial(layers_kernel, n, cap),
        out_shape=pltpu.VMEM((rows, width), BF16),
        in_specs=[anyspec, vspec, vspec, vspec] + [anyspec] * 6,
        out_specs=vspec,
        scratch_shapes=[
            vmem((rows, width)), vmem((rows, width)), vmem((128, rows), F32), vmem((128, rows), F32),
            vmem(expert_gate.shape[1:]), vmem(expert_up.shape[1:]), vmem(expert_down.shape[1:]),
            vmem(both), vmem(expert_down.shape[1:]), vmem(both), vmem(expert_down.shape[1:]),
            vmem(shared_gate.shape), vmem(shared_up.shape), vmem(shared_down.shape),
            vmem((n, cap, width)), vmem((8 * q, cap, width)), vmem((8 * q, cap, width)), vmem((n, cap, width)),
            vmem((rows, width), F32), vmem((4 * q * cap, ff)), vmem((2 * q * cap, ff)), vmem((4, rows, q * cap)),
            sems(7), sems(5), sems(6), sems(8), sems(PARTS + STRIPS), sems(PARTS + STRIPS),
            sems(STRIPS), sems(STRIPS),
        ],
        compiler_params=pltpu.CompilerParams(
            collective_id=0, has_side_effects=True, vmem_limit_bytes=62 * 1024 * 1024 + 512 * 1024),
    )(tokens, norm_gain.reshape(1, width), routes.T, route_weights.T, expert_gate, expert_up,
      expert_down, shared_gate, shared_up, shared_down)


def on_device(*args):
    n, groups = lax.axis_size("ep"), lax.axis_size("grp")
    if groups == 2 and n % 8 == 0 and n <= 32:
        return on_layers(*args)
    return on_halves(*args)


def solution(mesh):
    return jax.shard_map(
        on_device,
        mesh=mesh,
        in_specs=(
            P(("grp", "ep"), None),
            P(),
            P(("grp", "ep"), None),
            P(("grp", "ep"), None),
            P("ep", None, None),
            P("ep", None, None),
            P("ep", None, None),
            P(),
            P(),
            P(),
        ),
        out_specs=P(("grp", "ep"), None),
        check_vma=False,
    )
```

```python
import functools

import jax
import jax.numpy as jnp
from jax import lax
from jax.experimental import pallas as pl
from jax.experimental.pallas import tpu as pltpu
from jax.sharding import PartitionSpec as P

BF16 = jnp.bfloat16
F32 = jnp.float32
PIECES = 2
SLABS = 4
PARTS = 8
STRIPS = 8
GROUPS = tuple((i, 1) for i in range(STRIPS))


def dot(a, b, dims=((1,), (0,))):
    return lax.dot_general(a, b, (dims, ((), ())), preferred_element_type=F32)


def hidden_rows(rows, w_gate, w_up):
    gate_part = dot(rows, w_gate)
    up_part = dot(rows, w_up)
    return (gate_part / (1.0 + jnp.exp(-gate_part)) * up_part).astype(BF16)


def halves_kernel(
    n, groups, cap,
    tokens_hbm, gain_ref, routes_ref, rw_ref, eg_hbm, eu_hbm, ed_hbm, sg_hbm, su_hbm, sd_hbm,
    out_ref,
    tok, normed, place, scale, wg, wu, wd, fg, fu, fd, sg, su, sd, obuf, arr, ybuf, ret, acc, hid, pick,
    load_sem, wsend, wrecv, xsend, xrecv, dsend, drecv, rsend, rrecv,
):
    half = n // 2
    me = lax.axis_index("ep")
    grp = lax.axis_index("grp")
    base = (me // half) * half
    mine = me % half
    far = (base + half) % n + (mine + half // 2) % half
    rows = tok.shape[0]
    width = tok.shape[1]

    def peer(j):
        total, bit = 0, 1
        while bit < half:
            total = total + bit * (((mine // bit) % 2 + (j // bit) % 2) % 2)
            bit *= 2
        return total

    capp = ret.shape[2]
    if capp > cap:
        low = cap // 16 * 16
        ret[:, :, low:, :] = jnp.zeros((2, half, capp - low, width), BF16)
    barrier = pltpu.get_barrier_semaphore()

    def greet(i, c):
        pl.semaphore_signal(barrier, inc=1, device_id={"ep": base + peer(i)})
        return c

    lax.fori_loop(1, half, greet, 0)
    pl.semaphore_signal(barrier, inc=1, device_id={"ep": far})
    for k in range(1, groups):
        pl.semaphore_signal(barrier, inc=1, device_id={"grp": (grp + k) % groups})

    loads = [(tokens_hbm, tok), (eg_hbm.at[0], wg), (eu_hbm.at[0], wu), (ed_hbm.at[0], wd),
             (sg_hbm, sg), (su_hbm, su), (sd_hbm, sd)]
    loads = [pltpu.make_async_copy(a, b, load_sem.at[i]) for i, (a, b) in enumerate(loads)]
    loads[0].start()

    slab = width // SLABS

    def region(group, a, piece):
        depth = (fg, fu, fd)[a].shape[0] // groups
        if a == 2:
            return pl.ds(pl.multiple_of(group * depth, depth), depth), pl.ds(piece * slab, slab)
        depth = depth // PIECES
        start = (group * PIECES + piece) * depth
        return pl.ds(pl.multiple_of(start, depth), depth), pl.ds(0, fg.shape[1])

    chunks = [(a, piece) for piece in range(PIECES) for a in range(2)]
    chunks += [(2, piece) for piece in range(SLABS)]

    def weight_copy(a, piece):
        src, dst = ((eg_hbm, fg), (eu_hbm, fu), (ed_hbm, fd))[a]
        at, i = region(grp, a, piece), chunks.index((a, piece))
        return pltpu.make_async_remote_copy(
            src_ref=src.at[0, at[0], at[1]], dst_ref=dst.at[at[0], at[1]],
            send_sem=wsend.at[i], recv_sem=wrecv.at[i], device_id={"ep": far})

    def forward_copy(a, piece, k):
        dst = (fg, fu, fd)[a]
        at = region(grp, a, piece)
        i = chunks.index((a, piece)) * max(1, groups - 1) + k - 1
        return pltpu.make_async_remote_copy(
            src_ref=dst.at[at[0], at[1]], dst_ref=dst.at[at[0], at[1]],
            send_sem=xsend.at[i], recv_sem=xrecv.at[i],
            device_id={"grp": (grp + k) % groups})

    pl.semaphore_wait(barrier, half - 1 + 1 + groups - 1)
    weight_copy(*chunks[0]).start()

    lane = lax.broadcasted_iota(jnp.int32, (rows, 128), 1)
    chosen = jnp.zeros((rows, 128), F32)
    weight = jnp.zeros((rows, 128), F32)
    for k in range(routes_ref.shape[1]):
        hit = lane == routes_ref[:, k:k + 1]
        chosen = chosen + jnp.where(hit, 1.0, 0.0)
        weight = weight + jnp.where(hit, rw_ref[:, k:k + 1], 0.0)
    chosen_t = chosen.T
    earlier = (lax.broadcasted_iota(jnp.int32, (rows, rows), 0)
               < lax.broadcasted_iota(jnp.int32, (rows, rows), 1))
    before = dot(chosen_t.astype(BF16), jnp.where(earlier, 1.0, 0.0).astype(BF16))
    place[...] = jnp.where(chosen_t > 0.5, before, -1.0)
    scale[...] = weight.T

    loads[0].wait()
    for copy in loads[1:]:
        copy.start()

    def norm_step(i, c):
        at = pl.ds(pl.multiple_of(i * 32, 32), 32)
        x = tok[at, :].astype(F32)
        factor = lax.rsqrt(jnp.mean(x * x, axis=-1, keepdims=True) + 1e-06)
        normed[at, :] = (x * factor * gain_ref[...]).astype(BF16)
        return c

    lax.fori_loop(0, rows // 32, norm_step, 0)
    slot = lax.broadcasted_iota(jnp.int32, (capp, rows), 0).astype(F32)
    slot = jnp.where(slot < cap, slot, -2.0)

    def gather(p):
        ours = slot == place[pl.ds(base + p, 1), :]
        theirs = slot == place[pl.ds((base + half) % n + (p + half // 2) % half, 1), :]
        want = jnp.concatenate([jnp.where(ours, 1.0, 0.0), jnp.where(theirs, 1.0, 0.0)], axis=0)
        got = dot(want.astype(BF16), normed[...])
        return got[:capp].astype(BF16), got[capp:].astype(BF16)

    used = pl.ds(0, cap)

    def dispatch_copy(p):
        return pltpu.make_async_remote_copy(
            src_ref=obuf.at[:, p, used], dst_ref=arr.at[:, mine, used],
            send_sem=dsend.at[p], recv_sem=drecv.at[mine], device_id={"ep": base + p})

    def dispatch_wait(p):
        pltpu.make_async_remote_copy(
            src_ref=obuf.at[:, p, used], dst_ref=arr.at[:, p, used],
            send_sem=dsend.at[p], recv_sem=drecv.at[p], device_id={"ep": base + p}).wait_recv()

    def message(ref, p, m):
        if m == 0:
            return ref.at[0, p, used]
        return ref.at[1, p, used, pl.ds((m - 1) * slab, slab)]

    def return_copy(p, m):
        return pltpu.make_async_remote_copy(
            src_ref=message(ybuf, p, m), dst_ref=message(ret, mine, m),
            send_sem=rsend.at[p, m], recv_sem=rrecv.at[mine, m], device_id={"ep": base + p})

    def return_wait(p, m):
        pltpu.make_async_remote_copy(
            src_ref=message(ybuf, p, m), dst_ref=message(ret, p, m),
            send_sem=rsend.at[p, m], recv_sem=rrecv.at[p, m],
            device_id={"ep": base + p}).wait_recv()

    def dispatch_step(i, c):
        p = peer(half - 1 - i)
        first, second = gather(p)
        obuf[0, p] = first
        obuf[1, p] = second
        dispatch_copy(p).start()
        return c

    lax.fori_loop(0, half - 1, dispatch_step, 0)
    for a, piece in chunks[1:-SLABS]:
        weight_copy(a, piece).start()
    first, second = gather(mine)
    arr[0, mine] = first
    arr[1, mine] = second

    for copy in loads[4:]:
        copy.wait()
    acc[...] = dot(hidden_rows(normed[...], sg[...], su[...]), sd[...])
    for copy in loads[1:4]:
        copy.wait()

    for b in range(2):
        for p in range(half):
            at = pl.ds((base + b * half) % n + (p + b * (half // 2)) % half, 1)
            want = jnp.where(slot == place[at, :], scale[at, :], 0.0)
            pick[b, p * capp:(p + 1) * capp, :] = want.astype(BF16)

    def own_step(i, c):
        p = peer((i + half // 2 - 1) % (half - 1) + 1)
        dispatch_wait(p)
        ybuf[0, p] = dot(hidden_rows(arr[0, p], wg[...], wu[...]), wd[...]).astype(BF16)
        return_copy(p, 0).start()
        return c

    def forward(a, piece):
        weight_copy(a, piece).wait_recv()
        for k in range(1, groups):
            forward_copy(a, piece, k).start()

    def forwarded(a, piece):
        for k in range(1, groups):
            forward_copy(a, piece, k).wait_recv()

    early = chunks[:-SLABS]
    done = 0
    for i, (a, piece) in enumerate(early):
        until = (half - 1) * (i + 1) // len(early)
        lax.fori_loop(done, until, own_step, 0)
        done = until
        forward(a, piece)
        weight_copy(*chunks[len(early) + i]).start()
    own = dot(hidden_rows(arr[0, mine], wg[...], wu[...]), wd[...]).astype(BF16)
    ret[0, mine] = own

    for a, piece in early:
        forwarded(a, piece)
    hid[...] = hidden_rows(arr[1].reshape(half * capp, width), fg[...], fu[...])

    def far_slab(c):
        forwarded(2, c)
        cols = pl.ds(c * slab, slab)
        got = dot(hid[...], fd[:, cols]).astype(BF16)
        ybuf[1, :, :, cols] = got.reshape(half, capp, slab)

        def send(i, k):
            return_copy(peer(half - 1 - i), 1 + c).start()
            return k

        lax.fori_loop(0, half - 1, send, 0)
        ret[1, mine, :, cols] = ybuf[1, mine, :, cols]

    for c in range(SLABS):
        forward(2, c)
        if c > 0:
            far_slab(c - 1)
    far_slab(SLABS - 1)

    def arrive(m):
        def step(i, k):
            return_wait(peer(i + 1), m)
            return k

        lax.fori_loop(0, half - 1, step, 0)

    arrive(0)
    acc[...] += dot(pick[0], ret[0].reshape(half * capp, width), ((0,), (0,)))
    for c in range(SLABS):
        arrive(1 + c)
        cols = pl.ds(c * slab, slab)
        total = acc[:, cols] + dot(
            pick[1], ret[1, :, :, cols].reshape(half * capp, slab), ((0,), (0,)))
        out_ref[:, cols] = total.astype(BF16)

    def drain(i, c):
        p = peer(half - 1 - i)
        dispatch_copy(p).wait_send()
        for m in range(1 + SLABS):
            return_copy(p, m).wait_send()
        return c

    lax.fori_loop(0, half - 1, drain, 0)
    for a, piece in chunks:
        weight_copy(a, piece).wait_send()
        for k in range(1, groups):
            forward_copy(a, piece, k).wait_send()


def on_halves(tokens, norm_gain, routes, route_weights, expert_gate, expert_up, expert_down,
              shared_gate, shared_up, shared_down):
    rows, width = tokens.shape
    n, groups = lax.axis_size("ep"), lax.axis_size("grp")
    half = n // 2
    cap = -(-(5 * rows * routes.shape[1] // (4 * n)) // 8) * 8
    nchunk = 2 * PIECES + SLABS
    nfwd = nchunk * max(1, groups - 1)
    vmem = lambda shape, kind=BF16: pltpu.VMEM(shape, kind)
    anyspec = pl.BlockSpec(memory_space=pl.ANY)
    vspec = pl.BlockSpec(memory_space=pltpu.VMEM)
    capp = cap
    block = (2, half, capp, width)
    return pl.pallas_call(
        functools.partial(halves_kernel, n, groups, cap),
        out_shape=jax.ShapeDtypeStruct((rows, width), BF16),
        in_specs=[anyspec, vspec, vspec, vspec] + [anyspec] * 6,
        out_specs=vspec,
        scratch_shapes=[
            vmem((rows, width)), vmem((rows, width)), vmem((128, rows), F32), vmem((128, rows), F32),
            vmem(expert_gate.shape[1:]), vmem(expert_up.shape[1:]), vmem(expert_down.shape[1:]),
            vmem(expert_gate.shape[1:]), vmem(expert_up.shape[1:]), vmem(expert_down.shape[1:]),
            vmem(shared_gate.shape), vmem(shared_up.shape), vmem(shared_down.shape),
            vmem(block), vmem(block), vmem(block), vmem(block), vmem((rows, width), F32),
            vmem((half * capp, expert_gate.shape[2])), vmem((2, half * capp, rows)),
            pltpu.SemaphoreType.DMA((7,)),
            pltpu.SemaphoreType.DMA((nchunk,)), pltpu.SemaphoreType.DMA((nchunk,)),
            pltpu.SemaphoreType.DMA((nfwd,)), pltpu.SemaphoreType.DMA((nfwd,)),
            pltpu.SemaphoreType.DMA((half,)), pltpu.SemaphoreType.DMA((half,)),
            pltpu.SemaphoreType.DMA((half, 1 + SLABS)), pltpu.SemaphoreType.DMA((half, 1 + SLABS)),
        ],
        compiler_params=pltpu.CompilerParams(
            collective_id=0, has_side_effects=True, vmem_limit_bytes=60 * 1024 * 1024),
    )(tokens, norm_gain.reshape(1, width), routes, route_weights, expert_gate, expert_up,
      expert_down, shared_gate, shared_up, shared_down)


def layers_kernel(
    n, cap,
    tokens_hbm, gain_ref, routes_ref, rw_ref, eg_hbm, eu_hbm, ed_hbm, sg_hbm, su_hbm, sd_hbm,
    out_ref,
    tok, normed, place, scale, wg, wu, wd, fgu, fd, pgu, pd, sg, su, sd, obuf, arr, ybuf, ret, acc, hid, phid, pick,
    load_sem, sent, wsent, landed, wrecv, precv, orecv, mrecv,
):
    q = n // 4
    me = lax.axis_index("ep")
    grp = lax.axis_index("grp")
    layer, s = me // q, me % q
    side = layer // 2
    inner = (layer % 3 + 1) // 2
    outer = 1 - inner
    inner_l, outer_l = 1 + side, 3 * side
    other_l = inner_l + outer_l - layer
    far_in, far_out = 2 - side, 3 - 3 * side
    par = (grp + s) % 2
    twin = s + 1 - 2 * (s % 2)
    rows, width = tok.shape
    is_a = (inner == 1) & (par == 0)
    is_b = (inner == 1) & (par == 1)
    is_c = (inner == 0) & (par == 0)
    is_d = (inner == 0) & (par == 1)

    barrier = pltpu.get_barrier_semaphore()

    def greet(i, c):
        k = (grp * 2 * q + me % (2 * q) + i) % (4 * q)
        pl.semaphore_signal(barrier, inc=1, device_id={"grp": k // (2 * q), "ep": side * 2 * q + k % (2 * q)})
        return c

    lax.fori_loop(1, 4 * q, greet, 0)

    @pl.when(inner == 1)
    def _():
        pl.semaphore_signal(barrier, inc=1, device_id={"ep": far_in * q + s})
        pl.semaphore_signal(barrier, inc=1, device_id={"ep": far_in * q + twin})

    loads = [(tokens_hbm, tok), (eg_hbm.at[0], wg), (eu_hbm.at[0], wu), (ed_hbm.at[0], wd),
             (sg_hbm, sg), (su_hbm, su), (sd_hbm, sd)]
    loads = [pltpu.make_async_copy(a, b, load_sem.at[i]) for i, (a, b) in enumerate(loads)]
    for copy in loads:
        copy.start()

    strip = width // STRIPS
    depth = fgu.shape[1] // PARTS

    def chunk_copies(i, srcs, dsts, sem, recv, to):
        if i < PARTS:
            at = pl.ds(i * depth, depth)
            pairs = [(srcs[a].at[at], dsts[a].at[at], sem + a) for a in range(2)]
        else:
            at = pl.ds((i - PARTS) * strip, strip)
            pairs = [(srcs[2].at[:, at], dsts[2].at[:, at], sem + 2)]
        return [pltpu.make_async_remote_copy(
            src_ref=a, dst_ref=b, send_sem=wsent.at[k], recv_sem=recv.at[i], device_id={"ep": to})
            for a, b, k in pairs]

    own = (eg_hbm.at[0], eu_hbm.at[0], ed_hbm.at[0])
    far = (fgu.at[0], fgu.at[1], fd)
    passed = (pgu.at[0], pgu.at[1], pd)
    nchunk = PARTS + STRIPS

    def cross(i):
        return chunk_copies(i, own, far, 0, wrecv, far_in * q + s)

    def relay(i):
        return chunk_copies(i, far, far, 3, wrecv, outer_l * q + s)

    def inward(i):
        return chunk_copies(i, own, passed, 0, precv, inner_l * q + twin)

    def onward(i):
        return chunk_copies(i, passed, far, 6, wrecv, far_in * q + twin)

    def start(copies):
        for copy in copies:
            copy.start()

    def remote(ref, sem):
        return pltpu.make_async_remote_copy(
            src_ref=ref, dst_ref=ref, send_sem=sem, recv_sem=sem, device_id={"ep": other_l * q + s})

    def chunk_landed(i, gu, down, recv):
        if i < PARTS:
            remote(gu.at[:, pl.ds(i * depth, depth)], recv.at[i]).wait_recv()
        else:
            remote(down.at[:, pl.ds((i - PARTS) * strip, strip)], recv.at[i]).wait_recv()

    def weights_sent(srcs, k):
        for a in range(3):
            remote(srcs[a], wsent.at[k + a]).wait_send()

    expert = lax.broadcasted_iota(jnp.int32, (128, rows), 0)
    chosen = jnp.zeros((128, rows), F32)
    weight = jnp.zeros((128, rows), F32)
    for k in range(routes_ref.shape[0]):
        hit = expert == routes_ref[k:k + 1, :]
        chosen = chosen + jnp.where(hit, 1.0, 0.0)
        weight = weight + jnp.where(hit, rw_ref[k:k + 1, :], 0.0)
    earlier = (lax.broadcasted_iota(jnp.int32, (rows, rows), 0)
               < lax.broadcasted_iota(jnp.int32, (rows, rows), 1))
    before = dot(chosen.astype(BF16), jnp.where(earlier, 1.0, 0.0).astype(BF16))
    place[...] = jnp.where(chosen > 0.5, before, -1.0)
    scale[...] = weight

    loads[0].wait()

    def norm_step(i, c):
        at = pl.ds(pl.multiple_of(i * 32, 32), 32)
        x = tok[at, :].astype(F32)
        factor = lax.rsqrt(jnp.mean(x * x, axis=-1, keepdims=True) + 1e-06)
        normed[at, :] = (x * factor * gain_ref[...]).astype(BF16)
        return c

    lax.fori_loop(0, rows // 32, norm_step, 0)
    slot = lax.broadcasted_iota(jnp.int32, (cap, rows), 0).astype(F32)

    class_layer = (other_l, layer, far_out, far_in)
    near_at = outer * q + s
    land_at = (outer * near_at + inner * (6 * q + grp * q + s), near_at,
               2 * q + outer * 2 * q + grp * q + s, 2 * q + grp * q + s)
    land_on = (outer + inner * 4, 0, 3, 2)
    at_home = (is_a, inner < 2, is_b, par == 0)
    home = (twin, s, s, s)

    def host(cls, t):
        if cls == 0:
            return outer * grp + inner * ((t + 1) % 2), inner_l * q + outer * t + inner * (t + 1 - 2 * (t % 2))
        if cls == 1:
            return grp, layer * q + t
        if cls == 2:
            return (t + 1) % 2, inner_l * q + t
        return t % 2, layer * q + t

    def dispatch_copy(cls, t):
        hg, he = host(cls, t)
        return pltpu.make_async_remote_copy(
            src_ref=obuf.at[cls * q + t], dst_ref=arr.at[land_at[cls]],
            send_sem=sent.at[0], recv_sem=landed.at[land_on[cls]], device_id={"grp": hg, "ep": he})

    def one_hot(cls, values):
        at = [pl.ds(class_layer[cls] * q + t, 1) for t in range(q)]
        return jnp.concatenate([jnp.where(slot == place[a, :], values(a), 0.0) for a in at], axis=0)

    def gather(cls):
        got = dot(one_hot(cls, lambda a: 1.0).astype(BF16), normed[...]).astype(BF16)
        obuf[cls * q:(cls + 1) * q] = got.reshape(q, cap, width)

    def dispatch(cls):
        def send(i, c):
            dispatch_copy(cls, (home[cls] + 1 + i) % q).start()
            return c

        lax.fori_loop(0, q - 1, send, 0)

        @pl.when(at_home[cls])
        def _():
            arr[land_at[cls]] = obuf[cls * q + home[cls]]

        if cls != 1:
            @pl.when(jnp.logical_not(at_home[cls]))
            def _():
                dispatch_copy(cls, home[cls]).start()

    gather(1)
    gather(0)
    pl.semaphore_wait(barrier, 4 * q - 1 + 2 * inner)

    @pl.when(is_a)
    def _():
        for i in range(nchunk):
            start(cross(i))

    @pl.when(inner == 0)
    def _():
        dispatch(0)

    dispatch(1)

    @pl.when(is_d)
    def _():
        for i in range(PARTS):
            start(inward(i))

    gather(3)
    gather(2)

    @pl.when(inner == 0)
    def _():
        dispatch(3)
        dispatch(2)

    @pl.when(is_d)
    def _():
        for i in range(PARTS, nchunk):
            start(inward(i))

    for cls in range(4):
        pick[cls] = one_hot(cls, lambda a: scale[a, :]).T.astype(BF16)
    for copy in loads[4:]:
        copy.wait()
    acc[...] = dot(hidden_rows(normed[...], sg[...], su[...]), sd[...])
    for copy in loads[1:4]:
        copy.wait()

    def group_cols(m):
        first, count = GROUPS[m]
        return pl.ds(first * strip, count * strip)

    def near_return(base, cls, t):
        to = (other_l, layer)[cls]
        return pltpu.make_async_remote_copy(
            src_ref=ybuf.at[base + t], dst_ref=ret.at[cls * q + s],
            send_sem=sent.at[1], recv_sem=landed.at[5 + cls], device_id={"ep": to * q + t})

    def near(cls):
        base = (inner * q, outer * q)[cls]
        remote(arr.at[pl.ds(0, q - cls)], landed.at[1 - cls]).wait_recv()
        block = pl.ds(base, q)
        got = hidden_rows(arr[block].reshape(q * cap, width), wg[...], wu[...])
        ybuf[block] = dot(got, wd[...]).astype(BF16).reshape(q, cap, width)
        if cls == 1:
            ret[q + s] = ybuf[base + s]
            near_send(1)

    def near_send(cls):
        base = (inner * q, outer * q)[cls]

        def send(i, c):
            near_return(base, cls, (s + 1 + i) % q).start()
            return c

        lax.fori_loop(0, q - cls, send, 0)

    def far_peer(i):
        k = (grp * q + s + i) % (2 * q)
        return k // q, k % q

    def inner_return(i):
        g, t = far_peer(i)
        return pltpu.make_async_remote_copy(
            src_ref=ybuf.at[2 * q + g * q + t], dst_ref=ret.at[3 * q + s],
            send_sem=sent.at[2], recv_sem=landed.at[7], device_id={"grp": g, "ep": layer * q + t})

    def outer_return(i, m):
        sel, g, t = i // (2 * q), *far_peer(i % (2 * q))
        cols = group_cols(m)
        k = sel * 2 * q + g * q + t
        return pltpu.make_async_remote_copy(
            src_ref=ybuf.at[2 * q + k, :, cols], dst_ref=ret.at[2 * q + s, :, cols],
            send_sem=sent.at[3], recv_sem=orecv.at[m],
            device_id={"grp": g, "ep": (inner_l + sel * (outer_l - inner_l)) * q + t})

    def passed_return(i, m):
        g, t = far_peer(i)
        cols = group_cols(m)
        return pltpu.make_async_remote_copy(
            src_ref=ybuf.at[6 * q + g * q + t, :, cols], dst_ref=ret.at[twin, :, cols],
            send_sem=sent.at[4], recv_sem=mrecv.at[m], device_id={"grp": g, "ep": layer * q + t})

    def far_arrived(count, k):
        remote(arr.at[pl.ds(0, count)], landed.at[k]).wait_recv()

    def hand_on(i):
        chunk_landed(i, pgu, pd, precv)
        start(onward(i))

    def take(i):
        chunk_landed(i, fgu, fd, wrecv)
        start(relay(i))

    @pl.when(is_a)
    def _():
        for i in range(PARTS):
            take(i)
            if i == 3:
                dispatch(3)
            if i == 5:
                dispatch(0)
        dispatch(2)
        for i in range(PARTS):
            hand_on(i)
            if i < STRIPS:
                take(PARTS + i)
        for i in range(2 * PARTS, nchunk):
            take(i)

    near(1)

    @pl.when(is_b)
    def _():
        dispatch(3)
        dispatch(0)
        dispatch(2)

    @pl.when(inner == 1)
    def _():
        near(0)

    @pl.when(par == 0)
    def _():
        @pl.when(inner == 0)
        def _():
            for i in range(nchunk):
                chunk_landed(i, fgu, fd, wrecv)

        @pl.when(inner == 1)
        def _():
            near_send(0)

        far_arrived(2 * q - 1, 2)
        hid[:2 * q * cap] = hidden_rows(
            arr[2 * q:4 * q].reshape(2 * q * cap, width), fgu[0], fgu[1])
        got = dot(hid[:2 * q * cap], fd[...]).astype(BF16)
        ybuf[2 * q:4 * q] = got.reshape(2 * q, cap, width)

        def send(i, c):
            inner_return(i).start()
            return c

        lax.fori_loop(1, 2 * q, send, 0)
        ret[3 * q + s] = ybuf[2 * q + grp * q + s]

    def passed_strips(m):
        cols = group_cols(m)
        got = dot(phid[...], pd[:, cols]).astype(BF16)
        ybuf[6 * q:, :, cols] = got.reshape(2 * q, cap, cols.size)

        def send(i, c):
            passed_return(i, m).start()
            return c

        lax.fori_loop(1, 2 * q, send, 0)
        ret[twin, :, cols] = ybuf[6 * q + grp * q + s, :, cols]

    def outer_strips(m):
        first, count = GROUPS[m]
        cols = group_cols(m)
        for i in range(first, first + count):
            chunk_landed(PARTS + i, fgu, fd, wrecv)
        got = dot(hid[...], fd[:, cols]).astype(BF16)
        ybuf[2 * q:6 * q, :, cols] = got.reshape(4 * q, cap, cols.size)

        def send(i, c):
            outer_return(4 * q - i, m).start()
            return c

        lax.fori_loop(1, 4 * q, send, 0)
        ret[2 * q + s, :, cols] = ybuf[2 * q + grp * q + s, :, cols]

    @pl.when(is_a)
    def _():
        far_arrived(2 * q - 1, 4)
        phid[...] = hidden_rows(arr[6 * q:].reshape(2 * q * cap, width), pgu[0], pgu[1])
        for m, (first, count) in enumerate(GROUPS):
            for i in range(first, first + count):
                hand_on(PARTS + i)
            passed_strips(m)

    @pl.when(is_b)
    def _():
        near_send(0)
        for i in range(PARTS):
            chunk_landed(i, fgu, fd, wrecv)
        far_arrived(4 * q - 1, 3)
        hid[...] = hidden_rows(arr[2 * q:6 * q].reshape(4 * q * cap, width), fgu[0], fgu[1])
        for m in range(len(GROUPS)):
            outer_strips(m)

    def back(k, home):
        remote(ret.at[pl.ds(0, q - home)], landed.at[k]).wait_recv()

    def strip_back(at, sem, m, home):
        remote(ret.at[pl.ds(at, q - home), :, group_cols(m)], sem.at[m]).wait_recv()

    def weighted(cls, cols):
        return dot(pick[cls], ret[cls * q:(cls + 1) * q, :, cols].reshape(q * cap, -1))

    back(6, 1)
    acc[...] += weighted(1, slice(None))

    @pl.when(par == 0)
    def _():
        back(7, 1)

    @pl.when(par == 1)
    def _():
        back(7, 0)

    acc[...] += weighted(3, slice(None))

    @pl.when(inner == 0)
    def _():
        back(5, 0)

    for m, (first, count) in enumerate(GROUPS):
        @pl.when(is_b)
        def _():
            strip_back(0, mrecv, m, 0)
            strip_back(2 * q, orecv, m, 1)

        @pl.when(is_a)
        def _():
            strip_back(0, mrecv, m, 1)

        @pl.when(jnp.logical_not(is_b))
        def _():
            strip_back(2 * q, orecv, m, 0)

        cols = slice(first * strip, (first + count) * strip)
        out_ref[:, cols] = (acc[:, cols] + weighted(0, cols) + weighted(2, cols)).astype(BF16)

    def drain(ref, count, k):
        remote(ref.at[pl.ds(0, count)], sent.at[k]).wait_send()

    @pl.when(is_a)
    def _():
        drain(obuf, 4 * q - 3, 0)
        drain(ybuf, 2 * q - 1, 1)
        drain(ybuf, 2 * q - 1, 2)
        drain(ybuf, 2 * q - 1, 4)
        weights_sent(own, 0)
        weights_sent(far, 3)
        weights_sent(passed, 6)

    @pl.when(is_b)
    def _():
        drain(obuf, 4 * q - 2, 0)
        drain(ybuf, 2 * q - 1, 1)
        drain(ybuf, 4 * q - 1, 3)

    @pl.when(is_c)
    def _():
        drain(obuf, 4 * q - 2, 0)
        drain(ybuf, q - 1, 1)
        drain(ybuf, 2 * q - 1, 2)

    @pl.when(is_d)
    def _():
        drain(obuf, 4 * q - 1, 0)
        drain(ybuf, q - 1, 1)
        weights_sent(own, 0)


def on_layers(tokens, norm_gain, routes, route_weights, expert_gate, expert_up, expert_down,
              shared_gate, shared_up, shared_down):
    rows, width = tokens.shape
    n = lax.axis_size("ep")
    q = n // 4
    cap = -(-(5 * rows * routes.shape[1] // (4 * n)) // 8) * 8
    vmem = lambda shape, kind=BF16: pltpu.VMEM(shape, kind)
    sems = lambda *shape: pltpu.SemaphoreType.DMA(shape)
    anyspec = pl.BlockSpec(memory_space=pl.ANY)
    vspec = pl.BlockSpec(memory_space=pltpu.VMEM)
    ff = expert_gate.shape[2]
    both = (2,) + expert_gate.shape[1:]
    return pl.pallas_call(
        functools.partial(layers_kernel, n, cap),
        out_shape=pltpu.VMEM((rows, width), BF16),
        in_specs=[anyspec, vspec, vspec, vspec] + [anyspec] * 6,
        out_specs=vspec,
        scratch_shapes=[
            vmem((rows, width)), vmem((rows, width)), vmem((128, rows), F32), vmem((128, rows), F32),
            vmem(expert_gate.shape[1:]), vmem(expert_up.shape[1:]), vmem(expert_down.shape[1:]),
            vmem(both), vmem(expert_down.shape[1:]), vmem(both), vmem(expert_down.shape[1:]),
            vmem(shared_gate.shape), vmem(shared_up.shape), vmem(shared_down.shape),
            vmem((n, cap, width)), vmem((8 * q, cap, width)), vmem((8 * q, cap, width)), vmem((n, cap, width)),
            vmem((rows, width), F32), vmem((4 * q * cap, ff)), vmem((2 * q * cap, ff)), vmem((4, rows, q * cap)),
            sems(7), sems(5), sems(9), sems(8), sems(PARTS + STRIPS), sems(PARTS + STRIPS),
            sems(len(GROUPS)), sems(len(GROUPS)),
        ],
        compiler_params=pltpu.CompilerParams(
            collective_id=0, has_side_effects=True, vmem_limit_bytes=62 * 1024 * 1024 + 512 * 1024),
    )(tokens, norm_gain.reshape(1, width), routes.T, route_weights.T, expert_gate, expert_up,
      expert_down, shared_gate, shared_up, shared_down)


def on_device(*args):
    n, groups = lax.axis_size("ep"), lax.axis_size("grp")
    if groups == 2 and n % 8 == 0 and n <= 32:
        return on_layers(*args)
    return on_halves(*args)


def solution(mesh):
    return jax.shard_map(
        on_device,
        mesh=mesh,
        in_specs=(
            P(("grp", "ep"), None),
            P(),
            P(("grp", "ep"), None),
            P(("grp", "ep"), None),
            P("ep", None, None),
            P("ep", None, None),
            P("ep", None, None),
            P(),
            P(),
            P(),
        ),
        out_specs=P(("grp", "ep"), None),
        check_vma=False,
    )
```

```python
import functools

import jax
import jax.numpy as jnp
from jax import lax
from jax.experimental import pallas as pl
from jax.experimental.pallas import tpu as pltpu
from jax.sharding import PartitionSpec as P

BF16 = jnp.bfloat16
F32 = jnp.float32
PIECES = 2
SLABS = 4
PARTS = 8
STRIPS = 8
HELD = 2
GROUPS = tuple((i, 1) for i in range(STRIPS))


def dot(a, b, dims=((1,), (0,))):
    return lax.dot_general(a, b, (dims, ((), ())), preferred_element_type=F32)


def hidden_rows(rows, w_gate, w_up):
    gate_part = dot(rows, w_gate)
    up_part = dot(rows, w_up)
    return (gate_part / (1.0 + jnp.exp(-gate_part)) * up_part).astype(BF16)


def halves_kernel(
    n, groups, cap,
    tokens_hbm, gain_ref, routes_ref, rw_ref, eg_hbm, eu_hbm, ed_hbm, sg_hbm, su_hbm, sd_hbm,
    out_ref,
    tok, normed, place, scale, wg, wu, wd, fg, fu, fd, sg, su, sd, obuf, arr, ybuf, ret, acc, hid, pick,
    load_sem, wsend, wrecv, xsend, xrecv, dsend, drecv, rsend, rrecv,
):
    half = n // 2
    me = lax.axis_index("ep")
    grp = lax.axis_index("grp")
    base = (me // half) * half
    mine = me % half
    far = (base + half) % n + (mine + half // 2) % half
    rows = tok.shape[0]
    width = tok.shape[1]

    def peer(j):
        total, bit = 0, 1
        while bit < half:
            total = total + bit * (((mine // bit) % 2 + (j // bit) % 2) % 2)
            bit *= 2
        return total

    capp = ret.shape[2]
    if capp > cap:
        low = cap // 16 * 16
        ret[:, :, low:, :] = jnp.zeros((2, half, capp - low, width), BF16)
    barrier = pltpu.get_barrier_semaphore()

    def greet(i, c):
        pl.semaphore_signal(barrier, inc=1, device_id={"ep": base + peer(i)})
        return c

    lax.fori_loop(1, half, greet, 0)
    pl.semaphore_signal(barrier, inc=1, device_id={"ep": far})
    for k in range(1, groups):
        pl.semaphore_signal(barrier, inc=1, device_id={"grp": (grp + k) % groups})

    loads = [(tokens_hbm, tok), (eg_hbm.at[0], wg), (eu_hbm.at[0], wu), (ed_hbm.at[0], wd),
             (sg_hbm, sg), (su_hbm, su), (sd_hbm, sd)]
    loads = [pltpu.make_async_copy(a, b, load_sem.at[i]) for i, (a, b) in enumerate(loads)]
    loads[0].start()

    slab = width // SLABS

    def region(group, a, piece):
        depth = (fg, fu, fd)[a].shape[0] // groups
        if a == 2:
            return pl.ds(pl.multiple_of(group * depth, depth), depth), pl.ds(piece * slab, slab)
        depth = depth // PIECES
        start = (group * PIECES + piece) * depth
        return pl.ds(pl.multiple_of(start, depth), depth), pl.ds(0, fg.shape[1])

    chunks = [(a, piece) for piece in range(PIECES) for a in range(2)]
    chunks += [(2, piece) for piece in range(SLABS)]

    def weight_copy(a, piece):
        src, dst = ((eg_hbm, fg), (eu_hbm, fu), (ed_hbm, fd))[a]
        at, i = region(grp, a, piece), chunks.index((a, piece))
        return pltpu.make_async_remote_copy(
            src_ref=src.at[0, at[0], at[1]], dst_ref=dst.at[at[0], at[1]],
            send_sem=wsend.at[i], recv_sem=wrecv.at[i], device_id={"ep": far})

    def forward_copy(a, piece, k):
        dst = (fg, fu, fd)[a]
        at = region(grp, a, piece)
        i = chunks.index((a, piece)) * max(1, groups - 1) + k - 1
        return pltpu.make_async_remote_copy(
            src_ref=dst.at[at[0], at[1]], dst_ref=dst.at[at[0], at[1]],
            send_sem=xsend.at[i], recv_sem=xrecv.at[i],
            device_id={"grp": (grp + k) % groups})

    pl.semaphore_wait(barrier, half - 1 + 1 + groups - 1)
    weight_copy(*chunks[0]).start()

    lane = lax.broadcasted_iota(jnp.int32, (rows, 128), 1)
    chosen = jnp.zeros((rows, 128), F32)
    weight = jnp.zeros((rows, 128), F32)
    for k in range(routes_ref.shape[1]):
        hit = lane == routes_ref[:, k:k + 1]
        chosen = chosen + jnp.where(hit, 1.0, 0.0)
        weight = weight + jnp.where(hit, rw_ref[:, k:k + 1], 0.0)
    chosen_t = chosen.T
    earlier = (lax.broadcasted_iota(jnp.int32, (rows, rows), 0)
               < lax.broadcasted_iota(jnp.int32, (rows, rows), 1))
    before = dot(chosen_t.astype(BF16), jnp.where(earlier, 1.0, 0.0).astype(BF16))
    place[...] = jnp.where(chosen_t > 0.5, before, -1.0)
    scale[...] = weight.T

    loads[0].wait()
    for copy in loads[1:]:
        copy.start()

    def norm_step(i, c):
        at = pl.ds(pl.multiple_of(i * 32, 32), 32)
        x = tok[at, :].astype(F32)
        factor = lax.rsqrt(jnp.mean(x * x, axis=-1, keepdims=True) + 1e-06)
        normed[at, :] = (x * factor * gain_ref[...]).astype(BF16)
        return c

    lax.fori_loop(0, rows // 32, norm_step, 0)
    slot = lax.broadcasted_iota(jnp.int32, (capp, rows), 0).astype(F32)
    slot = jnp.where(slot < cap, slot, -2.0)

    def gather(p):
        ours = slot == place[pl.ds(base + p, 1), :]
        theirs = slot == place[pl.ds((base + half) % n + (p + half // 2) % half, 1), :]
        want = jnp.concatenate([jnp.where(ours, 1.0, 0.0), jnp.where(theirs, 1.0, 0.0)], axis=0)
        got = dot(want.astype(BF16), normed[...])
        return got[:capp].astype(BF16), got[capp:].astype(BF16)

    used = pl.ds(0, cap)

    def dispatch_copy(p):
        return pltpu.make_async_remote_copy(
            src_ref=obuf.at[:, p, used], dst_ref=arr.at[:, mine, used],
            send_sem=dsend.at[p], recv_sem=drecv.at[mine], device_id={"ep": base + p})

    def dispatch_wait(p):
        pltpu.make_async_remote_copy(
            src_ref=obuf.at[:, p, used], dst_ref=arr.at[:, p, used],
            send_sem=dsend.at[p], recv_sem=drecv.at[p], device_id={"ep": base + p}).wait_recv()

    def message(ref, p, m):
        if m == 0:
            return ref.at[0, p, used]
        return ref.at[1, p, used, pl.ds((m - 1) * slab, slab)]

    def return_copy(p, m):
        return pltpu.make_async_remote_copy(
            src_ref=message(ybuf, p, m), dst_ref=message(ret, mine, m),
            send_sem=rsend.at[p, m], recv_sem=rrecv.at[mine, m], device_id={"ep": base + p})

    def return_wait(p, m):
        pltpu.make_async_remote_copy(
            src_ref=message(ybuf, p, m), dst_ref=message(ret, p, m),
            send_sem=rsend.at[p, m], recv_sem=rrecv.at[p, m],
            device_id={"ep": base + p}).wait_recv()

    def dispatch_step(i, c):
        p = peer(half - 1 - i)
        first, second = gather(p)
        obuf[0, p] = first
        obuf[1, p] = second
        dispatch_copy(p).start()
        return c

    lax.fori_loop(0, half - 1, dispatch_step, 0)
    for a, piece in chunks[1:-SLABS]:
        weight_copy(a, piece).start()
    first, second = gather(mine)
    arr[0, mine] = first
    arr[1, mine] = second

    for copy in loads[4:]:
        copy.wait()
    acc[...] = dot(hidden_rows(normed[...], sg[...], su[...]), sd[...])
    for copy in loads[1:4]:
        copy.wait()

    for b in range(2):
        for p in range(half):
            at = pl.ds((base + b * half) % n + (p + b * (half // 2)) % half, 1)
            want = jnp.where(slot == place[at, :], scale[at, :], 0.0)
            pick[b, p * capp:(p + 1) * capp, :] = want.astype(BF16)

    def own_step(i, c):
        p = peer((i + half // 2 - 1) % (half - 1) + 1)
        dispatch_wait(p)
        ybuf[0, p] = dot(hidden_rows(arr[0, p], wg[...], wu[...]), wd[...]).astype(BF16)
        return_copy(p, 0).start()
        return c

    def forward(a, piece):
        weight_copy(a, piece).wait_recv()
        for k in range(1, groups):
            forward_copy(a, piece, k).start()

    def forwarded(a, piece):
        for k in range(1, groups):
            forward_copy(a, piece, k).wait_recv()

    early = chunks[:-SLABS]
    done = 0
    for i, (a, piece) in enumerate(early):
        until = (half - 1) * (i + 1) // len(early)
        lax.fori_loop(done, until, own_step, 0)
        done = until
        forward(a, piece)
        weight_copy(*chunks[len(early) + i]).start()
    own = dot(hidden_rows(arr[0, mine], wg[...], wu[...]), wd[...]).astype(BF16)
    ret[0, mine] = own

    for a, piece in early:
        forwarded(a, piece)
    hid[...] = hidden_rows(arr[1].reshape(half * capp, width), fg[...], fu[...])

    def far_slab(c):
        forwarded(2, c)
        cols = pl.ds(c * slab, slab)
        got = dot(hid[...], fd[:, cols]).astype(BF16)
        ybuf[1, :, :, cols] = got.reshape(half, capp, slab)

        def send(i, k):
            return_copy(peer(half - 1 - i), 1 + c).start()
            return k

        lax.fori_loop(0, half - 1, send, 0)
        ret[1, mine, :, cols] = ybuf[1, mine, :, cols]

    for c in range(SLABS):
        forward(2, c)
        if c > 0:
            far_slab(c - 1)
    far_slab(SLABS - 1)

    def arrive(m):
        def step(i, k):
            return_wait(peer(i + 1), m)
            return k

        lax.fori_loop(0, half - 1, step, 0)

    arrive(0)
    acc[...] += dot(pick[0], ret[0].reshape(half * capp, width), ((0,), (0,)))
    for c in range(SLABS):
        arrive(1 + c)
        cols = pl.ds(c * slab, slab)
        total = acc[:, cols] + dot(
            pick[1], ret[1, :, :, cols].reshape(half * capp, slab), ((0,), (0,)))
        out_ref[:, cols] = total.astype(BF16)

    def drain(i, c):
        p = peer(half - 1 - i)
        dispatch_copy(p).wait_send()
        for m in range(1 + SLABS):
            return_copy(p, m).wait_send()
        return c

    lax.fori_loop(0, half - 1, drain, 0)
    for a, piece in chunks:
        weight_copy(a, piece).wait_send()
        for k in range(1, groups):
            forward_copy(a, piece, k).wait_send()


def on_halves(tokens, norm_gain, routes, route_weights, expert_gate, expert_up, expert_down,
              shared_gate, shared_up, shared_down):
    rows, width = tokens.shape
    n, groups = lax.axis_size("ep"), lax.axis_size("grp")
    half = n // 2
    cap = -(-(5 * rows * routes.shape[1] // (4 * n)) // 8) * 8
    nchunk = 2 * PIECES + SLABS
    nfwd = nchunk * max(1, groups - 1)
    vmem = lambda shape, kind=BF16: pltpu.VMEM(shape, kind)
    anyspec = pl.BlockSpec(memory_space=pl.ANY)
    vspec = pl.BlockSpec(memory_space=pltpu.VMEM)
    capp = cap
    block = (2, half, capp, width)
    return pl.pallas_call(
        functools.partial(halves_kernel, n, groups, cap),
        out_shape=jax.ShapeDtypeStruct((rows, width), BF16),
        in_specs=[anyspec, vspec, vspec, vspec] + [anyspec] * 6,
        out_specs=vspec,
        scratch_shapes=[
            vmem((rows, width)), vmem((rows, width)), vmem((128, rows), F32), vmem((128, rows), F32),
            vmem(expert_gate.shape[1:]), vmem(expert_up.shape[1:]), vmem(expert_down.shape[1:]),
            vmem(expert_gate.shape[1:]), vmem(expert_up.shape[1:]), vmem(expert_down.shape[1:]),
            vmem(shared_gate.shape), vmem(shared_up.shape), vmem(shared_down.shape),
            vmem(block), vmem(block), vmem(block), vmem(block), vmem((rows, width), F32),
            vmem((half * capp, expert_gate.shape[2])), vmem((2, half * capp, rows)),
            pltpu.SemaphoreType.DMA((7,)),
            pltpu.SemaphoreType.DMA((nchunk,)), pltpu.SemaphoreType.DMA((nchunk,)),
            pltpu.SemaphoreType.DMA((nfwd,)), pltpu.SemaphoreType.DMA((nfwd,)),
            pltpu.SemaphoreType.DMA((half,)), pltpu.SemaphoreType.DMA((half,)),
            pltpu.SemaphoreType.DMA((half, 1 + SLABS)), pltpu.SemaphoreType.DMA((half, 1 + SLABS)),
        ],
        compiler_params=pltpu.CompilerParams(
            collective_id=0, has_side_effects=True, vmem_limit_bytes=60 * 1024 * 1024),
    )(tokens, norm_gain.reshape(1, width), routes, route_weights, expert_gate, expert_up,
      expert_down, shared_gate, shared_up, shared_down)


def layers_kernel(
    n, cap,
    tokens_hbm, gain_ref, routes_ref, rw_ref, eg_hbm, eu_hbm, ed_hbm, sg_hbm, su_hbm, sd_hbm,
    out_ref,
    tok, normed, place, scale, wg, wu, wd, fgu, fd, pgu, pd, sg, su, sd, obuf, arr, ybuf, ret, acc, gsum, hid, phid, pick,
    load_sem, sent, wsent, landed, wrecv, precv, orecv, mrecv,
):
    q = n // 4
    me = lax.axis_index("ep")
    grp = lax.axis_index("grp")
    layer, s = me // q, me % q
    side = layer // 2
    inner = (layer % 3 + 1) // 2
    outer = 1 - inner
    inner_l, outer_l = 1 + side, 3 * side
    other_l = inner_l + outer_l - layer
    far_in, far_out = 2 - side, 3 - 3 * side
    par = (grp + s) % 2
    twin = s + 1 - 2 * (s % 2)
    rows, width = tok.shape
    is_a = (inner == 1) & (par == 0)
    is_b = (inner == 1) & (par == 1)
    is_c = (inner == 0) & (par == 0)
    is_d = (inner == 0) & (par == 1)

    barrier = pltpu.get_barrier_semaphore()

    first_ep = side * 2 * q
    for g in range(2):
        for i in range(1 - g, 2 * q):
            pl.semaphore_signal(barrier, inc=1, device_id={
                "grp": 1 - grp if g else grp, "ep": first_ep + lax.rem(me - first_ep + i, 2 * q)})

    @pl.when(inner == 1)
    def _():
        pl.semaphore_signal(barrier, inc=1, device_id={"ep": far_in * q + s})
        pl.semaphore_signal(barrier, inc=1, device_id={"ep": far_in * q + twin})

    loads = [(tokens_hbm, tok), (eg_hbm.at[0], wg), (eu_hbm.at[0], wu), (ed_hbm.at[0], wd),
             (sg_hbm, sg), (su_hbm, su), (sd_hbm, sd)]
    loads = [pltpu.make_async_copy(a, b, load_sem.at[i]) for i, (a, b) in enumerate(loads)]
    for copy in loads:
        copy.start()

    strip = width // STRIPS
    depth = fgu.shape[1] // PARTS

    def chunk_copies(i, srcs, dsts, sem, recv, to):
        if i < PARTS:
            at = pl.ds(i * depth, depth)
            pairs = [(srcs[a].at[at], dsts[a].at[at], sem + a) for a in range(2)]
        else:
            at = pl.ds((i - PARTS) * strip, strip)
            pairs = [(srcs[2].at[:, at], dsts[2].at[:, at], sem + 2)]
        return [pltpu.make_async_remote_copy(
            src_ref=a, dst_ref=b, send_sem=wsent.at[k], recv_sem=recv.at[i], device_id={"ep": to})
            for a, b, k in pairs]

    own = (wg, wu, wd)
    far = (fgu.at[0], fgu.at[1], fd)
    passed = (pgu.at[0], pgu.at[1], pd)
    nchunk = PARTS + STRIPS

    def cross(i):
        return chunk_copies(i, own, far, 0, wrecv, far_in * q + s)

    def relay(i):
        return chunk_copies(i, far, far, 3, wrecv, outer_l * q + s)

    def inward(i):
        return chunk_copies(i, own, passed, 0, precv, inner_l * q + twin)

    def onward(i):
        return chunk_copies(i, passed, far, 6, wrecv, far_in * q + twin)

    def start(copies):
        for copy in copies:
            copy.start()

    def remote(ref, sem):
        return pltpu.make_async_remote_copy(
            src_ref=ref, dst_ref=ref, send_sem=sem, recv_sem=sem, device_id={"ep": other_l * q + s})

    def chunk_landed(i, gu, down, recv):
        if i < PARTS:
            remote(gu.at[:, pl.ds(i * depth, depth)], recv.at[i]).wait_recv()
        else:
            remote(down.at[:, pl.ds((i - PARTS) * strip, strip)], recv.at[i]).wait_recv()

    def weights_sent(srcs, k):
        for a in range(3):
            remote(srcs[a], wsent.at[k + a]).wait_send()

    expert = lax.broadcasted_iota(jnp.int32, (128, rows), 0)
    chosen = jnp.zeros((128, rows), F32)
    weight = jnp.zeros((128, rows), F32)
    for k in range(routes_ref.shape[0]):
        hit = expert == routes_ref[k:k + 1, :]
        chosen = chosen + jnp.where(hit, 1.0, 0.0)
        weight = weight + jnp.where(hit, rw_ref[k:k + 1, :], 0.0)
    earlier = (lax.broadcasted_iota(jnp.int32, (rows, rows), 0)
               < lax.broadcasted_iota(jnp.int32, (rows, rows), 1))
    before = dot(chosen.astype(BF16), jnp.where(earlier, 1.0, 0.0).astype(BF16))
    place[...] = jnp.where(chosen > 0.5, before, -1.0)
    scale[...] = weight

    loads[0].wait()

    def norm_step(i, c):
        at = pl.ds(pl.multiple_of(i * 32, 32), 32)
        x = tok[at, :].astype(F32)
        factor = lax.rsqrt(jnp.mean(x * x, axis=-1, keepdims=True) + 1e-06)
        normed[at, :] = (x * factor * gain_ref[...]).astype(BF16)
        return c

    lax.fori_loop(0, rows // 32, norm_step, 0)
    slot = lax.broadcasted_iota(jnp.int32, (cap, rows), 0).astype(F32)

    class_layer = (other_l, layer, far_out, far_in)
    near_at = outer * q + s
    land_at = (outer * near_at + inner * (6 * q + grp * q + s), near_at,
               2 * q + outer * 2 * q + grp * q + s, 2 * q + grp * q + s)
    land_on = (outer + inner * 4, 0, 3, 2)
    at_home = (is_a, inner < 2, is_b, par == 0)
    home = (twin, s, s, s)

    def host(cls, t):
        if cls == 0:
            return outer * grp + inner * ((t + 1) % 2), inner_l * q + outer * t + inner * (t + 1 - 2 * (t % 2))
        if cls == 1:
            return grp, layer * q + t
        if cls == 2:
            return (t + 1) % 2, inner_l * q + t
        return t % 2, layer * q + t

    def dispatch_copy(cls, t):
        hg, he = host(cls, t)
        return pltpu.make_async_remote_copy(
            src_ref=obuf.at[cls * q + t], dst_ref=arr.at[land_at[cls]],
            send_sem=sent.at[0], recv_sem=landed.at[land_on[cls]], device_id={"grp": hg, "ep": he})

    def one_hot(cls, values):
        at = [pl.ds(class_layer[cls] * q + t, 1) for t in range(q)]
        return jnp.concatenate([jnp.where(slot == place[a, :], values(a), 0.0) for a in at], axis=0)

    def gather(cls):
        got = dot(one_hot(cls, lambda a: 1.0).astype(BF16), normed[...]).astype(BF16)
        obuf[cls * q:(cls + 1) * q] = got.reshape(q, cap, width)

    def dispatch(cls):
        def send(i, c):
            dispatch_copy(cls, (home[cls] + 1 + i) % q).start()
            return c

        lax.fori_loop(0, q - 1, send, 0)

        @pl.when(at_home[cls])
        def _():
            arr[land_at[cls]] = obuf[cls * q + home[cls]]

        if cls != 1:
            @pl.when(jnp.logical_not(at_home[cls]))
            def _():
                dispatch_copy(cls, home[cls]).start()

    for copy in loads[1:4]:
        copy.wait()
    pl.semaphore_wait(barrier, 4 * q - 1 + 2 * inner)

    @pl.when(is_a)
    def _():
        for i in range(nchunk - HELD):
            start(cross(i))

    gather(0)

    @pl.when(inner == 0)
    def _():
        dispatch(0)

    gather(1)
    dispatch(1)

    @pl.when(is_d)
    def _():
        for i in range(PARTS):
            start(inward(i))

    gather(3)
    gather(2)

    @pl.when(inner == 0)
    def _():
        dispatch(3)
        dispatch(2)

    @pl.when(is_d)
    def _():
        for i in range(PARTS, nchunk):
            start(inward(i))

    for cls in range(4):
        pick[cls] = one_hot(cls, lambda a: scale[a, :]).T.astype(BF16)
    for copy in loads[4:]:
        copy.wait()
    acc[...] = dot(hidden_rows(normed[...], sg[...], su[...]), sd[...])

    def group_cols(m):
        first, count = GROUPS[m]
        return pl.ds(first * strip, count * strip)

    def near_return(base, cls, t):
        to = (other_l, layer)[cls]
        return pltpu.make_async_remote_copy(
            src_ref=ybuf.at[base + t], dst_ref=ret.at[cls * q + s],
            send_sem=sent.at[1], recv_sem=landed.at[5 + cls], device_id={"ep": to * q + t})

    def near(cls):
        base = (inner * q, outer * q)[cls]
        remote(arr.at[pl.ds(0, q - cls)], landed.at[1 - cls]).wait_recv()
        block = pl.ds(base, q)
        got = hidden_rows(arr[block].reshape(q * cap, width), wg[...], wu[...])
        ybuf[block] = dot(got, wd[...]).astype(BF16).reshape(q, cap, width)
        if cls == 1:
            ret[q + s] = ybuf[base + s]
            near_send(1)

    def near_send(cls):
        base = (inner * q, outer * q)[cls]

        def send(i, c):
            near_return(base, cls, (s + 1 + i) % q).start()
            return c

        lax.fori_loop(0, q - cls, send, 0)

    def far_peer(i):
        k = (grp * q + s + i) % (2 * q)
        return k // q, k % q

    def part_cols(part):
        cut = (STRIPS - HELD) * strip
        return pl.ds(cut, width - cut) if part else pl.ds(0, cut)

    def inner_return(i, part):
        g, t = far_peer(i)
        cols = part_cols(part)
        return pltpu.make_async_remote_copy(
            src_ref=ybuf.at[2 * q + g * q + t, :, cols], dst_ref=ret.at[3 * q + s, :, cols],
            send_sem=sent.at[2], recv_sem=landed.at[7 + part], device_id={"grp": g, "ep": layer * q + t})

    def outer_return(i, m):
        sel, g, t = i // (2 * q), *far_peer(i % (2 * q))
        cols = group_cols(m)
        k = sel * 2 * q + g * q + t
        return pltpu.make_async_remote_copy(
            src_ref=ybuf.at[2 * q + k, :, cols], dst_ref=ret.at[2 * q + s, :, cols],
            send_sem=sent.at[3], recv_sem=orecv.at[m],
            device_id={"grp": g, "ep": (inner_l + sel * (outer_l - inner_l)) * q + t})

    def passed_return(i, m):
        g, t = far_peer(i)
        cols = group_cols(m)
        return pltpu.make_async_remote_copy(
            src_ref=ybuf.at[6 * q + g * q + t, :, cols], dst_ref=ret.at[twin, :, cols],
            send_sem=sent.at[4], recv_sem=mrecv.at[m], device_id={"grp": g, "ep": layer * q + t})

    def far_arrived(count, k):
        remote(arr.at[pl.ds(0, count)], landed.at[k]).wait_recv()

    def hand_on(i):
        chunk_landed(i, pgu, pd, precv)
        start(onward(i))

    def take(i):
        chunk_landed(i, fgu, fd, wrecv)
        start(relay(i))

    @pl.when(is_a)
    def _():
        for i in range(PARTS):
            take(i)
            if i == 3:
                dispatch(3)
            if i == 5:
                dispatch(0)
        dispatch(2)

    near(1)

    @pl.when(is_b)
    def _():
        dispatch(3)
        dispatch(0)
        dispatch(2)

    @pl.when(inner == 1)
    def _():
        near(0)
        near_send(0)

    @pl.when(is_a)
    def _():
        for i in range(PARTS):
            hand_on(i)
            if i < STRIPS - HELD:
                take(PARTS + i)
        for i in range(nchunk - HELD, nchunk):
            start(cross(i))

    def inner_hidden():
        far_arrived(2 * q - 1, 2)
        hid[:2 * q * cap] = hidden_rows(
            arr[2 * q:4 * q].reshape(2 * q * cap, width), fgu[0], fgu[1])

    def inner_result(part):
        cols = part_cols(part)
        got = dot(hid[:2 * q * cap], fd[:, cols]).astype(BF16)
        ybuf[2 * q:4 * q, :, cols] = got.reshape(2 * q, cap, cols.size)

        def send(i, c):
            inner_return(i, part).start()
            return c

        lax.fori_loop(1, 2 * q, send, 0)
        ret[3 * q + s, :, cols] = ybuf[2 * q + grp * q + s, :, cols]

    @pl.when(is_c)
    def _():
        for i in range(PARTS):
            chunk_landed(i, fgu, fd, wrecv)
        inner_hidden()
        for i in range(PARTS, nchunk - HELD):
            chunk_landed(i, fgu, fd, wrecv)
        inner_result(0)
        for i in range(nchunk - HELD, nchunk):
            chunk_landed(i, fgu, fd, wrecv)
        if HELD:
            inner_result(1)

    def passed_strips(m):
        cols = group_cols(m)
        got = dot(phid[...], pd[:, cols]).astype(BF16)
        ybuf[6 * q:, :, cols] = got.reshape(2 * q, cap, cols.size)

        def send(i, c):
            passed_return(i, m).start()
            return c

        lax.fori_loop(1, 2 * q, send, 0)
        ret[twin, :, cols] = ybuf[6 * q + grp * q + s, :, cols]

    def outer_strips(m):
        first, count = GROUPS[m]
        cols = group_cols(m)
        for i in range(first, first + count):
            chunk_landed(PARTS + i, fgu, fd, wrecv)
        got = dot(hid[...], fd[:, cols]).astype(BF16)
        ybuf[2 * q:6 * q, :, cols] = got.reshape(4 * q, cap, cols.size)

        def send(i, c):
            outer_return(4 * q - i, m).start()
            return c

        lax.fori_loop(1, 4 * q, send, 0)
        ret[2 * q + s, :, cols] = ybuf[2 * q + grp * q + s, :, cols]

    @pl.when(is_a)
    def _():
        inner_hidden()
        inner_result(0)
        far_arrived(2 * q - 1, 4)
        phid[...] = hidden_rows(arr[6 * q:].reshape(2 * q * cap, width), pgu[0], pgu[1])
        for m in range(STRIPS):
            hand_on(PARTS + m)
            passed_strips(m)
            if m < HELD:
                take(nchunk - HELD + m)
            if m == HELD - 1:
                inner_result(1)

    @pl.when(is_b)
    def _():
        far_arrived(4 * q - 1, 3)
        for i in range(PARTS):
            chunk_landed(i, fgu, fd, wrecv)
            at = pl.ds(i * depth, depth)
            block = arr[2 * q:6 * q, :, at].reshape(4 * q * cap, depth)
            gate, up = dot(block, fgu[0, at]), dot(block, fgu[1, at])
            if i:
                gate, up = gate + gsum[0], up + gsum[1]
            if i < PARTS - 1:
                gsum[0], gsum[1] = gate, up
        hid[...] = (gate / (1.0 + jnp.exp(-gate)) * up).astype(BF16)
        for m in range(len(GROUPS)):
            outer_strips(m)

    def back(k, home):
        remote(ret.at[pl.ds(0, q - home)], landed.at[k]).wait_recv()

    def strip_back(at, sem, m, home):
        remote(ret.at[pl.ds(at, q - home), :, group_cols(m)], sem.at[m]).wait_recv()

    def weighted(cls, cols):
        return dot(pick[cls], ret[cls * q:(cls + 1) * q, :, cols].reshape(q * cap, -1))

    back(6, 1)
    acc[...] += weighted(1, slice(None))

    for part in range(2 if HELD else 1):
        cols = part_cols(part)

        def wait_part(count):
            remote(ret.at[pl.ds(0, count), :, cols], landed.at[7 + part]).wait_recv()

        @pl.when(par == 0)
        def _():
            wait_part(q - 1)

        @pl.when(par == 1)
        def _():
            wait_part(q)

        acc[:, cols] += weighted(3, cols)


    @pl.when(inner == 0)
    def _():
        back(5, 0)

    for m, (first, count) in enumerate(GROUPS):
        @pl.when(is_b)
        def _():
            strip_back(0, mrecv, m, 0)
            strip_back(2 * q, orecv, m, 1)

        @pl.when(is_a)
        def _():
            strip_back(0, mrecv, m, 1)

        @pl.when(jnp.logical_not(is_b))
        def _():
            strip_back(2 * q, orecv, m, 0)

        cols = slice(first * strip, (first + count) * strip)
        out_ref[:, cols] = (acc[:, cols] + weighted(0, cols) + weighted(2, cols)).astype(BF16)

    def drain(ref, count, k):
        remote(ref.at[pl.ds(0, count)], sent.at[k]).wait_send()

    @pl.when(is_a)
    def _():
        drain(obuf, 4 * q - 3, 0)
        drain(ybuf, 2 * q - 1, 1)
        drain(ybuf, 2 * q - 1, 2)
        drain(ybuf, 2 * q - 1, 4)
        weights_sent(own, 0)
        weights_sent(far, 3)
        weights_sent(passed, 6)

    @pl.when(is_b)
    def _():
        drain(obuf, 4 * q - 2, 0)
        drain(ybuf, 2 * q - 1, 1)
        drain(ybuf, 4 * q - 1, 3)

    @pl.when(is_c)
    def _():
        drain(obuf, 4 * q - 2, 0)
        drain(ybuf, q - 1, 1)
        drain(ybuf, 2 * q - 1, 2)

    @pl.when(is_d)
    def _():
        drain(obuf, 4 * q - 1, 0)
        drain(ybuf, q - 1, 1)
        weights_sent(own, 0)


def on_layers(tokens, norm_gain, routes, route_weights, expert_gate, expert_up, expert_down,
              shared_gate, shared_up, shared_down):
    rows, width = tokens.shape
    n = lax.axis_size("ep")
    q = n // 4
    cap = -(-(5 * rows * routes.shape[1] // (4 * n)) // 8) * 8
    vmem = lambda shape, kind=BF16: pltpu.VMEM(shape, kind)
    sems = lambda *shape: pltpu.SemaphoreType.DMA(shape)
    anyspec = pl.BlockSpec(memory_space=pl.ANY)
    vspec = pl.BlockSpec(memory_space=pltpu.VMEM)
    ff = expert_gate.shape[2]
    both = (2,) + expert_gate.shape[1:]
    return pl.pallas_call(
        functools.partial(layers_kernel, n, cap),
        out_shape=pltpu.VMEM((rows, width), BF16),
        in_specs=[anyspec, vspec, vspec, vspec] + [anyspec] * 6,
        out_specs=vspec,
        scratch_shapes=[
            vmem((rows, width)), vmem((rows, width)), vmem((128, rows), F32), vmem((128, rows), F32),
            vmem(expert_gate.shape[1:]), vmem(expert_up.shape[1:]), vmem(expert_down.shape[1:]),
            vmem(both), vmem(expert_down.shape[1:]), vmem(both), vmem(expert_down.shape[1:]),
            vmem(shared_gate.shape), vmem(shared_up.shape), vmem(shared_down.shape),
            vmem((n, cap, width)), vmem((8 * q, cap, width)), vmem((8 * q, cap, width)), vmem((n, cap, width)),
            vmem((rows, width), F32), vmem((2, 4 * q * cap, ff), F32), vmem((4 * q * cap, ff)), vmem((2 * q * cap, ff)), vmem((4, rows, q * cap)),
            sems(7), sems(5), sems(9), sems(9), sems(PARTS + STRIPS), sems(PARTS + STRIPS),
            sems(len(GROUPS)), sems(len(GROUPS)),
        ],
        compiler_params=pltpu.CompilerParams(
            collective_id=0, has_side_effects=True, vmem_limit_bytes=62 * 1024 * 1024 + 512 * 1024),
    )(tokens, norm_gain.reshape(1, width), routes.T, route_weights.T, expert_gate, expert_up,
      expert_down, shared_gate, shared_up, shared_down)


def on_device(*args):
    n, groups = lax.axis_size("ep"), lax.axis_size("grp")
    if groups == 2 and n % 8 == 0 and n <= 32:
        return on_layers(*args)
    return on_halves(*args)


def solution(mesh):
    return jax.shard_map(
        on_device,
        mesh=mesh,
        in_specs=(
            P(("grp", "ep"), None),
            P(),
            P(("grp", "ep"), None),
            P(("grp", "ep"), None),
            P("ep", None, None),
            P("ep", None, None),
            P("ep", None, None),
            P(),
            P(),
            P(),
        ),
        out_specs=P(("grp", "ep"), None),
        check_vma=False,
    )
```

```python
import functools

import jax
import jax.numpy as jnp
from jax import lax
from jax.experimental import pallas as pl
from jax.experimental.pallas import tpu as pltpu
from jax.sharding import PartitionSpec as P

BF16 = jnp.bfloat16
F32 = jnp.float32
PIECES = 2
SLABS = 4
PARTS = 8
SPANS = ((0, 1), (1, 1)) + tuple((i, 2) for i in range(2, 16, 2))
STRIPS = len(SPANS)
HELD = 4


def dot(a, b, dims=((1,), (0,))):
    return lax.dot_general(a, b, (dims, ((), ())), preferred_element_type=F32)


def hidden_rows(rows, w_gate, w_up):
    gate_part = dot(rows, w_gate)
    up_part = dot(rows, w_up)
    return (gate_part / (1.0 + jnp.exp(-gate_part)) * up_part).astype(BF16)


def halves_kernel(
    n, groups, cap,
    tokens_hbm, gain_ref, routes_ref, rw_ref, eg_hbm, eu_hbm, ed_hbm, sg_hbm, su_hbm, sd_hbm,
    out_ref,
    tok, normed, place, scale, wg, wu, wd, fg, fu, fd, sg, su, sd, obuf, arr, ybuf, ret, acc, hid, pick,
    load_sem, wsend, wrecv, xsend, xrecv, dsend, drecv, rsend, rrecv,
):
    half = n // 2
    me = lax.axis_index("ep")
    grp = lax.axis_index("grp")
    base = (me // half) * half
    mine = me % half
    far = (base + half) % n + (mine + half // 2) % half
    rows = tok.shape[0]
    width = tok.shape[1]

    def peer(j):
        total, bit = 0, 1
        while bit < half:
            total = total + bit * (((mine // bit) % 2 + (j // bit) % 2) % 2)
            bit *= 2
        return total

    capp = ret.shape[2]
    if capp > cap:
        low = cap // 16 * 16
        ret[:, :, low:, :] = jnp.zeros((2, half, capp - low, width), BF16)
    barrier = pltpu.get_barrier_semaphore()

    def greet(i, c):
        pl.semaphore_signal(barrier, inc=1, device_id={"ep": base + peer(i)})
        return c

    lax.fori_loop(1, half, greet, 0)
    pl.semaphore_signal(barrier, inc=1, device_id={"ep": far})
    for k in range(1, groups):
        pl.semaphore_signal(barrier, inc=1, device_id={"grp": (grp + k) % groups})

    loads = [(tokens_hbm, tok), (eg_hbm.at[0], wg), (eu_hbm.at[0], wu), (ed_hbm.at[0], wd),
             (sg_hbm, sg), (su_hbm, su), (sd_hbm, sd)]
    loads = [pltpu.make_async_copy(a, b, load_sem.at[i]) for i, (a, b) in enumerate(loads)]
    loads[0].start()

    slab = width // SLABS

    def region(group, a, piece):
        depth = (fg, fu, fd)[a].shape[0] // groups
        if a == 2:
            return pl.ds(pl.multiple_of(group * depth, depth), depth), pl.ds(piece * slab, slab)
        depth = depth // PIECES
        start = (group * PIECES + piece) * depth
        return pl.ds(pl.multiple_of(start, depth), depth), pl.ds(0, fg.shape[1])

    chunks = [(a, piece) for piece in range(PIECES) for a in range(2)]
    chunks += [(2, piece) for piece in range(SLABS)]

    def weight_copy(a, piece):
        src, dst = ((eg_hbm, fg), (eu_hbm, fu), (ed_hbm, fd))[a]
        at, i = region(grp, a, piece), chunks.index((a, piece))
        return pltpu.make_async_remote_copy(
            src_ref=src.at[0, at[0], at[1]], dst_ref=dst.at[at[0], at[1]],
            send_sem=wsend.at[i], recv_sem=wrecv.at[i], device_id={"ep": far})

    def forward_copy(a, piece, k):
        dst = (fg, fu, fd)[a]
        at = region(grp, a, piece)
        i = chunks.index((a, piece)) * max(1, groups - 1) + k - 1
        return pltpu.make_async_remote_copy(
            src_ref=dst.at[at[0], at[1]], dst_ref=dst.at[at[0], at[1]],
            send_sem=xsend.at[i], recv_sem=xrecv.at[i],
            device_id={"grp": (grp + k) % groups})

    pl.semaphore_wait(barrier, half - 1 + 1 + groups - 1)
    weight_copy(*chunks[0]).start()

    lane = lax.broadcasted_iota(jnp.int32, (rows, 128), 1)
    chosen = jnp.zeros((rows, 128), F32)
    weight = jnp.zeros((rows, 128), F32)
    for k in range(routes_ref.shape[1]):
        hit = lane == routes_ref[:, k:k + 1]
        chosen = chosen + jnp.where(hit, 1.0, 0.0)
        weight = weight + jnp.where(hit, rw_ref[:, k:k + 1], 0.0)
    chosen_t = chosen.T
    earlier = (lax.broadcasted_iota(jnp.int32, (rows, rows), 0)
               < lax.broadcasted_iota(jnp.int32, (rows, rows), 1))
    before = dot(chosen_t.astype(BF16), jnp.where(earlier, 1.0, 0.0).astype(BF16))
    place[...] = jnp.where(chosen_t > 0.5, before, -1.0)
    scale[...] = weight.T

    loads[0].wait()
    for copy in loads[1:]:
        copy.start()

    def norm_step(i, c):
        at = pl.ds(pl.multiple_of(i * 32, 32), 32)
        x = tok[at, :].astype(F32)
        factor = lax.rsqrt(jnp.mean(x * x, axis=-1, keepdims=True) + 1e-06)
        normed[at, :] = (x * factor * gain_ref[...]).astype(BF16)
        return c

    lax.fori_loop(0, rows // 32, norm_step, 0)
    slot = lax.broadcasted_iota(jnp.int32, (capp, rows), 0).astype(F32)
    slot = jnp.where(slot < cap, slot, -2.0)

    def gather(p):
        ours = slot == place[pl.ds(base + p, 1), :]
        theirs = slot == place[pl.ds((base + half) % n + (p + half // 2) % half, 1), :]
        want = jnp.concatenate([jnp.where(ours, 1.0, 0.0), jnp.where(theirs, 1.0, 0.0)], axis=0)
        got = dot(want.astype(BF16), normed[...])
        return got[:capp].astype(BF16), got[capp:].astype(BF16)

    used = pl.ds(0, cap)

    def dispatch_copy(p):
        return pltpu.make_async_remote_copy(
            src_ref=obuf.at[:, p, used], dst_ref=arr.at[:, mine, used],
            send_sem=dsend.at[p], recv_sem=drecv.at[mine], device_id={"ep": base + p})

    def dispatch_wait(p):
        pltpu.make_async_remote_copy(
            src_ref=obuf.at[:, p, used], dst_ref=arr.at[:, p, used],
            send_sem=dsend.at[p], recv_sem=drecv.at[p], device_id={"ep": base + p}).wait_recv()

    def message(ref, p, m):
        if m == 0:
            return ref.at[0, p, used]
        return ref.at[1, p, used, pl.ds((m - 1) * slab, slab)]

    def return_copy(p, m):
        return pltpu.make_async_remote_copy(
            src_ref=message(ybuf, p, m), dst_ref=message(ret, mine, m),
            send_sem=rsend.at[p, m], recv_sem=rrecv.at[mine, m], device_id={"ep": base + p})

    def return_wait(p, m):
        pltpu.make_async_remote_copy(
            src_ref=message(ybuf, p, m), dst_ref=message(ret, p, m),
            send_sem=rsend.at[p, m], recv_sem=rrecv.at[p, m],
            device_id={"ep": base + p}).wait_recv()

    def dispatch_step(i, c):
        p = peer(half - 1 - i)
        first, second = gather(p)
        obuf[0, p] = first
        obuf[1, p] = second
        dispatch_copy(p).start()
        return c

    lax.fori_loop(0, half - 1, dispatch_step, 0)
    for a, piece in chunks[1:-SLABS]:
        weight_copy(a, piece).start()
    first, second = gather(mine)
    arr[0, mine] = first
    arr[1, mine] = second

    for copy in loads[4:]:
        copy.wait()
    acc[...] = dot(hidden_rows(normed[...], sg[...], su[...]), sd[...])
    for copy in loads[1:4]:
        copy.wait()

    for b in range(2):
        for p in range(half):
            at = pl.ds((base + b * half) % n + (p + b * (half // 2)) % half, 1)
            want = jnp.where(slot == place[at, :], scale[at, :], 0.0)
            pick[b, p * capp:(p + 1) * capp, :] = want.astype(BF16)

    def own_step(i, c):
        p = peer((i + half // 2 - 1) % (half - 1) + 1)
        dispatch_wait(p)
        ybuf[0, p] = dot(hidden_rows(arr[0, p], wg[...], wu[...]), wd[...]).astype(BF16)
        return_copy(p, 0).start()
        return c

    def forward(a, piece):
        weight_copy(a, piece).wait_recv()
        for k in range(1, groups):
            forward_copy(a, piece, k).start()

    def forwarded(a, piece):
        for k in range(1, groups):
            forward_copy(a, piece, k).wait_recv()

    early = chunks[:-SLABS]
    done = 0
    for i, (a, piece) in enumerate(early):
        until = (half - 1) * (i + 1) // len(early)
        lax.fori_loop(done, until, own_step, 0)
        done = until
        forward(a, piece)
        weight_copy(*chunks[len(early) + i]).start()
    own = dot(hidden_rows(arr[0, mine], wg[...], wu[...]), wd[...]).astype(BF16)
    ret[0, mine] = own

    for a, piece in early:
        forwarded(a, piece)
    hid[...] = hidden_rows(arr[1].reshape(half * capp, width), fg[...], fu[...])

    def far_slab(c):
        forwarded(2, c)
        cols = pl.ds(c * slab, slab)
        got = dot(hid[...], fd[:, cols]).astype(BF16)
        ybuf[1, :, :, cols] = got.reshape(half, capp, slab)

        def send(i, k):
            return_copy(peer(half - 1 - i), 1 + c).start()
            return k

        lax.fori_loop(0, half - 1, send, 0)
        ret[1, mine, :, cols] = ybuf[1, mine, :, cols]

    for c in range(SLABS):
        forward(2, c)
        if c > 0:
            far_slab(c - 1)
    far_slab(SLABS - 1)

    def arrive(m):
        def step(i, k):
            return_wait(peer(i + 1), m)
            return k

        lax.fori_loop(0, half - 1, step, 0)

    arrive(0)
    acc[...] += dot(pick[0], ret[0].reshape(half * capp, width), ((0,), (0,)))
    for c in range(SLABS):
        arrive(1 + c)
        cols = pl.ds(c * slab, slab)
        total = acc[:, cols] + dot(
            pick[1], ret[1, :, :, cols].reshape(half * capp, slab), ((0,), (0,)))
        out_ref[:, cols] = total.astype(BF16)

    def drain(i, c):
        p = peer(half - 1 - i)
        dispatch_copy(p).wait_send()
        for m in range(1 + SLABS):
            return_copy(p, m).wait_send()
        return c

    lax.fori_loop(0, half - 1, drain, 0)
    for a, piece in chunks:
        weight_copy(a, piece).wait_send()
        for k in range(1, groups):
            forward_copy(a, piece, k).wait_send()


def on_halves(tokens, norm_gain, routes, route_weights, expert_gate, expert_up, expert_down,
              shared_gate, shared_up, shared_down):
    rows, width = tokens.shape
    n, groups = lax.axis_size("ep"), lax.axis_size("grp")
    half = n // 2
    cap = -(-(5 * rows * routes.shape[1] // (4 * n)) // 8) * 8
    nchunk = 2 * PIECES + SLABS
    nfwd = nchunk * max(1, groups - 1)
    vmem = lambda shape, kind=BF16: pltpu.VMEM(shape, kind)
    anyspec = pl.BlockSpec(memory_space=pl.ANY)
    vspec = pl.BlockSpec(memory_space=pltpu.VMEM)
    capp = cap
    block = (2, half, capp, width)
    return pl.pallas_call(
        functools.partial(halves_kernel, n, groups, cap),
        out_shape=jax.ShapeDtypeStruct((rows, width), BF16),
        in_specs=[anyspec, vspec, vspec, vspec] + [anyspec] * 6,
        out_specs=vspec,
        scratch_shapes=[
            vmem((rows, width)), vmem((rows, width)), vmem((128, rows), F32), vmem((128, rows), F32),
            vmem(expert_gate.shape[1:]), vmem(expert_up.shape[1:]), vmem(expert_down.shape[1:]),
            vmem(expert_gate.shape[1:]), vmem(expert_up.shape[1:]), vmem(expert_down.shape[1:]),
            vmem(shared_gate.shape), vmem(shared_up.shape), vmem(shared_down.shape),
            vmem(block), vmem(block), vmem(block), vmem(block), vmem((rows, width), F32),
            vmem((half * capp, expert_gate.shape[2])), vmem((2, half * capp, rows)),
            pltpu.SemaphoreType.DMA((7,)),
            pltpu.SemaphoreType.DMA((nchunk,)), pltpu.SemaphoreType.DMA((nchunk,)),
            pltpu.SemaphoreType.DMA((nfwd,)), pltpu.SemaphoreType.DMA((nfwd,)),
            pltpu.SemaphoreType.DMA((half,)), pltpu.SemaphoreType.DMA((half,)),
            pltpu.SemaphoreType.DMA((half, 1 + SLABS)), pltpu.SemaphoreType.DMA((half, 1 + SLABS)),
        ],
        compiler_params=pltpu.CompilerParams(
            collective_id=0, has_side_effects=True, vmem_limit_bytes=60 * 1024 * 1024),
    )(tokens, norm_gain.reshape(1, width), routes, route_weights, expert_gate, expert_up,
      expert_down, shared_gate, shared_up, shared_down)


def layers_kernel(
    n, cap,
    tokens_hbm, gain_ref, routes_ref, rw_ref, eg_hbm, eu_hbm, ed_hbm, sg_hbm, su_hbm, sd_hbm,
    out_ref,
    tok, normed, place, scale, wg, wu, wd, fgu, fd, pgu, pd, sg, su, sd, obuf, arr, ybuf, ret, acc, gsum, hid, phid, pick,
    load_sem, sent, wsent, landed, wrecv, precv, orecv,
):
    q = n // 4
    me = lax.axis_index("ep")
    grp = lax.axis_index("grp")
    layer, s = me // q, me % q
    side = layer // 2
    inner = (layer % 3 + 1) // 2
    outer = 1 - inner
    inner_l, outer_l = 1 + side, 3 * side
    other_l = inner_l + outer_l - layer
    far_in, far_out = 2 - side, 3 - 3 * side
    par = (grp + s) % 2
    twin = s + 1 - 2 * (s % 2)
    rows, width = tok.shape
    is_a = (inner == 1) & (par == 0)
    is_b = (inner == 1) & (par == 1)
    is_c = (inner == 0) & (par == 0)
    is_d = (inner == 0) & (par == 1)

    barrier = pltpu.get_barrier_semaphore()

    first_ep = side * 2 * q
    for g in range(2):
        for i in range(1 - g, 2 * q):
            pl.semaphore_signal(barrier, inc=1, device_id={
                "grp": 1 - grp if g else grp, "ep": first_ep + lax.rem(me - first_ep + i, 2 * q)})

    @pl.when(inner == 1)
    def _():
        pl.semaphore_signal(barrier, inc=1, device_id={"ep": far_in * q + s})
        pl.semaphore_signal(barrier, inc=1, device_id={"ep": far_in * q + twin})

    loads = [(tokens_hbm, tok), (eg_hbm.at[0], wg), (eu_hbm.at[0], wu), (ed_hbm.at[0], wd),
             (sg_hbm, sg), (su_hbm, su), (sd_hbm, sd)]
    loads = [pltpu.make_async_copy(a, b, load_sem.at[i]) for i, (a, b) in enumerate(loads)]
    for copy in loads:
        copy.start()

    unit = width // 16

    def span(m):
        first, count = SPANS[m]
        return pl.ds(first * unit, count * unit)

    depth = fgu.shape[1] // PARTS

    def chunk_copies(i, srcs, dsts, sem, recv, to):
        if i < PARTS:
            at = pl.ds(i * depth, depth)
            pairs = [(srcs[a].at[at], dsts[a].at[at], sem + a) for a in range(2)]
        else:
            at = span(i - PARTS)
            pairs = [(srcs[2].at[:, at], dsts[2].at[:, at], sem + 2)]
        return [pltpu.make_async_remote_copy(
            src_ref=a, dst_ref=b, send_sem=wsent.at[k], recv_sem=recv.at[i], device_id={"ep": to})
            for a, b, k in pairs]

    own = (wg, wu, wd)
    far = (fgu.at[0], fgu.at[1], fd)
    passed = (pgu.at[0], pgu.at[1], pd)
    nchunk = PARTS + STRIPS

    def cross(i):
        return chunk_copies(i, own, far, 0, wrecv, far_in * q + s)

    def relay(i):
        return chunk_copies(i, far, far, 3, wrecv, outer_l * q + s)

    def inward(i):
        return chunk_copies(i, own, passed, 0, precv, inner_l * q + twin)

    def onward(i):
        return chunk_copies(i, passed, far, 6, wrecv, far_in * q + twin)

    def start(copies):
        for copy in copies:
            copy.start()

    def remote(ref, sem):
        return pltpu.make_async_remote_copy(
            src_ref=ref, dst_ref=ref, send_sem=sem, recv_sem=sem, device_id={"ep": other_l * q + s})

    def chunk_landed(i, gu, down, recv):
        if i < PARTS:
            remote(gu.at[:, pl.ds(i * depth, depth)], recv.at[i]).wait_recv()
        else:
            remote(down.at[:, span(i - PARTS)], recv.at[i]).wait_recv()

    def weights_sent(srcs, k):
        for a in range(3):
            remote(srcs[a], wsent.at[k + a]).wait_send()

    expert = lax.broadcasted_iota(jnp.int32, (128, rows), 0)
    chosen = jnp.zeros((128, rows), F32)
    weight = jnp.zeros((128, rows), F32)
    for k in range(routes_ref.shape[0]):
        hit = expert == routes_ref[k:k + 1, :]
        chosen = chosen + jnp.where(hit, 1.0, 0.0)
        weight = weight + jnp.where(hit, rw_ref[k:k + 1, :], 0.0)
    earlier = (lax.broadcasted_iota(jnp.int32, (rows, rows), 0)
               < lax.broadcasted_iota(jnp.int32, (rows, rows), 1))
    before = dot(chosen.astype(BF16), jnp.where(earlier, 1.0, 0.0).astype(BF16))
    place[...] = jnp.where(chosen > 0.5, before, -1.0)
    scale[...] = weight

    loads[0].wait()

    def norm_step(i, c):
        at = pl.ds(pl.multiple_of(i * 32, 32), 32)
        x = tok[at, :].astype(F32)
        factor = lax.rsqrt(jnp.mean(x * x, axis=-1, keepdims=True) + 1e-06)
        normed[at, :] = (x * factor * gain_ref[...]).astype(BF16)
        return c

    lax.fori_loop(0, rows // 32, norm_step, 0)
    slot = lax.broadcasted_iota(jnp.int32, (cap, rows), 0).astype(F32)

    class_layer = (other_l, layer, far_out, far_in)
    near_at = outer * q + s
    land_at = (outer * near_at + inner * (6 * q + grp * q + s), near_at,
               2 * q + outer * 2 * q + grp * q + s, 2 * q + grp * q + s)
    land_on = (outer + inner * 4, 0, 3, 2)
    at_home = (is_a, inner < 2, is_b, par == 0)
    home = (twin, s, s, s)

    def host(cls, t):
        if cls == 0:
            return outer * grp + inner * ((t + 1) % 2), inner_l * q + outer * t + inner * (t + 1 - 2 * (t % 2))
        if cls == 1:
            return grp, layer * q + t
        if cls == 2:
            return (t + 1) % 2, inner_l * q + t
        return t % 2, layer * q + t

    def dispatch_copy(cls, t):
        hg, he = host(cls, t)
        return pltpu.make_async_remote_copy(
            src_ref=obuf.at[cls * q + t], dst_ref=arr.at[land_at[cls]],
            send_sem=sent.at[0], recv_sem=landed.at[land_on[cls]], device_id={"grp": hg, "ep": he})

    def one_hot(cls, values):
        at = [pl.ds(class_layer[cls] * q + t, 1) for t in range(q)]
        return jnp.concatenate([jnp.where(slot == place[a, :], values(a), 0.0) for a in at], axis=0)

    def gather(cls):
        got = dot(one_hot(cls, lambda a: 1.0).astype(BF16), normed[...]).astype(BF16)
        obuf[cls * q:(cls + 1) * q] = got.reshape(q, cap, width)

    def dispatch(cls):
        def send(i, c):
            dispatch_copy(cls, (home[cls] + 1 + i) % q).start()
            return c

        lax.fori_loop(0, q - 1, send, 0)

        @pl.when(at_home[cls])
        def _():
            arr[land_at[cls]] = obuf[cls * q + home[cls]]

        if cls != 1:
            @pl.when(jnp.logical_not(at_home[cls]))
            def _():
                dispatch_copy(cls, home[cls]).start()

    for copy in loads[1:4]:
        copy.wait()
    pl.semaphore_wait(barrier, 4 * q - 1 + 2 * inner)

    @pl.when(is_a)
    def _():
        for i in range(nchunk - HELD):
            start(cross(i))

    gather(0)

    @pl.when(inner == 0)
    def _():
        dispatch(0)

    gather(1)
    dispatch(1)

    @pl.when(is_d)
    def _():
        for i in range(PARTS):
            start(inward(i))

    gather(3)
    gather(2)

    @pl.when(inner == 0)
    def _():
        dispatch(3)
        dispatch(2)

    @pl.when(is_d)
    def _():
        for i in range(PARTS, nchunk):
            start(inward(i))

    for cls in range(4):
        pick[cls] = one_hot(cls, lambda a: scale[a, :]).T.astype(BF16)
    for copy in loads[4:]:
        copy.wait()
    acc[...] = dot(hidden_rows(normed[...], sg[...], su[...]), sd[...])

    def near_return(base, cls, t):
        to = (other_l, layer)[cls]
        return pltpu.make_async_remote_copy(
            src_ref=ybuf.at[base + t], dst_ref=ret.at[cls * q + s],
            send_sem=sent.at[1], recv_sem=landed.at[5 + cls], device_id={"ep": to * q + t})

    def near(cls):
        base = (inner * q, outer * q)[cls]
        remote(arr.at[pl.ds(0, q - cls)], landed.at[1 - cls]).wait_recv()
        block = pl.ds(base, q)
        got = hidden_rows(arr[block].reshape(q * cap, width), wg[...], wu[...])
        ybuf[block] = dot(got, wd[...]).astype(BF16).reshape(q, cap, width)
        if cls == 1:
            ret[q + s] = ybuf[base + s]
            near_send(1)

    def near_send(cls):
        base = (inner * q, outer * q)[cls]

        def send(i, c):
            near_return(base, cls, (s + 1 + i) % q).start()
            return c

        lax.fori_loop(0, q - cls, send, 0)

    def far_peer(i):
        k = (grp * q + s + i) % (2 * q)
        return k // q, k % q

    def part_cols(part):
        cut = SPANS[STRIPS - HELD][0] * unit if HELD else width
        return pl.ds(cut, width - cut) if part else pl.ds(0, cut)

    def inner_return(i, part):
        g, t = far_peer(i)
        cols = part_cols(part)
        return pltpu.make_async_remote_copy(
            src_ref=ybuf.at[2 * q + g * q + t, :, cols], dst_ref=ret.at[3 * q + s, :, cols],
            send_sem=sent.at[2], recv_sem=landed.at[7 + part], device_id={"grp": g, "ep": layer * q + t})

    def outer_return(i, m):
        sel = i // (2 * q)
        turn = lax.rem((1 - sel) * (grp * q + s) + sel * grp * (s // (q // 2)) * (2 * q - 2) + i, 2 * q)
        g, t = turn // q, turn % q
        cols = span(m)
        k = sel * 2 * q + g * q + t
        return pltpu.make_async_remote_copy(
            src_ref=ybuf.at[2 * q + k, :, cols], dst_ref=ret.at[2 * q + s, :, cols],
            send_sem=sent.at[3], recv_sem=orecv.at[m],
            device_id={"grp": g, "ep": (inner_l + sel * (outer_l - inner_l)) * q + t})

    def passed_return(i, m):
        g, t = far_peer(i)
        cols = span(m)
        return pltpu.make_async_remote_copy(
            src_ref=ybuf.at[6 * q + g * q + t, :, cols], dst_ref=ret.at[twin, :, cols],
            send_sem=sent.at[4], recv_sem=orecv.at[m], device_id={"grp": g, "ep": layer * q + t})

    def far_arrived(count, k):
        remote(arr.at[pl.ds(0, count)], landed.at[k]).wait_recv()

    def hand_on(i):
        chunk_landed(i, pgu, pd, precv)
        start(onward(i))

    def take(i):
        chunk_landed(i, fgu, fd, wrecv)
        start(relay(i))

    @pl.when(is_a)
    def _():
        for i in range(PARTS):
            take(i)
            if i == 3:
                dispatch(3)
            if i == 5:
                dispatch(0)
        dispatch(2)

    near(1)

    @pl.when(is_b)
    def _():
        dispatch(3)
        dispatch(0)
        dispatch(2)

    @pl.when(inner == 1)
    def _():
        near(0)
        near_send(0)

    @pl.when(is_a)
    def _():
        for i in range(PARTS):
            hand_on(i)
            if i < STRIPS - HELD:
                take(PARTS + i)
        for i in range(nchunk - HELD, nchunk):
            start(cross(i))

    def inner_hidden():
        far_arrived(2 * q - 1, 2)
        hid[:2 * q * cap] = hidden_rows(
            arr[2 * q:4 * q].reshape(2 * q * cap, width), fgu[0], fgu[1])

    def inner_result(part):
        cols = part_cols(part)
        got = dot(hid[:2 * q * cap], fd[:, cols]).astype(BF16)
        ybuf[2 * q:4 * q, :, cols] = got.reshape(2 * q, cap, cols.size)

        def send(i, c):
            inner_return(i, part).start()
            return c

        lax.fori_loop(1, 2 * q, send, 0)
        ret[3 * q + s, :, cols] = ybuf[2 * q + grp * q + s, :, cols]

    @pl.when(is_c)
    def _():
        for i in range(PARTS):
            chunk_landed(i, fgu, fd, wrecv)
        inner_hidden()
        for i in range(PARTS, nchunk - HELD):
            chunk_landed(i, fgu, fd, wrecv)
        inner_result(0)
        for i in range(nchunk - HELD, nchunk):
            chunk_landed(i, fgu, fd, wrecv)
        if HELD:
            inner_result(1)

    def passed_strips(m):
        cols = span(m)
        got = dot(phid[...], pd[:, cols]).astype(BF16)
        ybuf[6 * q:, :, cols] = got.reshape(2 * q, cap, cols.size)

        def send(i, c):
            passed_return(i, m).start()
            return c

        lax.fori_loop(1, 2 * q, send, 0)
        ret[twin, :, cols] = ybuf[6 * q + grp * q + s, :, cols]

    def outer_strips(m):
        cols = span(m)
        chunk_landed(PARTS + m, fgu, fd, wrecv)

        def send(i, c):
            outer_return(i, m).start()
            return c

        for sel in (1, 0):
            got = dot(hid[sel * 2 * q * cap:(sel + 1) * 2 * q * cap], fd[:, cols]).astype(BF16)
            ybuf[(2 + 2 * sel) * q:(4 + 2 * sel) * q, :, cols] = got.reshape(2 * q, cap, cols.size)
            lax.fori_loop(max(1, sel * 2 * q), (sel + 1) * 2 * q, send, 0)

        ret[2 * q + s, :, cols] = ybuf[2 * q + grp * q + s, :, cols]

    @pl.when(is_a)
    def _():
        inner_hidden()
        inner_result(0)
        far_arrived(2 * q - 1, 4)
        phid[...] = hidden_rows(arr[6 * q:].reshape(2 * q * cap, width), pgu[0], pgu[1])
        for m in range(STRIPS):
            hand_on(PARTS + m)
            passed_strips(m)
            if m < HELD:
                take(nchunk - HELD + m)
            if m == HELD - 1:
                inner_result(1)

    @pl.when(is_b)
    def _():
        far_arrived(4 * q - 1, 3)
        for i in range(PARTS):
            chunk_landed(i, fgu, fd, wrecv)
            at = pl.ds(i * depth, depth)
            block = arr[2 * q:6 * q, :, at].reshape(4 * q * cap, depth)
            gate, up = dot(block, fgu[0, at]), dot(block, fgu[1, at])
            if i:
                gate, up = gate + gsum[0], up + gsum[1]
            if i < PARTS - 1:
                gsum[0], gsum[1] = gate, up
        hid[...] = (gate / (1.0 + jnp.exp(-gate)) * up).astype(BF16)
        for m in range(STRIPS):
            outer_strips(m)

    def back(k, home):
        remote(ret.at[pl.ds(0, q - home)], landed.at[k]).wait_recv()

    def strip_back(m, count):
        remote(ret.at[pl.ds(0, count), :, span(m)], orecv.at[m]).wait_recv()

    def weighted(cls, cols):
        return dot(pick[cls], ret[cls * q:(cls + 1) * q, :, cols].reshape(q * cap, -1))

    back(6, 1)
    acc[...] += weighted(1, slice(None))

    for part in range(2 if HELD else 1):
        cols = part_cols(part)

        def wait_part(count):
            remote(ret.at[pl.ds(0, count), :, cols], landed.at[7 + part]).wait_recv()

        @pl.when(par == 0)
        def _():
            wait_part(q - 1)

        @pl.when(par == 1)
        def _():
            wait_part(q)

        acc[:, cols] += weighted(3, cols)


    @pl.when(inner == 0)
    def _():
        back(5, 0)

    for m in range(STRIPS):
        @pl.when(inner == 1)
        def _():
            strip_back(m, 2 * q - 1)

        @pl.when(inner == 0)
        def _():
            strip_back(m, q)

        cols = span(m)
        out_ref[:, cols] = (acc[:, cols] + weighted(0, cols) + weighted(2, cols)).astype(BF16)

    def drain(ref, count, k):
        remote(ref.at[pl.ds(0, count)], sent.at[k]).wait_send()

    @pl.when(is_a)
    def _():
        drain(obuf, 4 * q - 3, 0)
        drain(ybuf, 2 * q - 1, 1)
        drain(ybuf, 2 * q - 1, 2)
        drain(ybuf, 2 * q - 1, 4)
        weights_sent(own, 0)
        weights_sent(far, 3)
        weights_sent(passed, 6)

    @pl.when(is_b)
    def _():
        drain(obuf, 4 * q - 2, 0)
        drain(ybuf, 2 * q - 1, 1)
        drain(ybuf, 4 * q - 1, 3)

    @pl.when(is_c)
    def _():
        drain(obuf, 4 * q - 2, 0)
        drain(ybuf, q - 1, 1)
        drain(ybuf, 2 * q - 1, 2)

    @pl.when(is_d)
    def _():
        drain(obuf, 4 * q - 1, 0)
        drain(ybuf, q - 1, 1)
        weights_sent(own, 0)


def on_layers(tokens, norm_gain, routes, route_weights, expert_gate, expert_up, expert_down,
              shared_gate, shared_up, shared_down):
    rows, width = tokens.shape
    n = lax.axis_size("ep")
    q = n // 4
    cap = -(-(5 * rows * routes.shape[1] // (4 * n)) // 8) * 8
    vmem = lambda shape, kind=BF16: pltpu.VMEM(shape, kind)
    sems = lambda *shape: pltpu.SemaphoreType.DMA(shape)
    anyspec = pl.BlockSpec(memory_space=pl.ANY)
    vspec = pl.BlockSpec(memory_space=pltpu.VMEM)
    ff = expert_gate.shape[2]
    both = (2,) + expert_gate.shape[1:]
    return pl.pallas_call(
        functools.partial(layers_kernel, n, cap),
        out_shape=pltpu.VMEM((rows, width), BF16),
        in_specs=[anyspec, vspec, vspec, vspec] + [anyspec] * 6,
        out_specs=vspec,
        scratch_shapes=[
            vmem((rows, width)), vmem((rows, width)), vmem((128, rows), F32), vmem((128, rows), F32),
            vmem(expert_gate.shape[1:]), vmem(expert_up.shape[1:]), vmem(expert_down.shape[1:]),
            vmem(both), vmem(expert_down.shape[1:]), vmem(both), vmem(expert_down.shape[1:]),
            vmem(shared_gate.shape), vmem(shared_up.shape), vmem(shared_down.shape),
            vmem((n, cap, width)), vmem((8 * q, cap, width)), vmem((8 * q, cap, width)), vmem((n, cap, width)),
            vmem((rows, width), F32), vmem((2, 4 * q * cap, ff), F32), vmem((4 * q * cap, ff)), vmem((2 * q * cap, ff)), vmem((4, rows, q * cap)),
            sems(7), sems(5), sems(9), sems(9), sems(PARTS + STRIPS), sems(PARTS + STRIPS),
            sems(STRIPS),
        ],
        compiler_params=pltpu.CompilerParams(
            collective_id=0, has_side_effects=True, vmem_limit_bytes=62 * 1024 * 1024 + 512 * 1024),
    )(tokens, norm_gain.reshape(1, width), routes.T, route_weights.T, expert_gate, expert_up,
      expert_down, shared_gate, shared_up, shared_down)


def on_device(*args):
    n, groups = lax.axis_size("ep"), lax.axis_size("grp")
    if groups == 2 and n % 8 == 0 and n <= 32:
        return on_layers(*args)
    return on_halves(*args)


def solution(mesh):
    return jax.shard_map(
        on_device,
        mesh=mesh,
        in_specs=(
            P(("grp", "ep"), None),
            P(),
            P(("grp", "ep"), None),
            P(("grp", "ep"), None),
            P("ep", None, None),
            P("ep", None, None),
            P("ep", None, None),
            P(),
            P(),
            P(),
        ),
        out_specs=P(("grp", "ep"), None),
        check_vma=False,
    )
```

```python
import functools

import jax
import jax.numpy as jnp
from jax import lax
from jax.experimental import pallas as pl
from jax.experimental.pallas import tpu as pltpu
from jax.sharding import PartitionSpec as P

BF16 = jnp.bfloat16
F32 = jnp.float32
PIECES = 2
SLABS = 4
PARTS = 8
SPANS = tuple((i, 1) for i in range(4)) + tuple((i, 2) for i in range(4, 16, 2))
STRIPS = len(SPANS)
HELD = 4


def dot(a, b, dims=((1,), (0,))):
    return lax.dot_general(a, b, (dims, ((), ())), preferred_element_type=F32)


def hidden_rows(rows, w_gate, w_up):
    gate_part = dot(rows, w_gate)
    up_part = dot(rows, w_up)
    return (gate_part / (1.0 + jnp.exp(-gate_part)) * up_part).astype(BF16)


def halves_kernel(
    n, groups, cap,
    tokens_hbm, gain_ref, routes_ref, rw_ref, eg_hbm, eu_hbm, ed_hbm, sg_hbm, su_hbm, sd_hbm,
    out_ref,
    tok, normed, place, scale, wg, wu, wd, fg, fu, fd, sg, su, sd, obuf, arr, ybuf, ret, acc, hid, pick,
    load_sem, wsend, wrecv, xsend, xrecv, dsend, drecv, rsend, rrecv,
):
    half = n // 2
    me = lax.axis_index("ep")
    grp = lax.axis_index("grp")
    base = (me // half) * half
    mine = me % half
    far = (base + half) % n + (mine + half // 2) % half
    rows = tok.shape[0]
    width = tok.shape[1]

    def peer(j):
        total, bit = 0, 1
        while bit < half:
            total = total + bit * (((mine // bit) % 2 + (j // bit) % 2) % 2)
            bit *= 2
        return total

    capp = ret.shape[2]
    if capp > cap:
        low = cap // 16 * 16
        ret[:, :, low:, :] = jnp.zeros((2, half, capp - low, width), BF16)
    barrier = pltpu.get_barrier_semaphore()

    def greet(i, c):
        pl.semaphore_signal(barrier, inc=1, device_id={"ep": base + peer(i)})
        return c

    lax.fori_loop(1, half, greet, 0)
    pl.semaphore_signal(barrier, inc=1, device_id={"ep": far})
    for k in range(1, groups):
        pl.semaphore_signal(barrier, inc=1, device_id={"grp": (grp + k) % groups})

    loads = [(tokens_hbm, tok), (eg_hbm.at[0], wg), (eu_hbm.at[0], wu), (ed_hbm.at[0], wd),
             (sg_hbm, sg), (su_hbm, su), (sd_hbm, sd)]
    loads = [pltpu.make_async_copy(a, b, load_sem.at[i]) for i, (a, b) in enumerate(loads)]
    loads[0].start()

    slab = width // SLABS

    def region(group, a, piece):
        depth = (fg, fu, fd)[a].shape[0] // groups
        if a == 2:
            return pl.ds(pl.multiple_of(group * depth, depth), depth), pl.ds(piece * slab, slab)
        depth = depth // PIECES
        start = (group * PIECES + piece) * depth
        return pl.ds(pl.multiple_of(start, depth), depth), pl.ds(0, fg.shape[1])

    chunks = [(a, piece) for piece in range(PIECES) for a in range(2)]
    chunks += [(2, piece) for piece in range(SLABS)]

    def weight_copy(a, piece):
        src, dst = ((eg_hbm, fg), (eu_hbm, fu), (ed_hbm, fd))[a]
        at, i = region(grp, a, piece), chunks.index((a, piece))
        return pltpu.make_async_remote_copy(
            src_ref=src.at[0, at[0], at[1]], dst_ref=dst.at[at[0], at[1]],
            send_sem=wsend.at[i], recv_sem=wrecv.at[i], device_id={"ep": far})

    def forward_copy(a, piece, k):
        dst = (fg, fu, fd)[a]
        at = region(grp, a, piece)
        i = chunks.index((a, piece)) * max(1, groups - 1) + k - 1
        return pltpu.make_async_remote_copy(
            src_ref=dst.at[at[0], at[1]], dst_ref=dst.at[at[0], at[1]],
            send_sem=xsend.at[i], recv_sem=xrecv.at[i],
            device_id={"grp": (grp + k) % groups})

    pl.semaphore_wait(barrier, half - 1 + 1 + groups - 1)
    weight_copy(*chunks[0]).start()

    lane = lax.broadcasted_iota(jnp.int32, (rows, 128), 1)
    chosen = jnp.zeros((rows, 128), F32)
    weight = jnp.zeros((rows, 128), F32)
    for k in range(routes_ref.shape[1]):
        hit = lane == routes_ref[:, k:k + 1]
        chosen = chosen + jnp.where(hit, 1.0, 0.0)
        weight = weight + jnp.where(hit, rw_ref[:, k:k + 1], 0.0)
    chosen_t = chosen.T
    earlier = (lax.broadcasted_iota(jnp.int32, (rows, rows), 0)
               < lax.broadcasted_iota(jnp.int32, (rows, rows), 1))
    before = dot(chosen_t.astype(BF16), jnp.where(earlier, 1.0, 0.0).astype(BF16))
    place[...] = jnp.where(chosen_t > 0.5, before, -1.0)
    scale[...] = weight.T

    loads[0].wait()
    for copy in loads[1:]:
        copy.start()

    def norm_step(i, c):
        at = pl.ds(pl.multiple_of(i * 32, 32), 32)
        x = tok[at, :].astype(F32)
        factor = lax.rsqrt(jnp.mean(x * x, axis=-1, keepdims=True) + 1e-06)
        normed[at, :] = (x * factor * gain_ref[...]).astype(BF16)
        return c

    lax.fori_loop(0, rows // 32, norm_step, 0)
    slot = lax.broadcasted_iota(jnp.int32, (capp, rows), 0).astype(F32)
    slot = jnp.where(slot < cap, slot, -2.0)

    def gather(p):
        ours = slot == place[pl.ds(base + p, 1), :]
        theirs = slot == place[pl.ds((base + half) % n + (p + half // 2) % half, 1), :]
        want = jnp.concatenate([jnp.where(ours, 1.0, 0.0), jnp.where(theirs, 1.0, 0.0)], axis=0)
        got = dot(want.astype(BF16), normed[...])
        return got[:capp].astype(BF16), got[capp:].astype(BF16)

    used = pl.ds(0, cap)

    def dispatch_copy(p):
        return pltpu.make_async_remote_copy(
            src_ref=obuf.at[:, p, used], dst_ref=arr.at[:, mine, used],
            send_sem=dsend.at[p], recv_sem=drecv.at[mine], device_id={"ep": base + p})

    def dispatch_wait(p):
        pltpu.make_async_remote_copy(
            src_ref=obuf.at[:, p, used], dst_ref=arr.at[:, p, used],
            send_sem=dsend.at[p], recv_sem=drecv.at[p], device_id={"ep": base + p}).wait_recv()

    def message(ref, p, m):
        if m == 0:
            return ref.at[0, p, used]
        return ref.at[1, p, used, pl.ds((m - 1) * slab, slab)]

    def return_copy(p, m):
        return pltpu.make_async_remote_copy(
            src_ref=message(ybuf, p, m), dst_ref=message(ret, mine, m),
            send_sem=rsend.at[p, m], recv_sem=rrecv.at[mine, m], device_id={"ep": base + p})

    def return_wait(p, m):
        pltpu.make_async_remote_copy(
            src_ref=message(ybuf, p, m), dst_ref=message(ret, p, m),
            send_sem=rsend.at[p, m], recv_sem=rrecv.at[p, m],
            device_id={"ep": base + p}).wait_recv()

    def dispatch_step(i, c):
        p = peer(half - 1 - i)
        first, second = gather(p)
        obuf[0, p] = first
        obuf[1, p] = second
        dispatch_copy(p).start()
        return c

    lax.fori_loop(0, half - 1, dispatch_step, 0)
    for a, piece in chunks[1:-SLABS]:
        weight_copy(a, piece).start()
    first, second = gather(mine)
    arr[0, mine] = first
    arr[1, mine] = second

    for copy in loads[4:]:
        copy.wait()
    acc[...] = dot(hidden_rows(normed[...], sg[...], su[...]), sd[...])
    for copy in loads[1:4]:
        copy.wait()

    for b in range(2):
        for p in range(half):
            at = pl.ds((base + b * half) % n + (p + b * (half // 2)) % half, 1)
            want = jnp.where(slot == place[at, :], scale[at, :], 0.0)
            pick[b, p * capp:(p + 1) * capp, :] = want.astype(BF16)

    def own_step(i, c):
        p = peer((i + half // 2 - 1) % (half - 1) + 1)
        dispatch_wait(p)
        ybuf[0, p] = dot(hidden_rows(arr[0, p], wg[...], wu[...]), wd[...]).astype(BF16)
        return_copy(p, 0).start()
        return c

    def forward(a, piece):
        weight_copy(a, piece).wait_recv()
        for k in range(1, groups):
            forward_copy(a, piece, k).start()

    def forwarded(a, piece):
        for k in range(1, groups):
            forward_copy(a, piece, k).wait_recv()

    early = chunks[:-SLABS]
    done = 0
    for i, (a, piece) in enumerate(early):
        until = (half - 1) * (i + 1) // len(early)
        lax.fori_loop(done, until, own_step, 0)
        done = until
        forward(a, piece)
        weight_copy(*chunks[len(early) + i]).start()
    own = dot(hidden_rows(arr[0, mine], wg[...], wu[...]), wd[...]).astype(BF16)
    ret[0, mine] = own

    for a, piece in early:
        forwarded(a, piece)
    hid[...] = hidden_rows(arr[1].reshape(half * capp, width), fg[...], fu[...])

    def far_slab(c):
        forwarded(2, c)
        cols = pl.ds(c * slab, slab)
        got = dot(hid[...], fd[:, cols]).astype(BF16)
        ybuf[1, :, :, cols] = got.reshape(half, capp, slab)

        def send(i, k):
            return_copy(peer(half - 1 - i), 1 + c).start()
            return k

        lax.fori_loop(0, half - 1, send, 0)
        ret[1, mine, :, cols] = ybuf[1, mine, :, cols]

    for c in range(SLABS):
        forward(2, c)
        if c > 0:
            far_slab(c - 1)
    far_slab(SLABS - 1)

    def arrive(m):
        def step(i, k):
            return_wait(peer(i + 1), m)
            return k

        lax.fori_loop(0, half - 1, step, 0)

    arrive(0)
    acc[...] += dot(pick[0], ret[0].reshape(half * capp, width), ((0,), (0,)))
    for c in range(SLABS):
        arrive(1 + c)
        cols = pl.ds(c * slab, slab)
        total = acc[:, cols] + dot(
            pick[1], ret[1, :, :, cols].reshape(half * capp, slab), ((0,), (0,)))
        out_ref[:, cols] = total.astype(BF16)

    def drain(i, c):
        p = peer(half - 1 - i)
        dispatch_copy(p).wait_send()
        for m in range(1 + SLABS):
            return_copy(p, m).wait_send()
        return c

    lax.fori_loop(0, half - 1, drain, 0)
    for a, piece in chunks:
        weight_copy(a, piece).wait_send()
        for k in range(1, groups):
            forward_copy(a, piece, k).wait_send()


def on_halves(tokens, norm_gain, routes, route_weights, expert_gate, expert_up, expert_down,
              shared_gate, shared_up, shared_down):
    rows, width = tokens.shape
    n, groups = lax.axis_size("ep"), lax.axis_size("grp")
    half = n // 2
    cap = -(-(5 * rows * routes.shape[1] // (4 * n)) // 8) * 8
    nchunk = 2 * PIECES + SLABS
    nfwd = nchunk * max(1, groups - 1)
    vmem = lambda shape, kind=BF16: pltpu.VMEM(shape, kind)
    anyspec = pl.BlockSpec(memory_space=pl.ANY)
    vspec = pl.BlockSpec(memory_space=pltpu.VMEM)
    capp = cap
    block = (2, half, capp, width)
    return pl.pallas_call(
        functools.partial(halves_kernel, n, groups, cap),
        out_shape=jax.ShapeDtypeStruct((rows, width), BF16),
        in_specs=[anyspec, vspec, vspec, vspec] + [anyspec] * 6,
        out_specs=vspec,
        scratch_shapes=[
            vmem((rows, width)), vmem((rows, width)), vmem((128, rows), F32), vmem((128, rows), F32),
            vmem(expert_gate.shape[1:]), vmem(expert_up.shape[1:]), vmem(expert_down.shape[1:]),
            vmem(expert_gate.shape[1:]), vmem(expert_up.shape[1:]), vmem(expert_down.shape[1:]),
            vmem(shared_gate.shape), vmem(shared_up.shape), vmem(shared_down.shape),
            vmem(block), vmem(block), vmem(block), vmem(block), vmem((rows, width), F32),
            vmem((half * capp, expert_gate.shape[2])), vmem((2, half * capp, rows)),
            pltpu.SemaphoreType.DMA((7,)),
            pltpu.SemaphoreType.DMA((nchunk,)), pltpu.SemaphoreType.DMA((nchunk,)),
            pltpu.SemaphoreType.DMA((nfwd,)), pltpu.SemaphoreType.DMA((nfwd,)),
            pltpu.SemaphoreType.DMA((half,)), pltpu.SemaphoreType.DMA((half,)),
            pltpu.SemaphoreType.DMA((half, 1 + SLABS)), pltpu.SemaphoreType.DMA((half, 1 + SLABS)),
        ],
        compiler_params=pltpu.CompilerParams(
            collective_id=0, has_side_effects=True, vmem_limit_bytes=60 * 1024 * 1024),
    )(tokens, norm_gain.reshape(1, width), routes, route_weights, expert_gate, expert_up,
      expert_down, shared_gate, shared_up, shared_down)


def layers_kernel(
    n, cap,
    tokens_hbm, gain_ref, routes_ref, rw_ref, eg_hbm, eu_hbm, ed_hbm, sg_hbm, su_hbm, sd_hbm,
    out_ref,
    tok, normed, place, scale, wg, wu, wd, fgu, fd, pgu, pd, sg, su, sd, obuf, arr, ybuf, ret, acc, gsum, hid, phid, pick,
    load_sem, sent, wsent, landed, wrecv, precv, orecv,
):
    q = n // 4
    me = lax.axis_index("ep")
    grp = lax.axis_index("grp")
    layer, s = me // q, me % q
    side = layer // 2
    inner = (layer % 3 + 1) // 2
    outer = 1 - inner
    inner_l, outer_l = 1 + side, 3 * side
    other_l = inner_l + outer_l - layer
    far_in, far_out = 2 - side, 3 - 3 * side
    par = (grp + s) % 2
    twin = s + 1 - 2 * (s % 2)
    rows, width = tok.shape
    is_a = (inner == 1) & (par == 0)
    is_b = (inner == 1) & (par == 1)
    is_c = (inner == 0) & (par == 0)
    is_d = (inner == 0) & (par == 1)

    barrier = pltpu.get_barrier_semaphore()

    first_ep = side * 2 * q
    for g in range(2):
        for i in range(1 - g, 2 * q):
            pl.semaphore_signal(barrier, inc=1, device_id={
                "grp": 1 - grp if g else grp, "ep": first_ep + lax.rem(me - first_ep + i, 2 * q)})

    @pl.when(inner == 1)
    def _():
        pl.semaphore_signal(barrier, inc=1, device_id={"ep": far_in * q + s})
        pl.semaphore_signal(barrier, inc=1, device_id={"ep": far_in * q + twin})

    loads = [(tokens_hbm, tok), (eg_hbm.at[0], wg), (eu_hbm.at[0], wu), (ed_hbm.at[0], wd),
             (sg_hbm, sg), (su_hbm, su), (sd_hbm, sd)]
    loads = [pltpu.make_async_copy(a, b, load_sem.at[i]) for i, (a, b) in enumerate(loads)]
    for copy in loads:
        copy.start()

    unit = width // 16

    def span(m):
        first, count = SPANS[m]
        return pl.ds(first * unit, count * unit)

    depth = fgu.shape[1] // PARTS

    def chunk_copies(i, srcs, dsts, sem, recv, to):
        if i < PARTS:
            at = pl.ds(i * depth, depth)
            pairs = [(srcs[a].at[at], dsts[a].at[at], sem + a) for a in range(2)]
        else:
            at = span(i - PARTS)
            pairs = [(srcs[2].at[:, at], dsts[2].at[:, at], sem + 2)]
        return [pltpu.make_async_remote_copy(
            src_ref=a, dst_ref=b, send_sem=wsent.at[k], recv_sem=recv.at[i], device_id={"ep": to})
            for a, b, k in pairs]

    own = (wg, wu, wd)
    far = (fgu.at[0], fgu.at[1], fd)
    passed = (pgu.at[0], pgu.at[1], pd)
    nchunk = PARTS + STRIPS

    def cross(i):
        return chunk_copies(i, own, far, 0, wrecv, far_in * q + s)

    def relay(i):
        return chunk_copies(i, far, far, 3, wrecv, outer_l * q + s)

    def inward(i):
        return chunk_copies(i, own, passed, 0, precv, inner_l * q + twin)

    def onward(i):
        return chunk_copies(i, passed, far, 6, wrecv, far_in * q + twin)

    def start(copies):
        for copy in copies:
            copy.start()

    def remote(ref, sem):
        return pltpu.make_async_remote_copy(
            src_ref=ref, dst_ref=ref, send_sem=sem, recv_sem=sem, device_id={"ep": other_l * q + s})

    def chunk_landed(i, gu, down, recv):
        if i < PARTS:
            remote(gu.at[:, pl.ds(i * depth, depth)], recv.at[i]).wait_recv()
        else:
            remote(down.at[:, span(i - PARTS)], recv.at[i]).wait_recv()

    def weights_sent(srcs, k):
        for a in range(3):
            remote(srcs[a], wsent.at[k + a]).wait_send()

    expert = lax.broadcasted_iota(jnp.int32, (128, rows), 0)
    chosen = jnp.zeros((128, rows), F32)
    weight = jnp.zeros((128, rows), F32)
    for k in range(routes_ref.shape[0]):
        hit = expert == routes_ref[k:k + 1, :]
        chosen = chosen + jnp.where(hit, 1.0, 0.0)
        weight = weight + jnp.where(hit, rw_ref[k:k + 1, :], 0.0)
    earlier = (lax.broadcasted_iota(jnp.int32, (rows, rows), 0)
               < lax.broadcasted_iota(jnp.int32, (rows, rows), 1))
    before = dot(chosen.astype(BF16), jnp.where(earlier, 1.0, 0.0).astype(BF16))
    place[...] = jnp.where(chosen > 0.5, before, -1.0)
    scale[...] = weight

    loads[0].wait()

    def norm_step(i, c):
        at = pl.ds(pl.multiple_of(i * 32, 32), 32)
        x = tok[at, :].astype(F32)
        factor = lax.rsqrt(jnp.mean(x * x, axis=-1, keepdims=True) + 1e-06)
        normed[at, :] = (x * factor * gain_ref[...]).astype(BF16)
        return c

    lax.fori_loop(0, rows // 32, norm_step, 0)
    slot = lax.broadcasted_iota(jnp.int32, (cap, rows), 0).astype(F32)

    class_layer = (other_l, layer, far_out, far_in)
    near_at = outer * q + s
    land_at = (outer * near_at + inner * (6 * q + grp * q + s), near_at,
               2 * q + outer * 2 * q + grp * q + s, 2 * q + grp * q + s)
    land_on = (outer + inner * 4, 0, 3, 2)
    at_home = (is_a, inner < 2, is_b, par == 0)
    home = (twin, s, s, s)

    def host(cls, t):
        if cls == 0:
            return outer * grp + inner * ((t + 1) % 2), inner_l * q + outer * t + inner * (t + 1 - 2 * (t % 2))
        if cls == 1:
            return grp, layer * q + t
        if cls == 2:
            return (t + 1) % 2, inner_l * q + t
        return t % 2, layer * q + t

    def dispatch_copy(cls, t):
        hg, he = host(cls, t)
        return pltpu.make_async_remote_copy(
            src_ref=obuf.at[cls * q + t], dst_ref=arr.at[land_at[cls]],
            send_sem=sent.at[0], recv_sem=landed.at[land_on[cls]], device_id={"grp": hg, "ep": he})

    def one_hot(cls, values):
        at = [pl.ds(class_layer[cls] * q + t, 1) for t in range(q)]
        return jnp.concatenate([jnp.where(slot == place[a, :], values(a), 0.0) for a in at], axis=0)

    def gather(cls):
        got = dot(one_hot(cls, lambda a: 1.0).astype(BF16), normed[...]).astype(BF16)
        obuf[cls * q:(cls + 1) * q] = got.reshape(q, cap, width)

    def dispatch(cls):
        def send(i, c):
            dispatch_copy(cls, (home[cls] + 1 + i) % q).start()
            return c

        lax.fori_loop(0, q - 1, send, 0)

        @pl.when(at_home[cls])
        def _():
            arr[land_at[cls]] = obuf[cls * q + home[cls]]

        if cls != 1:
            @pl.when(jnp.logical_not(at_home[cls]))
            def _():
                dispatch_copy(cls, home[cls]).start()

    for copy in loads[1:4]:
        copy.wait()
    pl.semaphore_wait(barrier, 4 * q - 1 + 2 * inner)

    @pl.when(is_a)
    def _():
        for i in range(nchunk - HELD):
            start(cross(i))

    gather(0)

    @pl.when(inner == 0)
    def _():
        dispatch(0)

    gather(1)
    dispatch(1)

    @pl.when(is_d)
    def _():
        for i in range(PARTS):
            start(inward(i))

    gather(3)
    gather(2)

    @pl.when(inner == 0)
    def _():
        dispatch(3)
        dispatch(2)

    @pl.when(is_d)
    def _():
        for i in range(PARTS, nchunk):
            start(inward(i))

    for cls in range(4):
        pick[cls] = one_hot(cls, lambda a: scale[a, :]).T.astype(BF16)
    for copy in loads[4:]:
        copy.wait()
    acc[...] = dot(hidden_rows(normed[...], sg[...], su[...]), sd[...])

    def near_return(base, cls, t):
        to = (other_l, layer)[cls]
        return pltpu.make_async_remote_copy(
            src_ref=ybuf.at[base + t], dst_ref=ret.at[cls * q + s],
            send_sem=sent.at[1], recv_sem=landed.at[5 + cls], device_id={"ep": to * q + t})

    def near(cls):
        base = (inner * q, outer * q)[cls]
        remote(arr.at[pl.ds(0, q - cls)], landed.at[1 - cls]).wait_recv()
        block = pl.ds(base, q)
        got = hidden_rows(arr[block].reshape(q * cap, width), wg[...], wu[...])
        ybuf[block] = dot(got, wd[...]).astype(BF16).reshape(q, cap, width)
        if cls == 1:
            ret[q + s] = ybuf[base + s]
            near_send(1)

    def near_send(cls):
        base = (inner * q, outer * q)[cls]

        def send(i, c):
            near_return(base, cls, (s + 1 + i) % q).start()
            return c

        lax.fori_loop(0, q - cls, send, 0)

    def far_peer(i):
        k = (grp * q + s + i) % (2 * q)
        return k // q, k % q

    def part_cols(part):
        cut = SPANS[STRIPS - HELD][0] * unit if HELD else width
        return pl.ds(cut, width - cut) if part else pl.ds(0, cut)

    def inner_return(i, part):
        g, t = far_peer(i)
        cols = part_cols(part)
        return pltpu.make_async_remote_copy(
            src_ref=ybuf.at[2 * q + g * q + t, :, cols], dst_ref=ret.at[3 * q + s, :, cols],
            send_sem=sent.at[2], recv_sem=landed.at[7 + part], device_id={"grp": g, "ep": layer * q + t})

    def outer_return(i, m):
        sel = i // (2 * q)
        turn = lax.rem((1 - sel) * (grp * q + s) + sel * grp * (s // (q // 2)) * (2 * q - 2) + i, 2 * q)
        g, t = turn // q, turn % q
        cols = span(m)
        k = sel * 2 * q + g * q + t
        return pltpu.make_async_remote_copy(
            src_ref=ybuf.at[2 * q + k, :, cols], dst_ref=ret.at[2 * q + s, :, cols],
            send_sem=sent.at[3], recv_sem=orecv.at[m],
            device_id={"grp": g, "ep": (inner_l + sel * (outer_l - inner_l)) * q + t})

    def passed_return(i, m):
        g, t = far_peer(i)
        cols = span(m)
        return pltpu.make_async_remote_copy(
            src_ref=ybuf.at[6 * q + g * q + t, :, cols], dst_ref=ret.at[twin, :, cols],
            send_sem=sent.at[4], recv_sem=orecv.at[m], device_id={"grp": g, "ep": layer * q + t})

    def far_arrived(count, k):
        remote(arr.at[pl.ds(0, count)], landed.at[k]).wait_recv()

    def hand_on(i):
        chunk_landed(i, pgu, pd, precv)
        start(onward(i))

    def take(i):
        chunk_landed(i, fgu, fd, wrecv)
        start(relay(i))

    @pl.when(is_a)
    def _():
        for i in range(PARTS):
            take(i)
            if i == 3:
                dispatch(3)
            if i == 5:
                dispatch(0)
        dispatch(2)

    near(1)

    @pl.when(is_b)
    def _():
        dispatch(3)
        dispatch(0)
        dispatch(2)

    @pl.when(inner == 1)
    def _():
        near(0)
        near_send(0)

    @pl.when(is_a)
    def _():
        for i in range(PARTS):
            hand_on(i)
            if i < STRIPS - HELD:
                take(PARTS + i)
        for i in range(nchunk - HELD, nchunk):
            start(cross(i))

    def inner_hidden():
        far_arrived(2 * q - 1, 2)
        hid[:2 * q * cap] = hidden_rows(
            arr[2 * q:4 * q].reshape(2 * q * cap, width), fgu[0], fgu[1])

    def inner_result(part):
        cols = part_cols(part)
        got = dot(hid[:2 * q * cap], fd[:, cols]).astype(BF16)
        ybuf[2 * q:4 * q, :, cols] = got.reshape(2 * q, cap, cols.size)

        def send(i, c):
            inner_return(i, part).start()
            return c

        lax.fori_loop(1, 2 * q, send, 0)
        ret[3 * q + s, :, cols] = ybuf[2 * q + grp * q + s, :, cols]

    @pl.when(is_c)
    def _():
        for i in range(PARTS):
            chunk_landed(i, fgu, fd, wrecv)
        inner_hidden()
        for i in range(PARTS, nchunk - HELD):
            chunk_landed(i, fgu, fd, wrecv)
        inner_result(0)
        for i in range(nchunk - HELD, nchunk):
            chunk_landed(i, fgu, fd, wrecv)
        if HELD:
            inner_result(1)

    def passed_strips(m):
        cols = span(m)
        got = dot(phid[...], pd[:, cols]).astype(BF16)
        ybuf[6 * q:, :, cols] = got.reshape(2 * q, cap, cols.size)

        def send(i, c):
            passed_return(i, m).start()
            return c

        lax.fori_loop(1, 2 * q, send, 0)
        ret[twin, :, cols] = ybuf[6 * q + grp * q + s, :, cols]

    def outer_strips(m):
        cols = span(m)
        chunk_landed(PARTS + m, fgu, fd, wrecv)

        def send(i, c):
            outer_return(i, m).start()
            return c

        for sel in (1, 0):
            got = dot(hid[sel * 2 * q * cap:(sel + 1) * 2 * q * cap], fd[:, cols]).astype(BF16)
            ybuf[(2 + 2 * sel) * q:(4 + 2 * sel) * q, :, cols] = got.reshape(2 * q, cap, cols.size)
            lax.fori_loop(max(1, sel * 2 * q), (sel + 1) * 2 * q, send, 0)

        ret[2 * q + s, :, cols] = ybuf[2 * q + grp * q + s, :, cols]

    @pl.when(is_a)
    def _():
        inner_hidden()
        inner_result(0)
        far_arrived(2 * q - 1, 4)
        phid[...] = hidden_rows(arr[6 * q:].reshape(2 * q * cap, width), pgu[0], pgu[1])
        for m in range(STRIPS):
            hand_on(PARTS + m)
            passed_strips(m)
            if m < HELD:
                take(nchunk - HELD + m)
            if m == HELD - 1:
                inner_result(1)

    @pl.when(is_b)
    def _():
        far_arrived(4 * q - 1, 3)
        for i in range(PARTS):
            chunk_landed(i, fgu, fd, wrecv)
            at = pl.ds(i * depth, depth)
            block = arr[2 * q:6 * q, :, at].reshape(4 * q * cap, depth)
            gate, up = dot(block, fgu[0, at]), dot(block, fgu[1, at])
            if i:
                gate, up = gate + gsum[0], up + gsum[1]
            if i < PARTS - 1:
                gsum[0], gsum[1] = gate, up
        hid[...] = (gate / (1.0 + jnp.exp(-gate)) * up).astype(BF16)
        for m in range(STRIPS):
            outer_strips(m)

    def back(k, home):
        remote(ret.at[pl.ds(0, q - home)], landed.at[k]).wait_recv()

    def strip_back(m, count):
        remote(ret.at[pl.ds(0, count), :, span(m)], orecv.at[m]).wait_recv()

    def weighted(cls, cols):
        return dot(pick[cls], ret[cls * q:(cls + 1) * q, :, cols].reshape(q * cap, -1))

    back(6, 1)
    acc[...] += weighted(1, slice(None))

    for part in range(2 if HELD else 1):
        cols = part_cols(part)

        def wait_part(count):
            remote(ret.at[pl.ds(0, count), :, cols], landed.at[7 + part]).wait_recv()

        @pl.when(par == 0)
        def _():
            wait_part(q - 1)

        @pl.when(par == 1)
        def _():
            wait_part(q)

        acc[:, cols] += weighted(3, cols)


    @pl.when(inner == 0)
    def _():
        back(5, 0)

    for m in range(STRIPS):
        @pl.when(inner == 1)
        def _():
            strip_back(m, 2 * q - 1)

        @pl.when(inner == 0)
        def _():
            strip_back(m, q)

        cols = span(m)
        out_ref[:, cols] = (acc[:, cols] + weighted(0, cols) + weighted(2, cols)).astype(BF16)

    def drain(ref, count, k):
        remote(ref.at[pl.ds(0, count)], sent.at[k]).wait_send()

    @pl.when(is_a)
    def _():
        drain(obuf, 4 * q - 3, 0)
        drain(ybuf, 2 * q - 1, 1)
        drain(ybuf, 2 * q - 1, 2)
        drain(ybuf, 2 * q - 1, 4)
        weights_sent(own, 0)
        weights_sent(far, 3)
        weights_sent(passed, 6)

    @pl.when(is_b)
    def _():
        drain(obuf, 4 * q - 2, 0)
        drain(ybuf, 2 * q - 1, 1)
        drain(ybuf, 4 * q - 1, 3)

    @pl.when(is_c)
    def _():
        drain(obuf, 4 * q - 2, 0)
        drain(ybuf, q - 1, 1)
        drain(ybuf, 2 * q - 1, 2)

    @pl.when(is_d)
    def _():
        drain(obuf, 4 * q - 1, 0)
        drain(ybuf, q - 1, 1)
        weights_sent(own, 0)


def on_layers(tokens, norm_gain, routes, route_weights, expert_gate, expert_up, expert_down,
              shared_gate, shared_up, shared_down):
    rows, width = tokens.shape
    n = lax.axis_size("ep")
    q = n // 4
    cap = -(-(5 * rows * routes.shape[1] // (4 * n)) // 8) * 8
    vmem = lambda shape, kind=BF16: pltpu.VMEM(shape, kind)
    sems = lambda *shape: pltpu.SemaphoreType.DMA(shape)
    anyspec = pl.BlockSpec(memory_space=pl.ANY)
    vspec = pl.BlockSpec(memory_space=pltpu.VMEM)
    ff = expert_gate.shape[2]
    both = (2,) + expert_gate.shape[1:]
    return pl.pallas_call(
        functools.partial(layers_kernel, n, cap),
        out_shape=pltpu.VMEM((rows, width), BF16),
        in_specs=[anyspec, vspec, vspec, vspec] + [anyspec] * 6,
        out_specs=vspec,
        scratch_shapes=[
            vmem((rows, width)), vmem((rows, width)), vmem((128, rows), F32), vmem((128, rows), F32),
            vmem(expert_gate.shape[1:]), vmem(expert_up.shape[1:]), vmem(expert_down.shape[1:]),
            vmem(both), vmem(expert_down.shape[1:]), vmem(both), vmem(expert_down.shape[1:]),
            vmem(shared_gate.shape), vmem(shared_up.shape), vmem(shared_down.shape),
            vmem((n, cap, width)), vmem((8 * q, cap, width)), vmem((8 * q, cap, width)), vmem((n, cap, width)),
            vmem((rows, width), F32), vmem((2, 4 * q * cap, ff), F32), vmem((4 * q * cap, ff)), vmem((2 * q * cap, ff)), vmem((4, rows, q * cap)),
            sems(7), sems(5), sems(9), sems(9), sems(PARTS + STRIPS), sems(PARTS + STRIPS),
            sems(STRIPS),
        ],
        compiler_params=pltpu.CompilerParams(
            collective_id=0, has_side_effects=True, vmem_limit_bytes=62 * 1024 * 1024 + 512 * 1024),
    )(tokens, norm_gain.reshape(1, width), routes.T, route_weights.T, expert_gate, expert_up,
      expert_down, shared_gate, shared_up, shared_down)


def on_device(*args):
    n, groups = lax.axis_size("ep"), lax.axis_size("grp")
    if groups == 2 and n % 8 == 0 and n <= 32:
        return on_layers(*args)
    return on_halves(*args)


def solution(mesh):
    return jax.shard_map(
        on_device,
        mesh=mesh,
        in_specs=(
            P(("grp", "ep"), None),
            P(),
            P(("grp", "ep"), None),
            P(("grp", "ep"), None),
            P("ep", None, None),
            P("ep", None, None),
            P("ep", None, None),
            P(),
            P(),
            P(),
        ),
        out_specs=P(("grp", "ep"), None),
        check_vma=False,
    )
```
